512 devices in a mesh: sp: 32 (over z, x), tp: 16 (over y, core).
Axes of the slice: x: 4, y: 8, z: 8, core: 2. Of those that a mesh axis runs over, the one named last changes fastest.
Arguments:
- hidden_in: bfloat16 [2, 49152, 2048], P(None, ('sp', 'tp')), may hold values from -6 to 6
- w_value: bfloat16 [2048, 2048], P(None, 'tp'), may hold values from -0.125 to 0.125
- w_key: bfloat16 [2048, 2048], P(None, 'tp'), may hold values from -0.125 to 0.125
- w_step: bfloat16 [2048, 32], replicated, may hold values from -0.125 to 0.125
- conv_value: bfloat16 [4, 2048], P(None, 'tp'), may hold values from -3 to 3
- conv_key: bfloat16 [4, 2048], P(None, 'tp'), may hold values from -3 to 3
- step_bias: float32 [32], P('tp'), may hold values from -3 to -1
- decay_rate: float32 [32], P('tp'), may hold values from 2.03450521e-06 to 0.25
- decay_jump: float32 [2, 49152, 32], P(None, 'sp', 'tp'), may hold values from -0.75 to 0
- new_value: bfloat16 [2, 2048], P(None, 'tp'), may hold values from -60 to 60
- new_key: bfloat16 [2, 2048], P(None, 'tp'), may hold values from -6 to 6
- new_query: bfloat16 [2, 2048], P(None, 'tp'), may hold values from -6 to 6
- new_gate: bfloat16 [2, 2048], P(None, 'tp'), may hold values from -6 to 6
- new_step: float32 [2, 32], P(None, 'tp'), may hold values from -6 to 6
- read_gain: bfloat16 [2048], P('tp'), may hold values from 0.099609375 to 1.8984375
Outputs:
- prompt_state: bfloat16 [2, 32, 64, 128], P(None, 'tp', 'sp')
- read_out: bfloat16 [2, 32, 64], P(None, 'tp', 'sp')
The draws below stay inside these ranges and needn't reach their ends.
All inputs are finite; a program needn't handle non-finite values.
Results may differ from the reference program's by a relative error of at most 0.006.
Values may be sent and summed in bfloat16 or wider, within the bound.
No kernel may reach another device: no remote copies, remote signals or barrier semaphores. Data moves between devices by JAX's collectives and lax.ppermute only.
A program may use at most 64 MiB of HBM per device.

```python
import jax
import jax.numpy as jnp
from jax import lax

D = 2048
HEADS = 32
HEAD_DIM = 64
STATE = 128
GROUPS = 16
KERNEL = 4
PROMPT_COUNT = 2
SEG = 1536
PROMPT_LENGTH = 49152


def draw_decay_rate(key, part):
    uniform_draw = jax.random.uniform(key, (HEADS,), jnp.float32)
    bottom = 0.1 / PROMPT_LENGTH
    summit = 0.25
    return jnp.exp(jnp.log(bottom) + uniform_draw * (jnp.log(summit) - jnp.log(bottom)))


def draw_decay_jump(key, part):
    drain_key, noise_key, location_random_key, magnitude_random_key = jax.random.split(key, 4)
    blocks = PROMPT_LENGTH // SEG
    uniform_draw = jax.random.uniform(drain_key, (PROMPT_COUNT, blocks, 1, HEADS), jnp.float32)
    bottom_log = jnp.log(0.1)
    summit_log = jnp.log(1.0)
    leakage_rate = jnp.exp(bottom_log + uniform_draw * (summit_log - bottom_log)) / PROMPT_LENGTH
    roughness = jax.random.uniform(noise_key, (PROMPT_COUNT, blocks, SEG, HEADS), jnp.float32, 0.5, 1.5)
    leakage_rate = (leakage_rate * roughness).reshape(PROMPT_COUNT, PROMPT_LENGTH, HEADS)
    spike_locations = jax.random.randint(location_random_key, (PROMPT_COUNT, 2), 0, PROMPT_LENGTH)
    spike_magnitudes = jnp.log(jax.random.uniform(magnitude_random_key, (PROMPT_COUNT, 2), jnp.float32, 0.5, 0.8))
    token_position = jnp.arange(PROMPT_LENGTH)
    spike_contribution = jnp.sum(jnp.where(token_position[None, :, None] == spike_locations[:, None, :], spike_magnitudes[:, None, :], 0.0), axis=2)
    return spike_contribution[:, :, None] - leakage_rate


def draw_new_value(key, part):
    base = jnp.clip(jax.random.normal(key, (PROMPT_COUNT, HEADS, HEAD_DIM), jnp.float32), -6.0, 6.0)
    channel = jnp.arange(HEAD_DIM).astype(jnp.float32) / (HEAD_DIM - 1)
    rising = jnp.exp(jnp.log(10.0) * channel)
    return (base * rising).reshape(PROMPT_COUNT, HEADS * HEAD_DIM).astype(jnp.bfloat16)


def block_levels(key, shape, pieces, smallest, high):
    level, own = 1.0, jax.random.fold_in(key, 6)
    for dim, blocks in pieces:
        steps = jnp.exp(jax.random.uniform(jax.random.fold_in(own, dim), (blocks,), jnp.float32, smallest / len(pieces), high / len(pieces)))
        level = level * jnp.repeat(steps, shape[dim] // blocks).reshape([-1 if axis == dim else 1 for axis in range(len(shape))])
    return level


def gaussian(stream_key, dims, spread, limit, shards=(), kind=jnp.bfloat16):
    drawn = jax.random.normal(stream_key, dims, jnp.float32) * spread
    if len(shards) > 0:
        drawn = block_levels(stream_key, dims, shards, -0.22, 0.18) * drawn
    return jnp.clip(drawn, min=-limit, max=limit).astype(kind)


def setup_inputs(seed: int = 0) -> dict:
    splits = jax.random.split(jax.random.key(seed), 16)
    hidden_in = gaussian(splits[0], (PROMPT_COUNT, PROMPT_LENGTH, D), 1.0, 6.0, ((1, 512),))
    w_value = gaussian(splits[1], (D, HEADS * HEAD_DIM), D ** -0.5, 0.125, ((1, 16),))
    w_key = gaussian(splits[2], (D, GROUPS * STATE), D ** -0.5, 0.125, ((1, 16),))
    w_step = gaussian(splits[3], (D, HEADS), D ** -0.5, 0.125)
    conv_value = gaussian(splits[4], (KERNEL, HEADS * HEAD_DIM), KERNEL ** -0.5, 3.0, ((1, 16),))
    conv_key = gaussian(splits[5], (KERNEL, GROUPS * STATE), KERNEL ** -0.5, 3.0, ((1, 16),))
    step_bias = jnp.clip(-3.0 + 2.0 * jax.random.uniform(splits[6], (HEADS,), jnp.float32) ** block_levels(splits[6], (HEADS,), ((0, 16),), -0.2, 0.2), -3.0, -1.0)
    decay_rate = draw_decay_rate(jax.random.fold_in(splits[15], 71), 0)
    decay_jump = draw_decay_jump(jax.random.fold_in(splits[15], 71), 0)
    new_value = draw_new_value(jax.random.fold_in(splits[15], 71), 0)
    new_key = gaussian(splits[10], (PROMPT_COUNT, GROUPS * STATE), 1.0, 6.0, ((1, 16),))
    new_query = gaussian(splits[11], (PROMPT_COUNT, GROUPS * STATE), 1.0, 6.0, ((1, 16),))
    new_gate = gaussian(splits[12], (PROMPT_COUNT, HEADS * HEAD_DIM), 1.0, 6.0, ((1, 16),))
    new_step = gaussian(splits[13], (PROMPT_COUNT, HEADS), 1.0, 6.0, ((1, 16),), jnp.float32)
    read_gain = jnp.clip(1.0 + 0.18 * jax.random.normal(splits[14], (HEADS * HEAD_DIM,), jnp.float32), 0.099609375, 1.8984375).astype(jnp.bfloat16)
    return dict(hidden_in=hidden_in, w_value=w_value, w_key=w_key, w_step=w_step, conv_value=conv_value, conv_key=conv_key, step_bias=step_bias, decay_rate=decay_rate, decay_jump=decay_jump, new_value=new_value, new_key=new_key, new_query=new_query, new_gate=new_gate, new_step=new_step, read_gain=read_gain)


EPSILON = 1e-05

def causal_mix(padded_rows, conv_taps):
    tap_count = conv_taps.shape[0]
    length = padded_rows.shape[-2] - tap_count + 1
    running = jnp.zeros(padded_rows.shape[:-2] + (length, padded_rows.shape[-1]), jnp.float32)
    for tap_index in range(tap_count):
        running = running + padded_rows[..., tap_index:tap_index + length, :].astype(jnp.float32) * conv_taps[tap_index].astype(jnp.float32)
    return running

def reference(hidden_in, w_value, w_key, w_step, conv_value, conv_key, step_bias, decay_rate, decay_jump, new_value, new_key, new_query, new_gate, new_step, read_gain):
    per_group = HEADS // GROUPS
    value_cols = HEADS * HEAD_DIM
    conv_taps = jnp.concatenate([conv_value, conv_key], axis=1)

    def prompt_state(seq_pair):
        seq_rows, seq_jump = seq_pair
        proj_value = jnp.dot(seq_rows, w_value, preferred_element_type=jnp.float32).astype(jnp.bfloat16)
        proj_key = jnp.dot(seq_rows, w_key, preferred_element_type=jnp.float32).astype(jnp.bfloat16)
        proj_step = jnp.dot(seq_rows, w_step, preferred_element_type=jnp.float32).astype(jnp.bfloat16)
        joined_cols = jnp.concatenate([proj_value, proj_key], axis=1)
        padded_rows = jnp.pad(joined_cols, ((KERNEL - 1, 0), (0, 0)))
        mixed_rows = jax.nn.silu(causal_mix(padded_rows, conv_taps))
        step_size = jax.nn.softplus(proj_step.astype(jnp.float32) + step_bias)
        log_decay = seq_jump - decay_rate * step_size
        decay_after = lax.optimization_barrier(jnp.sum(log_decay, axis=0, keepdims=True)) - jnp.cumsum(log_decay, axis=0)
        weight = step_size * jnp.exp(decay_after)
        values = mixed_rows[:, :value_cols].reshape(PROMPT_LENGTH, GROUPS, per_group, HEAD_DIM) * weight.reshape(PROMPT_LENGTH, GROUPS, per_group)[..., None]
        keys = mixed_rows[:, value_cols:].reshape(PROMPT_LENGTH, GROUPS, STATE)
        states = jnp.einsum('lgep,lgn->gepn', values, keys, precision=lax.Precision.HIGHEST)
        return states.reshape(HEADS, HEAD_DIM, STATE)
    final_state = lax.map(prompt_state, (hidden_in, decay_jump))
    cache_state = final_state.astype(jnp.bfloat16)
    new_size = jax.nn.softplus(new_step + step_bias)
    keep_share = jnp.exp(-decay_rate * new_size)
    query = new_query.astype(jnp.float32).reshape(PROMPT_COUNT, GROUPS, STATE)
    own_key = new_key.astype(jnp.float32).reshape(PROMPT_COUNT, GROUPS, STATE)
    state_read = jnp.einsum('sgepn,sgn->sgep', final_state.reshape(PROMPT_COUNT, GROUPS, per_group, HEAD_DIM, STATE), query, precision=lax.Precision.HIGHEST)
    key_match = lax.optimization_barrier(jnp.sum(own_key * query, axis=-1))
    own_value = new_value.astype(jnp.float32).reshape(PROMPT_COUNT, GROUPS, per_group, HEAD_DIM)
    size_grid = new_size.reshape(PROMPT_COUNT, GROUPS, per_group)
    keep_grid = keep_share.reshape(PROMPT_COUNT, GROUPS, per_group)
    raw_read = keep_grid[..., None] * state_read + size_grid[..., None] * own_value * key_match[:, :, None, None]
    gated = raw_read.reshape(PROMPT_COUNT, GROUPS, per_group * HEAD_DIM) * jax.nn.silu(new_gate.astype(jnp.float32)).reshape(PROMPT_COUNT, GROUPS, per_group * HEAD_DIM)
    normed = gated * lax.rsqrt(lax.optimization_barrier(jnp.mean(gated * gated, axis=-1, keepdims=True)) + EPSILON)
    read_out = (normed.reshape(PROMPT_COUNT, HEADS * HEAD_DIM) * read_gain.astype(jnp.float32)).astype(jnp.bfloat16)
    return (cache_state, read_out.reshape(PROMPT_COUNT, HEADS, HEAD_DIM))
```

```python
import jax
import jax.numpy as jnp
from jax import lax
from jax.experimental import pallas as pl
from jax.experimental.pallas import tpu as pltpu
from jax.sharding import Mesh
from jax.sharding import PartitionSpec as P

HEAD_DIM = 64
STATE = 128
EPSILON = 1e-05
BF = jnp.bfloat16
F32 = jnp.float32


def mm(a, b, dims):
    return lax.dot_general(a, b, (dims, ((), ())), preferred_element_type=F32)


def piece_states(xs, pieces, places, w, taps, weight, own, other, rows):
    cols = w.shape[1]
    many = len(xs)

    def body(place, *refs):
        x_refs = refs[:many]
        w_ref, t_ref, wt_ref, own_ref, other_ref, own_out, other_out, ext = refs[many:]
        p = [mm(r[...], w_ref[...], ((1,), (0,))).astype(BF).astype(F32) for r in x_refs]
        for n, (i, j, base) in enumerate(pieces):
            for s in range(2):
                ext[2 * n + s, 4:8, :] = p[j][base + 4 * s : base + 4 * s + 4, :]
                ext[2 * n + s, 8 : 8 + rows, :] = p[i][s * rows : (s + 1) * rows, :]
        for s in range(2):
            sums = [own_ref[s], other_ref[s]]
            for n in range(len(pieces)):
                mixed = ext[2 * n + s, 5 : 5 + rows, :] * t_ref[0:1, :]
                for k in range(1, 4):
                    mixed = mixed + ext[2 * n + s, 5 + k : 5 + k + rows, :] * t_ref[k : k + 1, :]
                mixed = mixed / (1.0 + jnp.exp(-mixed))
                lift = wt_ref[place[n], s * rows : (s + 1) * rows, :]
                for g in range(2):
                    parts = [
                        mixed[:, 256 * g + 64 * e : 256 * g + 64 * e + 64] * lift[:, 2 * g + e : 2 * g + e + 1]
                        for e in range(2)
                    ]
                    values = jnp.concatenate(parts, axis=1).astype(BF)
                    keys = mixed[:, 256 * g + 128 : 256 * g + 256].astype(BF)
                    sums[g] = sums[g] + mm(values, keys, ((0,), (0,)))
            own_out[s] = sums[0]
            other_out[s] = sums[1]

    vmem = pl.BlockSpec(memory_space=pltpu.VMEM)
    return pl.pallas_call(
        body,
        out_shape=[jax.ShapeDtypeStruct(own.shape, F32)] * 2,
        in_specs=[pl.BlockSpec(memory_space=pltpu.SMEM)] + [vmem] * (many + 5),
        out_specs=[vmem] * 2,
        scratch_shapes=[pltpu.VMEM((2 * len(pieces), rows + 8, cols), F32)],
        cost_estimate=pl.CostEstimate(
            flops=16 * sum(x.shape[0] for x in xs) * w.size,
            transcendentals=0,
            bytes_accessed=2 * w.size,
        ),
        name="piece_states",
    )(places, *xs, w, taps, weight, own, other)


def packed(own, got, query, total, sp_count):
    share = HEAD_DIM // sp_count

    def body(a_ref, b_ref, q_ref, t_ref, out_ref):
        def put(row, value):
            out_ref[:, row : row + 1, :] = jnp.broadcast_to(value[None], (sp_count, 1, 128))

        left = t_ref[...]
        for k in range(3):
            part = left.astype(BF)
            left = left - part.astype(F32)
            put(12 + k, part)
        put(15, jnp.zeros((1, 128), BF))
        for s in range(2):
            state = a_ref[s] + b_ref[s]
            read = jnp.sum(state * q_ref[s : s + 1, :], axis=1).reshape(1, 128)
            high = read.astype(BF)
            put(8 + s, high)
            put(10 + s, (read - high.astype(F32)).astype(BF))
            for e in range(2):
                cut = state[64 * e : 64 * e + 64, :].astype(BF).reshape(sp_count, share, 128)
                out_ref[:, 4 * s + 2 * e : 4 * s + 2 * e + share, :] = cut

    return pl.pallas_call(
        body,
        out_shape=jax.ShapeDtypeStruct((sp_count, 16, 128), BF),
        in_specs=[pl.BlockSpec(memory_space=pltpu.VMEM)] * 4,
        out_specs=pl.BlockSpec(memory_space=pltpu.VMEM),
        name="packed",
    )(own, got, query, total)


def finished(got, fixed, back):
    sp_count = got.shape[0]

    def body(back_ref, got_ref, fix_ref, state_out, read_out):
        run = jnp.zeros((1, 128), F32)
        total = jnp.zeros((16, 128), F32)
        for j in reversed(range(sp_count)):
            g = got_ref[j].astype(F32)
            e = jnp.exp(run)
            one = [jnp.broadcast_to(e[:, i : i + 1], (1, 128)) for i in range(4)]
            mixed = [jnp.concatenate([one[2 * s][:, :64], one[2 * s + 1][:, 64:]], axis=1) for s in range(2)]
            scale = jnp.concatenate([one[0], one[0], one[1], one[1], one[2], one[2], one[3], one[3], *mixed, *mixed, *mixed, *mixed], axis=0)
            total = total + g * scale
            run = run + g[12:13] + g[13:14] + g[14:15]
        for s in range(2):
            for h in range(2):
                state_out[s, h] = total[4 * s + 2 * h : 4 * s + 2 * h + 2].astype(BF)
        read = total[8:10] + total[10:12]
        gated = (fix_ref[0:2] * read + fix_ref[2:4]) * fix_ref[4:6]
        mean = jnp.mean(gated * gated, axis=1, keepdims=True)
        out = gated * lax.rsqrt(mean + EPSILON) * fix_ref[6:7]
        out = jnp.concatenate([out, jnp.zeros((6, 128), F32)], axis=0)
        read_out[...] = pltpu.roll(out, back_ref[0], 1)

    vmem = pl.BlockSpec(memory_space=pltpu.VMEM)
    return pl.pallas_call(
        body,
        out_shape=[jax.ShapeDtypeStruct((2, 2, 2, 128), BF), jax.ShapeDtypeStruct((8, 128), F32)],
        in_specs=[pl.BlockSpec(memory_space=pltpu.SMEM), vmem, vmem],
        out_specs=[vmem] * 2,
        name="finished",
    )(back, got, fixed)


def per_device(
    hidden_in, w_value, w_key, w_step, conv_value, conv_key, step_bias, decay_rate, decay_jump,
    new_value, new_key, new_query, new_gate, new_step, read_gain,
):
    sp_count, y_count, c_count = (lax.axis_size(a) for a in ("sp", "y", "c"))
    sp, y, c = (lax.axis_index(a) for a in ("sp", "y", "c"))
    tp_count = y_count * c_count
    count = sp_count * tp_count
    rows, width = hidden_in.shape[1:]
    heads = step_bias.shape[0]
    share = HEAD_DIM // sp_count

    def swap(v):
        return lax.ppermute(v, "c", [(0, 1), (1, 0)])

    def onward(v):
        pairs = []
        for i in range(y_count):
            pairs.append((2 * i, 2 * ((i + 1) % y_count)))
            pairs.append((2 * i + 1, 2 * ((i - 1) % y_count) + 1))
        return lax.ppermute(v, ("y", "c"), pairs)

    a = [hidden_in.reshape(2 * rows, width)]
    a.append(onward(a[0]))
    ends = hidden_in[:, rows - 4 :, :].reshape(8, width)
    ends = lax.ppermute(ends, ("sp", "y", "c"), [(i, i + 1) for i in range(count - 1)])
    first = jnp.concatenate([a[0], ends], axis=0)
    xb = [jnp.concatenate([swap(first), ends], axis=0)]
    xb.append(onward(xb[0]))

    steps = mm(a[0], w_step, ((1,), (0,))).astype(BF)
    steps = steps.reshape(2, rows, tp_count, heads).transpose(2, 0, 3, 1)
    steps = lax.all_to_all(steps, ("y", "c"), 0, 0, tiled=True)
    steps = steps.transpose(1, 2, 0, 3).reshape(2, heads, tp_count * rows).astype(F32)
    size = jax.nn.softplus(steps + step_bias[None, :, None])
    log_decay = decay_jump.transpose(0, 2, 1) - decay_rate[None, :, None] * size
    total = jnp.sum(log_decay, axis=2)
    weight = size * jnp.exp(total[:, :, None] - jnp.cumsum(log_decay, axis=2))
    weight = weight.reshape(2, heads, tp_count, rows).transpose(2, 0, 3, 1)
    weight = weight.reshape(tp_count, 2 * rows, heads)
    weight = jnp.concatenate([weight, swap(weight)], axis=2)

    depth = w_value.shape[0]
    w_own = jnp.concatenate(
        [jnp.concatenate([w_value, conv_value], axis=0), jnp.concatenate([w_key, conv_key], axis=0)], axis=1
    )
    w_both = jnp.concatenate([w_own, swap(w_own)], axis=1)
    taps = w_both[depth:].astype(F32)
    w_both = w_both[:depth]

    def place(far, near):
        away = jnp.where(c == 0, y - far, y + far) % y_count
        return away * 2 + (c if near else 1 - c)

    def add(acc, xs, pieces, places):
        return piece_states(xs, pieces, jnp.stack(places).astype(jnp.int32), w_both, taps, weight, *acc, rows)

    acc = (jnp.zeros((2, 128, 128), F32),) * 2
    half = y_count // 2
    acc = add(acc, [first], [(0, 0, 2 * rows)], [place(0, True)])
    for s in range(1, half):
        acc = add(acc, [a[s], xb[s]], [(0, 1, 2 * rows + 8), (1, 1, 2 * rows)], [place(s, True), place(s, False)])
        a.append(onward(a[s]))
        if s + 1 < half:
            xb.append(onward(xb[s]))
    last_halo = onward(xb[half - 1][2 * rows + 8 :])
    own, other = add(acc, [a[half], last_halo], [(0, 1, 0)], [place(half, True)])

    query = new_query.astype(F32)
    new_size = jax.nn.softplus(new_step + step_bias)
    keep = jnp.repeat(jnp.exp(-decay_rate * new_size), HEAD_DIM, axis=1)
    match = jnp.sum(new_key.astype(F32) * query, axis=1)
    term = jnp.repeat(new_size * match[:, None], HEAD_DIM, axis=1) * new_value.astype(F32)
    gain = read_gain.astype(F32)[None]
    fixed = jnp.concatenate([keep, term, jax.nn.silu(new_gate.astype(F32)), gain, jnp.zeros_like(gain)], axis=0)
    lanes = jnp.pad(total.reshape(1, 2 * heads), ((0, 0), (0, 128 - 2 * heads)))

    sent = packed(own, swap(other), query, lanes, sp_count)
    got = lax.all_to_all(sent, "sp", 0, 0, tiled=True)
    back = jnp.reshape((128 - sp * share) % 128, (1,)).astype(jnp.int32)
    cache_state, read = finished(got, fixed, back)
    read = read[:2].reshape(2, heads, HEAD_DIM)[:, :, :share].astype(BF)
    return cache_state, read


def solution(mesh):
    tp = ("y", "c")
    chips = Mesh(mesh.devices.reshape(mesh.shape["sp"], mesh.shape["tp"] // 2, 2), ("sp", *tp))
    return jax.shard_map(
        per_device,
        mesh=chips,
        in_specs=(
            P(None, ("sp", *tp), None), P(None, tp), P(None, tp), P(), P(None, tp), P(None, tp), P(tp), P(tp),
            P(None, "sp", tp), P(None, tp), P(None, tp), P(None, tp), P(None, tp), P(None, tp), P(tp),
        ),
        out_specs=(P(None, tp, "sp", None), P(None, tp, "sp")),
        check_vma=False,
    )
```

```python
import jax
import jax.numpy as jnp
from jax import lax
from jax.experimental import pallas as pl
from jax.experimental.pallas import tpu as pltpu
from jax.sharding import Mesh
from jax.sharding import PartitionSpec as P

HEAD_DIM = 64
EPSILON = 1e-05
BF = jnp.bfloat16
F32 = jnp.float32


def mm(a, b, dims):
    return lax.dot_general(a, b, (dims, ((), ())), preferred_element_type=F32)


GRANT = pltpu.CompilerParams(vmem_limit_bytes=14 * 1024 * 1024)


def piece_states(xs, halo, places, w, weight, own, other, rows, pair):
    depth, cols = w.shape[0] - 4, w.shape[1]
    many = len(xs)

    def body(place, *refs):
        x_refs = refs[:many]
        h_ref, w_ref, wt_ref, own_ref, other_ref, own_out, other_out, ext = refs[many:]
        taps = w_ref[depth : depth + 4, :].astype(F32)

        def project(ref):
            return mm(ref[...], w_ref[:depth, :], ((1,), (0,))).astype(BF).astype(F32)

        p = [project(r) for r in x_refs]
        h = project(h_ref)
        low = place[2] == 0
        for s in range(2):
            before = [h[4 * s : 4 * s + 4, :]]
            if pair:
                ends = [v[(s + 1) * rows - 4 : (s + 1) * rows, :] for v in p]
                before = [jnp.where(low, before[0], ends[1]), jnp.where(low, ends[0], before[0])]
            for n in range(many):
                ext[2 * n + s, 4:8, :] = before[n]
                ext[2 * n + s, 8 : 8 + rows, :] = p[n][s * rows : (s + 1) * rows, :]
        for s in range(2):
            sums = [own_ref[s], other_ref[s]]
            for n in range(many):
                mixed = ext[2 * n + s, 5 : 5 + rows, :] * taps[0:1, :]
                for k in range(1, 4):
                    mixed = mixed + ext[2 * n + s, 5 + k : 5 + k + rows, :] * taps[k : k + 1, :]
                mixed = mixed / (1.0 + jnp.exp(-mixed))
                lift = wt_ref[place[n], s * rows : (s + 1) * rows, :]
                for g in range(2):
                    parts = [
                        mixed[:, 256 * g + 64 * e : 256 * g + 64 * e + 64] * lift[:, 2 * g + e : 2 * g + e + 1]
                        for e in range(2)
                    ]
                    values = jnp.concatenate(parts, axis=1).astype(BF)
                    keys = mixed[:, 256 * g + 128 : 256 * g + 256].astype(BF)
                    sums[g] = sums[g] + mm(values, keys, ((0,), (0,)))
            own_out[s] = sums[0]
            other_out[s] = sums[1]

    vmem = pl.BlockSpec(memory_space=pltpu.VMEM)
    return pl.pallas_call(
        body,
        out_shape=[jax.ShapeDtypeStruct(own.shape, F32)] * 2,
        in_specs=[pl.BlockSpec(memory_space=pltpu.SMEM)] + [vmem] * (many + 5),
        out_specs=[vmem] * 2,
        scratch_shapes=[pltpu.VMEM((2 * many, rows + 8, cols), F32)],
        cost_estimate=pl.CostEstimate(
            flops=16 * sum(x.shape[0] for x in xs) * w.size,
            transcendentals=0,
            bytes_accessed=2 * w.size,
        ),
        compiler_params=GRANT,
        name="piece_states",
    )(places, *xs, halo, w, weight, own, other)


def packed(own, got, query, total, sp_count):
    share = HEAD_DIM // sp_count

    def body(a_ref, b_ref, q_ref, t_ref, out_ref):
        def put(row, value):
            out_ref[:, row : row + 1, :] = jnp.broadcast_to(value[None], (sp_count, 1, 128))

        left = t_ref[...]
        for k in range(3):
            part = left.astype(BF)
            left = left - part.astype(F32)
            put(12 + k, part)
        put(15, jnp.zeros((1, 128), BF))
        for s in range(2):
            state = a_ref[s] + b_ref[s]
            read = jnp.sum(state * q_ref[s : s + 1, :], axis=1).reshape(1, 128)
            high = read.astype(BF)
            put(8 + s, high)
            put(10 + s, (read - high.astype(F32)).astype(BF))
            for e in range(2):
                cut = state[64 * e : 64 * e + 64, :].astype(BF).reshape(sp_count, share, 128)
                out_ref[:, 4 * s + 2 * e : 4 * s + 2 * e + share, :] = cut

    return pl.pallas_call(
        body,
        out_shape=jax.ShapeDtypeStruct((sp_count, 16, 128), BF),
        in_specs=[pl.BlockSpec(memory_space=pltpu.VMEM)] * 4,
        out_specs=pl.BlockSpec(memory_space=pltpu.VMEM),
        compiler_params=GRANT,
        name="packed",
    )(own, got, query, total)


def finished(got, fixed, back):
    sp_count = got.shape[0]

    def body(back_ref, got_ref, fix_ref, state_out, read_out):
        run = jnp.zeros((1, 128), F32)
        total = jnp.zeros((16, 128), F32)
        for j in reversed(range(sp_count)):
            g = got_ref[j].astype(F32)
            e = jnp.exp(run)
            one = [jnp.broadcast_to(e[:, i : i + 1], (1, 128)) for i in range(4)]
            mixed = [jnp.concatenate([one[2 * s][:, :64], one[2 * s + 1][:, 64:]], axis=1) for s in range(2)]
            scale = jnp.concatenate([one[0], one[0], one[1], one[1], one[2], one[2], one[3], one[3], *mixed, *mixed, *mixed, *mixed], axis=0)
            total = total + g * scale
            run = run + g[12:13] + g[13:14] + g[14:15]
        for s in range(2):
            for h in range(2):
                state_out[s, h] = total[4 * s + 2 * h : 4 * s + 2 * h + 2].astype(BF)
        read = total[8:10] + total[10:12]
        gated = (fix_ref[0:2] * read + fix_ref[2:4]) * fix_ref[4:6]
        mean = jnp.mean(gated * gated, axis=1, keepdims=True)
        out = gated * lax.rsqrt(mean + EPSILON) * fix_ref[6:7]
        out = jnp.concatenate([out, jnp.zeros((6, 128), F32)], axis=0)
        out = pltpu.roll(out, back_ref[0], 1)
        for s in range(2):
            for h in range(2):
                read_out[s, h : h + 1, :] = out[s : s + 1, 64 * h : 64 * h + 2].astype(BF)

    vmem = pl.BlockSpec(memory_space=pltpu.VMEM)
    return pl.pallas_call(
        body,
        out_shape=[jax.ShapeDtypeStruct((2, 2, 2, 128), BF), jax.ShapeDtypeStruct((2, 2, 2), BF)],
        in_specs=[pl.BlockSpec(memory_space=pltpu.SMEM), vmem, vmem],
        out_specs=[vmem] * 2,
        compiler_params=GRANT,
        name="finished",
    )(back, got, fixed)


def per_device(
    hidden_in, w_value, w_key, w_step, conv_value, conv_key, step_bias, decay_rate, decay_jump,
    new_value, new_key, new_query, new_gate, new_step, read_gain,
):
    sp_count, y_count, c_count = (lax.axis_size(a) for a in ("sp", "y", "c"))
    sp, y, c = (lax.axis_index(a) for a in ("sp", "y", "c"))
    tp_count = y_count * c_count
    count = sp_count * tp_count
    rows, width = hidden_in.shape[1:]
    heads = step_bias.shape[0]
    share = HEAD_DIM // sp_count

    def swap(v):
        return lax.ppermute(v, "c", [(0, 1), (1, 0)])

    def onward(v):
        pairs = []
        for i in range(y_count):
            pairs.append((2 * i, 2 * ((i + 1) % y_count)))
            pairs.append((2 * i + 1, 2 * ((i - 1) % y_count) + 1))
        return lax.ppermute(v, ("y", "c"), pairs)

    def last(v):
        return v[: 2 * rows].reshape(2, rows, width)[:, rows - 4 :, :].reshape(8, width)

    a = [hidden_in.reshape(2 * rows, width)]
    a.append(onward(a[0]))
    b = [swap(a[0])]
    b.append(onward(b[0]))
    early, first = lax.optimization_barrier((a[0], b[0]))
    ends = last(early), last(first)
    before = jnp.where(c == 1, *ends)
    before = lax.ppermute(before, ("sp", "y", "c"), [(i, i + 2) for i in range(count - 2)])
    halo = [before, onward(before)]

    steps = mm(early, w_step, ((1,), (0,))).astype(BF)
    steps = steps.reshape(2, rows, tp_count, heads).transpose(2, 0, 3, 1)
    steps = lax.all_to_all(steps, ("y", "c"), 0, 0, tiled=True)
    steps = steps.transpose(1, 2, 0, 3).reshape(2, heads, tp_count * rows).astype(F32)
    size = jax.nn.softplus(steps + step_bias[None, :, None])
    log_decay = decay_jump.transpose(0, 2, 1) - decay_rate[None, :, None] * size
    total = jnp.sum(log_decay, axis=2)
    weight = size * jnp.exp(total[:, :, None] - jnp.cumsum(log_decay, axis=2))
    weight = weight.reshape(2, heads, tp_count, rows).transpose(2, 0, 3, 1)
    weight = weight.reshape(tp_count, 2 * rows, heads)
    weight = jnp.concatenate([weight, swap(weight)], axis=2)

    w_own = jnp.concatenate(
        [jnp.concatenate([w_value, conv_value], axis=0), jnp.concatenate([w_key, conv_key], axis=0)], axis=1
    )
    w_both = jnp.concatenate([w_own, swap(w_own)], axis=1)

    def add(acc, xs, halo, far):
        away = jnp.where(c == 0, y - far, y + far) % y_count
        places = jnp.stack([away * 2 + c, away * 2 + 1 - c, c]).astype(jnp.int32)
        return piece_states(xs, halo, places, w_both, weight, *acc, rows, len(xs) == 2)

    acc = (jnp.zeros((2, 128, 128), F32),) * 2
    half = y_count // 2
    acc = add(acc, [a[0]], jnp.where(c == 0, before, ends[1]), 0)
    for s in range(1, half):
        a.append(onward(a[s]))
        if s + 1 < half:
            b.append(onward(b[s]))
            halo.append(onward(halo[s]))
        acc = add(acc, [a[s], b[s]], halo[s], s)
    last_halo = onward(jnp.where(c == 0, halo[half - 1], last(b[half - 1])))
    query = new_query.astype(F32)
    new_size = jax.nn.softplus(new_step + step_bias)
    keep = jnp.repeat(jnp.exp(-decay_rate * new_size), HEAD_DIM, axis=1)
    match = jnp.sum(new_key.astype(F32) * query, axis=1)
    term = jnp.repeat(new_size * match[:, None], HEAD_DIM, axis=1) * new_value.astype(F32)
    gain = read_gain.astype(F32)[None]
    fixed = jnp.concatenate([keep, term, jax.nn.silu(new_gate.astype(F32)), gain, jnp.zeros_like(gain)], axis=0)
    lanes = jnp.pad(total.reshape(1, 2 * heads), ((0, 0), (0, 128 - 2 * heads)))

    back = jnp.reshape((128 - sp * share) % 128, (1,)).astype(jnp.int32)
    acc, lanes, fixed, query, back = lax.optimization_barrier((acc, lanes, fixed, query, back))
    own, other = add(acc, [a[half]], last_halo, half)
    sent = packed(own, swap(other), query, lanes, sp_count)
    got = lax.all_to_all(sent, "sp", 0, 0, tiled=True)
    return tuple(finished(got, fixed, back))


def solution(mesh):
    tp = ("y", "c")
    chips = Mesh(mesh.devices.reshape(mesh.shape["sp"], mesh.shape["tp"] // 2, 2), ("sp", *tp))

    return jax.shard_map(
        per_device,
        mesh=chips,
        in_specs=(
            P(None, ("sp", *tp), None), P(None, tp), P(None, tp), P(), P(None, tp), P(None, tp), P(tp), P(tp),
            P(None, "sp", tp), P(None, tp), P(None, tp), P(None, tp), P(None, tp), P(None, tp), P(tp),
        ),
        out_specs=(P(None, tp, "sp", None), P(None, tp, "sp")),
        check_vma=False,
    )
```

```python
import jax
import jax.numpy as jnp
from jax import lax
from jax.experimental import pallas as pl
from jax.experimental.pallas import tpu as pltpu
from jax.sharding import Mesh
from jax.sharding import PartitionSpec as P

HEAD_DIM = 64
EPSILON = 1e-05
BF = jnp.bfloat16
F32 = jnp.float32


def mm(a, b, dims):
    return lax.dot_general(a, b, (dims, ((), ())), preferred_element_type=F32)


GRANT = pltpu.CompilerParams(vmem_limit_bytes=14 * 1024 * 1024)


def piece_states(xs, halo, places, w, weight, own, other, rows):
    depth = w[0].shape[0] - 4
    many = len(xs)

    def body(place, *refs):
        x_refs = refs[:many]
        h_ref, *w_refs, wt_ref, own_ref, other_ref, own_out, other_out, ext = refs[many:]
        taps = jnp.concatenate([r[depth : depth + 4, :] for r in w_refs], axis=1).astype(F32)

        def project(ref):
            parts = [mm(ref[...], r[:depth, :], ((1,), (0,))).astype(BF).astype(F32) for r in w_refs]
            return jnp.concatenate(parts, axis=1)

        p = [project(r) for r in x_refs]
        h = project(h_ref)
        low = place[2] == 0
        for s in range(2):
            before = [h[4 * s : 4 * s + 4, :]]
            if many == 2:
                ends = [v[(s + 1) * rows - 4 : (s + 1) * rows, :] for v in p]
                before = [jnp.where(low, before[0], ends[1]), jnp.where(low, ends[0], before[0])]
            for n in range(many):
                ext[2 * n + s, 4:8, :] = before[n]
                ext[2 * n + s, 8 : 8 + rows, :] = p[n][s * rows : (s + 1) * rows, :]
        for s in range(2):
            sums = [own_ref[s], other_ref[s]]
            for n in range(many):
                mixed = ext[2 * n + s, 5 : 5 + rows, :] * taps[0:1, :]
                for k in range(1, 4):
                    mixed = mixed + ext[2 * n + s, 5 + k : 5 + k + rows, :] * taps[k : k + 1, :]
                mixed = mixed / (1.0 + jnp.exp(-mixed))
                lift = wt_ref[place[n], s * rows : (s + 1) * rows, :]
                for g in range(2):
                    parts = [
                        mixed[:, 256 * g + 64 * e : 256 * g + 64 * e + 64] * lift[:, 2 * g + e : 2 * g + e + 1]
                        for e in range(2)
                    ]
                    values = jnp.concatenate(parts, axis=1).astype(BF)
                    keys = mixed[:, 256 * g + 128 : 256 * g + 256].astype(BF)
                    sums[g] = sums[g] + mm(values, keys, ((0,), (0,)))
            own_out[s] = sums[0]
            other_out[s] = sums[1]

    vmem = pl.BlockSpec(memory_space=pltpu.VMEM)
    return pl.pallas_call(
        body,
        out_shape=[jax.ShapeDtypeStruct(own.shape, F32)] * 2,
        in_specs=[pl.BlockSpec(memory_space=pltpu.SMEM)] + [vmem] * (many + 6),
        out_specs=[vmem] * 2,
        scratch_shapes=[pltpu.VMEM((2 * many, rows + 8, 512), F32)],
        cost_estimate=pl.CostEstimate(
            flops=32 * sum(x.shape[0] for x in xs) * w[0].size,
            transcendentals=0,
            bytes_accessed=4 * w[0].size,
        ),
        compiler_params=GRANT,
        name="piece_states",
    )(places, *xs, halo, *w, weight, own, other)


def joined(w_value, w_key, conv_value, conv_key):
    depth = w_value.shape[0]

    def body(v_ref, k_ref, cv_ref, ck_ref, out_ref):
        out_ref[:depth, :128] = v_ref[...]
        out_ref[:depth, 128:] = k_ref[...]
        out_ref[depth:, :128] = cv_ref[...]
        out_ref[depth:, 128:] = ck_ref[...]

    return pl.pallas_call(
        body,
        out_shape=jax.ShapeDtypeStruct((depth + conv_value.shape[0], 256), BF),
        in_specs=[pl.BlockSpec(memory_space=pltpu.VMEM)] * 4,
        out_specs=pl.BlockSpec(memory_space=pltpu.VMEM),
        compiler_params=GRANT,
        name="joined",
    )(w_value, w_key, conv_value, conv_key)


def packed(own, got, query, total, sp_count):
    share = HEAD_DIM // sp_count

    def body(a_ref, b_ref, q_ref, t_ref, out_ref):
        def put(row, value):
            out_ref[:, row : row + 1, :] = jnp.broadcast_to(value[None], (sp_count, 1, 128))

        left = t_ref[...]
        for k in range(3):
            part = left.astype(BF)
            left = left - part.astype(F32)
            put(12 + k, part)
        put(15, jnp.zeros((1, 128), BF))
        for s in range(2):
            state = a_ref[s] + b_ref[s]
            read = jnp.sum(state * q_ref[s : s + 1, :], axis=1).reshape(1, 128)
            high = read.astype(BF)
            put(8 + s, high)
            put(10 + s, (read - high.astype(F32)).astype(BF))
            for e in range(2):
                cut = state[64 * e : 64 * e + 64, :].astype(BF).reshape(sp_count, share, 128)
                out_ref[:, 4 * s + 2 * e : 4 * s + 2 * e + share, :] = cut

    return pl.pallas_call(
        body,
        out_shape=jax.ShapeDtypeStruct((sp_count, 16, 128), BF),
        in_specs=[pl.BlockSpec(memory_space=pltpu.VMEM)] * 4,
        out_specs=pl.BlockSpec(memory_space=pltpu.VMEM),
        compiler_params=GRANT,
        name="packed",
    )(own, got, query, total)


def finished(got, fixed, back):
    sp_count = got.shape[0]

    def body(back_ref, got_ref, fix_ref, state_out, read_out):
        run = jnp.zeros((1, 128), F32)
        total = jnp.zeros((16, 128), F32)
        for j in reversed(range(sp_count)):
            g = got_ref[j].astype(F32)
            e = jnp.exp(run)
            one = [jnp.broadcast_to(e[:, i : i + 1], (1, 128)) for i in range(4)]
            mixed = [jnp.concatenate([one[2 * s][:, :64], one[2 * s + 1][:, 64:]], axis=1) for s in range(2)]
            scale = jnp.concatenate([one[0], one[0], one[1], one[1], one[2], one[2], one[3], one[3], *mixed, *mixed, *mixed, *mixed], axis=0)
            total = total + g * scale
            run = run + g[12:13] + g[13:14] + g[14:15]
        for s in range(2):
            for h in range(2):
                state_out[s, h] = total[4 * s + 2 * h : 4 * s + 2 * h + 2].astype(BF)
        read = total[8:10] + total[10:12]
        gated = (fix_ref[0:2] * read + fix_ref[2:4]) * fix_ref[4:6]
        mean = jnp.mean(gated * gated, axis=1, keepdims=True)
        out = gated * lax.rsqrt(mean + EPSILON) * fix_ref[6:7]
        out = jnp.concatenate([out, jnp.zeros((6, 128), F32)], axis=0)
        out = pltpu.roll(out, back_ref[0], 1)
        for s in range(2):
            for h in range(2):
                read_out[s, h : h + 1, :] = out[s : s + 1, 64 * h : 64 * h + 2].astype(BF)

    vmem = pl.BlockSpec(memory_space=pltpu.VMEM)
    return pl.pallas_call(
        body,
        out_shape=[jax.ShapeDtypeStruct((2, 2, 2, 128), BF), jax.ShapeDtypeStruct((2, 2, 2), BF)],
        in_specs=[pl.BlockSpec(memory_space=pltpu.SMEM), vmem, vmem],
        out_specs=[vmem] * 2,
        compiler_params=GRANT,
        name="finished",
    )(back, got, fixed)


def per_device(
    hidden_in, w_value, w_key, w_step, conv_value, conv_key, step_bias, decay_rate, decay_jump,
    new_value, new_key, new_query, new_gate, new_step, read_gain,
):
    sp_count, y_count, c_count = (lax.axis_size(a) for a in ("sp", "y", "c"))
    sp, y, c = (lax.axis_index(a) for a in ("sp", "y", "c"))
    tp_count = y_count * c_count
    count = sp_count * tp_count
    rows, width = hidden_in.shape[1:]
    heads = step_bias.shape[0]
    share = HEAD_DIM // sp_count

    def swap(v):
        return lax.ppermute(v, "c", [(0, 1), (1, 0)])

    def onward(v):
        pairs = []
        for i in range(y_count):
            pairs.append((2 * i, 2 * ((i + 1) % y_count)))
            pairs.append((2 * i + 1, 2 * ((i - 1) % y_count) + 1))
        return lax.ppermute(v, ("y", "c"), pairs)

    def last(v):
        return v[: 2 * rows].reshape(2, rows, width)[:, rows - 4 :, :].reshape(8, width)

    a = [hidden_in.reshape(2 * rows, width)]
    a.append(onward(a[0]))
    b = [swap(a[0])]
    b.append(onward(b[0]))
    early, first = lax.optimization_barrier((a[0], b[0]))
    ends = last(early), last(first)
    before = jnp.where(c == 1, *ends)
    before = lax.ppermute(before, ("sp", "y", "c"), [(i, i + 2) for i in range(count - 2)])

    def straight(v, far):
        pairs = []
        for i in range(y_count):
            pairs.append((2 * i + 1, 2 * ((i + far) % y_count)))
            pairs.append((2 * i, 2 * ((i - far) % y_count) + 1))
        return lax.ppermute(v, ("y", "c"), pairs)

    steps = mm(early, w_step, ((1,), (0,))).astype(BF)
    steps = steps.reshape(2, rows, tp_count, heads).transpose(2, 0, 3, 1)
    steps = lax.all_to_all(steps, ("y", "c"), 0, 0, tiled=True)
    steps = steps.transpose(1, 2, 0, 3).reshape(2, heads, tp_count * rows).astype(F32)
    size = jax.nn.softplus(steps + step_bias[None, :, None])
    log_decay = decay_jump.transpose(0, 2, 1) - decay_rate[None, :, None] * size
    total = jnp.sum(log_decay, axis=2)
    weight = size * jnp.exp(total[:, :, None] - jnp.cumsum(log_decay, axis=2))
    weight = weight.reshape(2, heads, tp_count, rows).transpose(2, 0, 3, 1)
    weight = weight.reshape(tp_count, 2 * rows, heads)
    weight = jnp.concatenate([weight, swap(weight)], axis=2)

    w_own = joined(w_value, w_key, conv_value, conv_key)
    w_both = w_own, swap(w_own)

    def add(acc, xs, halo, far):
        away = jnp.where(c == 0, y - far, y + far) % y_count
        places = jnp.stack([away * 2 + c, away * 2 + 1 - c, c]).astype(jnp.int32)
        return piece_states(xs, halo, places, w_both, weight, *acc, rows)

    acc = (jnp.zeros((2, 128, 128), F32),) * 2
    half = y_count // 2
    acc = add(acc, [a[0]], jnp.where(c == 0, before, ends[1]), 0)
    for s in range(1, half):
        a.append(onward(a[s]))
        if s + 1 < half:
            b.append(onward(b[s]))
        acc = add(acc, [a[s], b[s]], straight(before, s), s)
    last_halo = straight(jnp.where(c == 1, before, ends[0]), half)
    query = new_query.astype(F32)
    new_size = jax.nn.softplus(new_step + step_bias)
    keep = jnp.repeat(jnp.exp(-decay_rate * new_size), HEAD_DIM, axis=1)
    match = jnp.sum(new_key.astype(F32) * query, axis=1)
    term = jnp.repeat(new_size * match[:, None], HEAD_DIM, axis=1) * new_value.astype(F32)
    gain = read_gain.astype(F32)[None]
    fixed = jnp.concatenate([keep, term, jax.nn.silu(new_gate.astype(F32)), gain, jnp.zeros_like(gain)], axis=0)
    lanes = jnp.pad(total.reshape(1, 2 * heads), ((0, 0), (0, 128 - 2 * heads)))

    back = jnp.reshape((128 - sp * share) % 128, (1,)).astype(jnp.int32)
    acc, lanes, fixed, query, back = lax.optimization_barrier((acc, lanes, fixed, query, back))
    own, other = add(acc, [a[half]], last_halo, half)
    sent = packed(own, swap(other), query, lanes, sp_count)
    got = lax.all_to_all(sent, "sp", 0, 0, tiled=True)
    return tuple(finished(got, fixed, back))


def solution(mesh):
    tp = ("y", "c")
    chips = Mesh(mesh.devices.reshape(mesh.shape["sp"], mesh.shape["tp"] // 2, 2), ("sp", *tp))

    return jax.shard_map(
        per_device,
        mesh=chips,
        in_specs=(
            P(None, ("sp", *tp), None), P(None, tp), P(None, tp), P(), P(None, tp), P(None, tp), P(tp), P(tp),
            P(None, "sp", tp), P(None, tp), P(None, tp), P(None, tp), P(None, tp), P(None, tp), P(tp),
        ),
        out_specs=(P(None, tp, "sp", None), P(None, tp, "sp")),
        check_vma=False,
    )
```

```python
import jax
import jax.numpy as jnp
from jax import lax
from jax.experimental import pallas as pl
from jax.experimental.pallas import tpu as pltpu
from jax.sharding import Mesh
from jax.sharding import PartitionSpec as P

HEAD_DIM = 64
EPSILON = 1e-05
BF = jnp.bfloat16
F32 = jnp.float32
GRANT = pltpu.CompilerParams(vmem_limit_bytes=16 * 1024 * 1024)
VMEM = pl.BlockSpec(memory_space=pltpu.VMEM)
SMEM = pl.BlockSpec(memory_space=pltpu.SMEM)


def mm(a, b, dims, precision=None):
    return lax.dot_general(a, b, (dims, ((), ())), preferred_element_type=F32, precision=precision)


def softplus(v):
    return jnp.maximum(v, 0.0) + jnp.log1p(jnp.exp(-jnp.abs(v)))


def piece_states(meta, xs, far, end, w_step, w, jump, rates, runs, rows, chips):
    depth = w[0].shape[0] - 4
    many, both = len(xs), 2 * rows
    given = [] if runs is None else list(runs)

    def body(m_ref, *refs):
        x_refs = refs[:many]
        s_ref, wa_ref, wb_ref, j_ref, r_ref = refs[many : many + 5]
        ins = refs[many + 5 : many + 5 + len(given)]
        own_out, other_out, ext = refs[many + 5 + len(given) :]
        outs = (own_out, other_out)
        y, c = m_ref[0], m_ref[1]
        low = c == 0
        away = jnp.where(low, y - far, y + far)
        wrapped = jnp.logical_or(away < 0, away >= chips)
        chip = jnp.where(away < 0, away + chips, jnp.where(away >= chips, away - chips, away))
        run = 2 if end else jnp.where(wrapped, 1, 0)
        place = (2 * chip + c, 2 * chip + 1 - c)
        for g in range(2):
            if given:
                outs[g][...] = ins[g][...]
            else:
                outs[g][...] = jnp.zeros(outs[g].shape, F32)

        lane = lax.broadcasted_iota(jnp.int32, (8, both), 1)
        i = lax.broadcasted_iota(jnp.int32, (both, both), 0)
        j = lax.broadcasted_iota(jnp.int32, (both, both), 1)
        below = jnp.where(jnp.logical_and(i > j, (i >= rows) == (j >= rows)), 1.0, 0.0)
        sizes, afters, sums = [], [], []
        for n in range(many):
            step = mm(s_ref[...], x_refs[n][...], ((1,), (1,))).astype(BF).astype(F32)[:, :both]
            size = softplus(step + r_ref[0][:, 0:1])
            decay = j_ref[place[n]] - r_ref[1][:, 0:1] * size
            sizes.append(size)
            afters.append(mm(decay, below, ((1,), (0,)), lax.Precision.HIGHEST))
            sums.append([
                jnp.sum(jnp.where(lane < rows, decay, 0.0), axis=1, keepdims=True),
                jnp.sum(jnp.where(lane < rows, 0.0, decay), axis=1, keepdims=True),
            ])
        total = [sum(v[s] for v in sums) for s in range(2)]
        before = [own_out[run, s, 128:136, :] for s in range(2)]
        lead = [jnp.where(low, v[:, 0:1], 0.0) for v in before]
        lifts = []
        for n in range(many):
            more = list(lead)
            if many == 2:
                first = low if n == 0 else jnp.logical_not(low)
                more = [more[s] + jnp.where(first, sums[1 - n][s], 0.0) for s in range(2)]
            weight = sizes[n] * jnp.exp(afters[n] + jnp.where(lane < rows, more[0], more[1]))
            weight = jnp.concatenate([weight, jnp.zeros((8, 256 - both), F32)], axis=1)
            lifts.append(jnp.transpose(weight))

        taps = jnp.concatenate([r[depth : depth + 4, :] for r in (wa_ref, wb_ref)], axis=1).astype(F32)
        for n in range(many):
            x = x_refs[n][...]
            for g, r in enumerate((wa_ref, wb_ref)):
                p = mm(x, r[:depth, :], ((1,), (0,))).astype(BF).astype(F32)
                for s in range(2):
                    ext[2 * n + s, 4:8, 256 * g : 256 * g + 256] = p[both + 4 * s : both + 4 * s + 4, :]
                    ext[2 * n + s, 8 : 8 + rows, 256 * g : 256 * g + 256] = p[s * rows : (s + 1) * rows, :]
        for s in range(2):
            states = [jnp.zeros((128, 128), F32)] * 2
            for n in range(many):
                mixed = ext[2 * n + s, 5 : 5 + rows, :] * taps[0:1, :]
                for k in range(1, 4):
                    mixed = mixed + ext[2 * n + s, 5 + k : 5 + k + rows, :] * taps[k : k + 1, :]
                mixed = mixed / (1.0 + jnp.exp(-mixed))
                lift = lifts[n][s * rows : (s + 1) * rows, :]
                for g in range(2):
                    parts = [
                        mixed[:, 256 * g + 64 * e : 256 * g + 64 * e + 64] * lift[:, 2 * g + e : 2 * g + e + 1]
                        for e in range(2)
                    ]
                    values = jnp.concatenate(parts, axis=1).astype(BF)
                    keys = mixed[:, 256 * g + 128 : 256 * g + 256].astype(BF)
                    states[g] = states[g] + mm(values, keys, ((0,), (0,)))
            fade = jnp.where(low, 1.0, jnp.exp(total[s]))
            for g in range(2):
                for e in range(2):
                    part = slice(64 * e, 64 * e + 64)
                    old = outs[g][run, s, part, :]
                    outs[g][run, s, part, :] = old * fade[2 * g + e : 2 * g + e + 1, :] + states[g][part, :]
                outs[g][run, s, 128:136, :] = before[s] + total[s]

    shape = (3, 2, 136, 128)
    return pl.pallas_call(
        body,
        out_shape=[jax.ShapeDtypeStruct(shape, F32)] * 2,
        in_specs=[SMEM] + [VMEM] * (many + 5 + len(given)),
        out_specs=[VMEM] * 2,
        scratch_shapes=[pltpu.VMEM((2 * many, rows + 8, 512), F32)],
        cost_estimate=pl.CostEstimate(
            flops=32 * sum(x.shape[0] for x in xs) * w[0].size,
            transcendentals=0,
            bytes_accessed=4 * w[0].size,
        ),
        compiler_params=GRANT,
        name="piece_states",
    )(meta, *xs, w_step, *w, jump, rates, *given)


def joined(w_value, w_key, conv_value, conv_key):
    depth = w_value.shape[0]

    def body(v_ref, k_ref, cv_ref, ck_ref, out_ref):
        out_ref[:depth, :128] = v_ref[...]
        out_ref[:depth, 128:] = k_ref[...]
        out_ref[depth:, :128] = cv_ref[...]
        out_ref[depth:, 128:] = ck_ref[...]

    return pl.pallas_call(
        body,
        out_shape=jax.ShapeDtypeStruct((depth + conv_value.shape[0], 256), BF),
        in_specs=[VMEM] * 4,
        out_specs=VMEM,
        compiler_params=GRANT,
        name="joined",
    )(w_value, w_key, conv_value, conv_key)


def terms(step_bias, decay_rate, new_step, new_value, new_key, new_query, new_gate, read_gain):
    def body(b_ref, r_ref, n_ref, v_ref, k_ref, q_ref, g_ref, gain_ref, out_ref, query_ref):
        lane = lax.broadcasted_iota(jnp.int32, (1, 128), 1)

        def spread(a, b):
            return jnp.where(lane < HEAD_DIM, a, b)

        query = q_ref[...].astype(F32)
        query_ref[...] = query
        value, key, gate = (r[...].astype(F32) for r in (v_ref, k_ref, g_ref))
        match = jnp.sum(key * query, axis=1, keepdims=True)
        gates = gate / (1.0 + jnp.exp(-gate))
        rate = spread(r_ref[0], r_ref[1])
        for s in range(2):
            size = softplus(spread(n_ref[s, 0] + b_ref[0], n_ref[s, 1] + b_ref[1]))
            out_ref[s : s + 1, :] = jnp.exp(-rate * size)
            out_ref[2 + s : 3 + s, :] = size * match[s : s + 1, :] * value[s : s + 1, :]
        out_ref[4:6, :] = gates
        out_ref[6:7, :] = gain_ref[...].astype(F32)
        out_ref[7:8, :] = jnp.zeros((1, 128), F32)

    return pl.pallas_call(
        body,
        out_shape=[jax.ShapeDtypeStruct((8, 128), F32), jax.ShapeDtypeStruct((2, 128), F32)],
        in_specs=[SMEM] * 3 + [VMEM] * 5,
        out_specs=[VMEM] * 2,
        compiler_params=GRANT,
        name="terms",
    )(step_bias, decay_rate, new_step, new_value, new_key, new_query, new_gate, read_gain.reshape(1, 128))


def packed(meta, own, got, query, sp_count, chips):
    share = HEAD_DIM // sp_count

    def body(m_ref, a_ref, b_ref, q_ref, out_ref):
        def put(row, value):
            out_ref[:, row : row + 1, :] = jnp.broadcast_to(value[None], (sp_count, 1, 128))

        low = m_ref[1] == 0
        late = m_ref[0] < chips // 2
        lane = lax.broadcasted_iota(jnp.int32, (1, 128), 1)
        left = jnp.zeros((1, 128), F32)
        for s in range(2):
            mine = [a_ref[r, s, 128:130, :] for r in range(3)]
            theirs = [b_ref[r, s, 130:132, :] for r in range(3)]
            d1, d2, d3 = (jnp.where(low, m, t) for m, t in zip(mine, theirs))
            u1, u2, u3 = (jnp.where(low, t, m) for m, t in zip(mine, theirs))
            last = d3 + u3
            after_u1 = d2 + jnp.where(late, last, 0.0)
            after_d1 = after_u1 + u1
            after_u3 = jnp.where(late, d2, after_d1 + d1)
            after_d3 = after_u3 + u3
            after_u2 = after_d1 + d1 + jnp.where(late, 0.0, last)
            total = after_u2 + u2
            for e in range(2):
                left = jnp.where(lane == 2 * s + e, total[e : e + 1, :], left)
            down = [jnp.exp(v) for v in (after_d1, jnp.zeros_like(d2), after_d3)]
            up = [jnp.exp(v) for v in (after_u1, after_u2, after_u3)]
            reads = []
            for e in range(2):
                state = jnp.zeros((64, 128), F32)
                for r in range(3):
                    part = slice(64 * e, 64 * e + 64)
                    scale_a = jnp.where(low, down[r], up[r])[e : e + 1, :]
                    scale_b = jnp.where(low, up[r], down[r])[e : e + 1, :]
                    state = state + a_ref[r, s, part, :] * scale_a + b_ref[r, s, part, :] * scale_b
                reads.append(jnp.sum(state * q_ref[s : s + 1, :], axis=1).reshape(1, 64))
                cut = state.astype(BF).reshape(sp_count, share, 128)
                out_ref[:, 4 * s + 2 * e : 4 * s + 2 * e + share, :] = cut
            read = jnp.concatenate(reads, axis=1)
            high = read.astype(BF)
            put(8 + s, high)
            put(10 + s, (read - high.astype(F32)).astype(BF))
        for k in range(3):
            part = left.astype(BF)
            left = left - part.astype(F32)
            put(12 + k, part)
        put(15, jnp.zeros((1, 128), BF))

    return pl.pallas_call(
        body,
        out_shape=jax.ShapeDtypeStruct((sp_count, 16, 128), BF),
        in_specs=[SMEM] + [VMEM] * 3,
        out_specs=VMEM,
        compiler_params=GRANT,
        name="packed",
    )(meta, own, got, query)


def finished(meta, got, fixed):
    sp_count = got.shape[0]

    def body(m_ref, got_ref, fix_ref, state_out, read_out):
        run = jnp.zeros((1, 128), F32)
        total = jnp.zeros((16, 128), F32)
        for j in reversed(range(sp_count)):
            g = got_ref[j].astype(F32)
            e = jnp.exp(run)
            one = [jnp.broadcast_to(e[:, i : i + 1], (1, 128)) for i in range(4)]
            both = [jnp.concatenate([one[2 * s][:, :64], one[2 * s + 1][:, 64:]], axis=1) for s in range(2)]
            scale = jnp.concatenate([one[i // 2] for i in range(8)] + both * 4, axis=0)
            total = total + g * scale
            run = run + g[12:13] + g[13:14] + g[14:15]
        for s in range(2):
            for h in range(2):
                state_out[s, h] = total[4 * s + 2 * h : 4 * s + 2 * h + 2].astype(BF)
        read = total[8:10] + total[10:12]
        gated = (fix_ref[0:2] * read + fix_ref[2:4]) * fix_ref[4:6]
        mean = jnp.mean(gated * gated, axis=1, keepdims=True)
        out = gated * lax.rsqrt(mean + EPSILON) * fix_ref[6:7]
        out = jnp.concatenate([out, jnp.zeros((6, 128), F32)], axis=0)
        out = pltpu.roll(out, m_ref[2], 1)
        for s in range(2):
            for h in range(2):
                read_out[s, h : h + 1, :] = out[s : s + 1, 64 * h : 64 * h + 2].astype(BF)

    return pl.pallas_call(
        body,
        out_shape=[jax.ShapeDtypeStruct((2, 2, 2, 128), BF), jax.ShapeDtypeStruct((2, 2, 2), BF)],
        in_specs=[SMEM, VMEM, VMEM],
        out_specs=[VMEM] * 2,
        compiler_params=GRANT,
        name="finished",
    )(meta, got, fixed)


def per_device(
    hidden_in, w_value, w_key, w_step, conv_value, conv_key, step_bias, decay_rate, decay_jump,
    new_value, new_key, new_query, new_gate, new_step, read_gain,
):
    sp_count, y_count, c_count = (lax.axis_size(a) for a in ("sp", "y", "c"))
    sp, y, c = (lax.axis_index(a) for a in ("sp", "y", "c"))
    tp_count = y_count * c_count
    count = sp_count * tp_count
    rows, width = hidden_in.shape[1:]
    heads = step_bias.shape[0]
    share = HEAD_DIM // sp_count
    half = y_count // 2

    def swap(v):
        return lax.ppermute(v, "c", [(0, 1), (1, 0)])

    def onward(v):
        pairs = []
        for i in range(y_count):
            pairs.append((2 * i, 2 * ((i + 1) % y_count)))
            pairs.append((2 * i + 1, 2 * ((i - 1) % y_count) + 1))
        return lax.ppermute(v, ("y", "c"), pairs)

    meta = jnp.stack([y, c, (128 - sp * share) % 128]).astype(jnp.int32)

    ends = hidden_in[:, rows - 4 :, :].reshape(8, width)
    ends = lax.ppermute(ends, ("sp", "y", "c"), [(i, i + 1) for i in range(count - 1)])
    a = [jnp.concatenate([hidden_in.reshape(2 * rows, width), ends], axis=0)]
    a.append(onward(a[0]))
    b = [swap(a[0])]
    b.append(onward(b[0]))

    w_own = joined(w_value, w_key, conv_value, conv_key)
    w_both = w_own, swap(w_own)
    pair = lax.dynamic_slice_in_dim(w_step.T, y * 2 * heads, 2 * heads, 0)
    pair = jnp.where(c == 0, pair, jnp.roll(pair, heads, axis=0))
    w_steps = jnp.pad(pair, ((0, 8 - 2 * heads), (0, 0)))
    rates = jnp.broadcast_to(jnp.stack([step_bias, decay_rate])[:, :, None], (2, heads, 128))
    jump = jnp.concatenate([decay_jump.transpose(0, 2, 1), rates], axis=2)
    jump = jnp.concatenate([jump, swap(jump)], axis=1)
    jump = jnp.pad(jump, ((0, 0), (0, 8 - 2 * heads), (0, 0)))
    rates = jump[:, :, tp_count * rows :]
    jump = jump[:, :, : tp_count * rows].reshape(2, 8, tp_count, rows).transpose(2, 1, 0, 3)
    jump = jump.reshape(tp_count, 8, 2 * rows)

    def add(runs, xs, far, end):
        return piece_states(meta, xs, far, end, w_steps, w_both, jump, rates, runs, rows, y_count)

    runs = add(None, [a[0]], 0, False)
    for s in range(1, half):
        a.append(onward(a[s]))
        if s + 1 < half:
            b.append(onward(b[s]))
        runs = add(runs, [a[s], b[s]], s, False)

    fixed, query = terms(step_bias, decay_rate, new_step, new_value, new_key, new_query, new_gate, read_gain)
    runs, fixed, query = lax.optimization_barrier((runs, fixed, query))
    own, other = add(runs, [a[half]], half, True)
    sent = packed(meta, own, swap(other), query, sp_count, y_count)
    got = lax.all_to_all(sent, "sp", 0, 0, tiled=True)
    return tuple(finished(meta, got, fixed))


def solution(mesh):
    tp = ("y", "c")
    chips = Mesh(mesh.devices.reshape(mesh.shape["sp"], mesh.shape["tp"] // 2, 2), ("sp", *tp))

    return jax.shard_map(
        per_device,
        mesh=chips,
        in_specs=(
            P(None, ("sp", *tp), None), P(None, tp), P(None, tp), P(), P(None, tp), P(None, tp), P(tp), P(tp),
            P(None, "sp", tp), P(None, tp), P(None, tp), P(None, tp), P(None, tp), P(None, tp), P(tp),
        ),
        out_specs=(P(None, tp, "sp", None), P(None, tp, "sp")),
        check_vma=False,
    )
```

```python
import jax
import jax.numpy as jnp
from jax import lax
from jax.experimental import pallas as pl
from jax.experimental.pallas import tpu as pltpu
from jax.sharding import Mesh
from jax.sharding import PartitionSpec as P

HEAD_DIM = 64
EPSILON = 1e-05
BF = jnp.bfloat16
F32 = jnp.float32
GRANT = pltpu.CompilerParams(vmem_limit_bytes=16 * 1024 * 1024)
VMEM = pl.BlockSpec(memory_space=pltpu.VMEM)
SMEM = pl.BlockSpec(memory_space=pltpu.SMEM)


def mm(a, b, dims, precision=None):
    return lax.dot_general(a, b, (dims, ((), ())), preferred_element_type=F32, precision=precision)


def halves(v):
    high = v.astype(BF)
    return high, (v - high.astype(F32)).astype(BF)


def product(a, b):
    (ah, al), (bh, bl) = halves(a), halves(b)
    dims = ((0,), (0,))
    return mm(ah, bh, dims) + (mm(al, bh, dims) + mm(ah, bl, dims))


def softplus(v):
    return jnp.maximum(v, 0.0) + jnp.log1p(jnp.exp(-jnp.abs(v)))


def piece_states(meta, xs, far, end, w_step, w, taps, jump, rates, runs, base, rows, chips):
    many, both = len(xs), 2 * rows
    given = [] if runs is None else list(runs)

    def body(m_ref, *refs):
        x_refs = refs[:many]
        s_ref, wa_ref, wb_ref, t_ref, j_ref, r_ref = refs[many : many + 6]
        ins = refs[many + 6 : many + 6 + len(given)]
        own_out, other_out, ext = refs[many + 6 + len(given) :]
        outs = (own_out, other_out)
        y, c = m_ref[0], m_ref[1]
        low = c == 0
        away = jnp.where(low, y - far, y + far)
        wrapped = jnp.logical_or(away < 0, away >= chips)
        chip = jnp.where(away < 0, away + chips, jnp.where(away >= chips, away - chips, away))
        run = 2 if end else jnp.where(wrapped, 1, 0)
        place = (2 * chip + c, 2 * chip + 1 - c)
        for g in range(2):
            if given:
                outs[g][...] = ins[g][...]
            else:
                outs[g][...] = jnp.zeros(outs[g].shape, F32)

        lane = lax.broadcasted_iota(jnp.int32, (8, both), 1)
        i = lax.broadcasted_iota(jnp.int32, (both, both), 0)
        j = lax.broadcasted_iota(jnp.int32, (both, both), 1)
        below = jnp.where(jnp.logical_and(i > j, (i >= rows) == (j >= rows)), 1.0, 0.0)
        sizes, afters, sums = [], [], []
        for n in range(many):
            step = mm(s_ref[...], x_refs[n][...], ((1,), (1,))).astype(BF).astype(F32)[:, :both]
            size = softplus(step + r_ref[0][:, 0:1])
            decay = j_ref[place[n]] - r_ref[1][:, 0:1] * size
            sizes.append(size)
            afters.append(mm(decay, below, ((1,), (0,)), lax.Precision.HIGHEST))
            sums.append([
                jnp.sum(jnp.where(lane < rows, decay, 0.0), axis=1, keepdims=True),
                jnp.sum(jnp.where(lane < rows, 0.0, decay), axis=1, keepdims=True),
            ])
        total = [sum(v[s] for v in sums) for s in range(2)]
        before = [own_out[run, s, 128:136, :] for s in range(2)]
        lead = [jnp.where(low, v[:, 0:1], 0.0) for v in before]
        lifts = []
        for n in range(many):
            more = list(lead)
            if many == 2:
                first = low if n == 0 else jnp.logical_not(low)
                more = [more[s] + jnp.where(first, sums[1 - n][s], 0.0) for s in range(2)]
            weight = sizes[n] * jnp.exp(afters[n] + jnp.where(lane < rows, more[0], more[1]))
            weight = jnp.concatenate([weight, jnp.zeros((8, 256 - both), F32)], axis=1)
            lifts.append(jnp.transpose(weight))

        for n in range(many):
            x = x_refs[n][...]
            for g, r in enumerate((wa_ref, wb_ref)):
                p = mm(x, r[...], ((1,), (0,))).astype(BF).astype(F32)
                for s in range(2):
                    ext[2 * n + s, 4:8, 256 * g : 256 * g + 256] = p[both + 4 * s : both + 4 * s + 4, :]
                    ext[2 * n + s, 8 : 8 + rows, 256 * g : 256 * g + 256] = p[s * rows : (s + 1) * rows, :]
        for s in range(2):
            states = [jnp.zeros((128, 128), F32)] * 2
            for n in range(many):
                mixed = ext[2 * n + s, 5 : 5 + rows, :] * t_ref[0:1, :]
                for k in range(1, 4):
                    mixed = mixed + ext[2 * n + s, 5 + k : 5 + k + rows, :] * t_ref[k : k + 1, :]
                mixed = mixed / (1.0 + jnp.exp(-mixed))
                lift = lifts[n][s * rows : (s + 1) * rows, :]
                for g in range(2):
                    parts = [
                        mixed[:, 256 * g + 64 * e : 256 * g + 64 * e + 64] * lift[:, base + 2 * g + e : base + 2 * g + e + 1]
                        for e in range(2)
                    ]
                    values = jnp.concatenate(parts, axis=1)
                    keys = mixed[:, 256 * g + 128 : 256 * g + 256]
                    states[g] = states[g] + product(values, keys)
            fade = jnp.where(low, 1.0, jnp.exp(total[s]))
            for g in range(2):
                for e in range(2):
                    part = slice(64 * e, 64 * e + 64)
                    old = outs[g][run, s, part, :]
                    outs[g][run, s, part, :] = old * fade[base + 2 * g + e : base + 2 * g + e + 1, :] + states[g][part, :]
                outs[g][run, s, 128:136, :] = before[s] + total[s]

    shape = (3, 2, 136, 128)
    return pl.pallas_call(
        body,
        out_shape=[jax.ShapeDtypeStruct(shape, F32)] * 2,
        in_specs=[SMEM] + [VMEM] * (many + 6 + len(given)),
        out_specs=[VMEM] * 2,
        scratch_shapes=[pltpu.VMEM((2 * many, rows + 8, 512), F32)],
        cost_estimate=pl.CostEstimate(
            flops=32 * sum(x.shape[0] for x in xs) * w[0].size,
            transcendentals=0,
            bytes_accessed=4 * w[0].size,
        ),
        compiler_params=GRANT,
        name="piece_states",
    )(meta, *xs, w_step, *w, taps, jump, rates, *given)


def joined(meta, w_value, w_key, parts):
    depth = w_value.shape[0]
    cut = depth // parts

    def body(m_ref, v_ref, k_ref, out_ref, part_ref):
        out_ref[:, :128] = v_ref[...]
        out_ref[:, 128:] = k_ref[...]
        start = pl.multiple_of(m_ref[3] * cut, cut)
        part_ref[:, :128] = v_ref[pl.ds(start, cut), :]
        part_ref[:, 128:] = k_ref[pl.ds(start, cut), :]

    return pl.pallas_call(
        body,
        out_shape=[jax.ShapeDtypeStruct((depth, 256), BF), jax.ShapeDtypeStruct((cut, 256), BF)],
        in_specs=[SMEM] + [VMEM] * 2,
        out_specs=[VMEM] * 2,
        compiler_params=GRANT,
        name="joined",
    )(meta, w_value, w_key)


def terms(step_bias, decay_rate, new_step, new_value, new_key, new_query, new_gate, read_gain):
    def body(b_ref, r_ref, n_ref, v_ref, k_ref, q_ref, g_ref, gain_ref, out_ref, query_ref):
        lane = lax.broadcasted_iota(jnp.int32, (1, 128), 1)

        def spread(a, b):
            return jnp.where(lane < HEAD_DIM, a, b)

        query = q_ref[...].astype(F32)
        query_ref[...] = query
        value, key, gate = (r[...].astype(F32) for r in (v_ref, k_ref, g_ref))
        match = jnp.sum(key * query, axis=1, keepdims=True)
        gates = gate / (1.0 + jnp.exp(-gate))
        rate = spread(r_ref[0], r_ref[1])
        for s in range(2):
            size = softplus(spread(n_ref[s, 0] + b_ref[0], n_ref[s, 1] + b_ref[1]))
            out_ref[s : s + 1, :] = jnp.exp(-rate * size)
            out_ref[2 + s : 3 + s, :] = size * match[s : s + 1, :] * value[s : s + 1, :]
        out_ref[4:6, :] = gates
        out_ref[6:7, :] = gain_ref[...].astype(F32)
        out_ref[7:8, :] = jnp.zeros((1, 128), F32)

    return pl.pallas_call(
        body,
        out_shape=[jax.ShapeDtypeStruct((8, 128), F32), jax.ShapeDtypeStruct((2, 128), F32)],
        in_specs=[SMEM] * 3 + [VMEM] * 5,
        out_specs=[VMEM] * 2,
        compiler_params=GRANT,
        name="terms",
    )(step_bias, decay_rate, new_step, new_value, new_key, new_query, new_gate, read_gain.reshape(1, 128))


def merged(meta, groups, decays, chips):
    def body(m_ref, *refs):
        g_refs, d_refs = refs[:4], refs[4:8]
        keep_out, send_out, total_out = refs[8:]
        y, c = m_ref[0], m_ref[1]
        lane = lax.broadcasted_iota(jnp.int32, (1, 128), 1)

        def turned(v):
            return jnp.where(v < 0, v + chips, jnp.where(v >= chips, v - chips, v))

        places = []
        for o in range(4):
            q = turned(y + chips // 2) if o >= 2 else y
            low = (c == 0) if o % 2 == 0 else (c != 0)
            reach = chips // 4
            first = jnp.where(low, 2 * jnp.maximum(q - reach + 1, 0), 2 * q + 1)
            second = jnp.where(low, 2 * jnp.minimum(q - reach + 1 + chips, chips), 0)
            third = jnp.where(low, 2 * turned(q - reach), 2 * turned(q + reach) + 1)
            places.append((first, second, third))
        left = jnp.zeros((1, 128), F32)
        for s in range(2):
            for g in range(4):
                after = [jnp.zeros((2, 128), F32)] * 3
                for o in range(4):
                    for k in range(3):
                        row = 2 * (g ^ o)
                        decay = d_refs[o][k, s, row : row + 2, :]
                        after = [v + jnp.where(places[o][k] > places[0][r], decay, 0.0) for r, v in enumerate(after)]
                        if g == 0:
                            for e in range(2):
                                left = left + jnp.where(lane == 2 * s + e, decay[e : e + 1, :], 0.0)
                scale = [jnp.exp(v) for v in after]
                for e in range(2):
                    part = slice(64 * e, 64 * e + 64)
                    state = sum(g_refs[g][r, s, part, :] * scale[r][e : e + 1, :] for r in range(3))
                    (keep_out if g % 2 == 0 else send_out)[g // 2, s, part, :] = state
        for k in range(3):
            part = left.astype(BF).astype(F32)
            left = left - part
            total_out[k : k + 1, :] = part
        total_out[3:, :] = jnp.zeros((5, 128), F32)

    return pl.pallas_call(
        body,
        out_shape=[jax.ShapeDtypeStruct((2, 2, 128, 128), F32)] * 2 + [jax.ShapeDtypeStruct((8, 128), F32)],
        in_specs=[SMEM] + [VMEM] * 8,
        out_specs=[VMEM] * 3,
        compiler_params=GRANT,
        name="merged",
    )(meta, *groups, *decays)


def summed(keep, got, query):
    def body(a_ref, b_ref, q_ref, own_out, far_out):
        own_out[...] = a_ref[0] + b_ref[0]
        for s in range(2):
            state = a_ref[1, s] + b_ref[1, s]
            far_out[s, :128, :] = state.astype(BF)
            read = jnp.sum(state * q_ref[s : s + 1, :], axis=1).reshape(1, 128)
            high, low = halves(read)
            far_out[s, 128:144, :] = jnp.concatenate([high, low, jnp.zeros((14, 128), BF)], axis=0)

    return pl.pallas_call(
        body,
        out_shape=[jax.ShapeDtypeStruct((2, 128, 128), F32), jax.ShapeDtypeStruct((2, 144, 128), BF)],
        in_specs=[VMEM] * 3,
        out_specs=[VMEM] * 2,
        compiler_params=GRANT,
        name="summed",
    )(keep, got, query)


def packed(own, got, query, total, sp_count):
    share = HEAD_DIM // sp_count

    def body(a_ref, b_ref, q_ref, t_ref, out_ref):
        def put(row, value):
            out_ref[:, row : row + 1, :] = jnp.broadcast_to(value[None], (sp_count, 1, 128))

        for s in range(2):
            state = a_ref[s] + b_ref[s, :128, :].astype(F32)
            far = b_ref[s, 128:144, :].astype(F32)
            read = jnp.sum(a_ref[s] * q_ref[s : s + 1, :], axis=1).reshape(1, 128)
            high, low = halves(read + far[0:1] + far[1:2])
            put(8 + s, high)
            put(10 + s, low)
            for e in range(2):
                cut = state[64 * e : 64 * e + 64, :].astype(BF).reshape(sp_count, share, 128)
                out_ref[:, 4 * s + 2 * e : 4 * s + 2 * e + share, :] = cut
        for k in range(4):
            put(12 + k, t_ref[k : k + 1, :].astype(BF))

    return pl.pallas_call(
        body,
        out_shape=jax.ShapeDtypeStruct((sp_count, 16, 128), BF),
        in_specs=[VMEM] * 4,
        out_specs=VMEM,
        compiler_params=GRANT,
        name="packed",
    )(own, got, query, total)


def finished(meta, got, fixed):
    sp_count = got.shape[0]

    def body(m_ref, got_ref, fix_ref, state_out, read_out):
        run = jnp.zeros((1, 128), F32)
        total = jnp.zeros((16, 128), F32)
        for j in reversed(range(sp_count)):
            g = got_ref[j].astype(F32)
            e = jnp.exp(run)
            one = [jnp.broadcast_to(e[:, i : i + 1], (1, 128)) for i in range(4)]
            both = [jnp.concatenate([one[2 * s][:, :64], one[2 * s + 1][:, 64:]], axis=1) for s in range(2)]
            scale = jnp.concatenate([one[i // 2] for i in range(8)] + both * 4, axis=0)
            total = total + g * scale
            run = run + g[12:13] + g[13:14] + g[14:15]
        for s in range(2):
            for h in range(2):
                state_out[s, h] = total[4 * s + 2 * h : 4 * s + 2 * h + 2].astype(BF)
        read = total[8:10] + total[10:12]
        gated = (fix_ref[0:2] * read + fix_ref[2:4]) * fix_ref[4:6]
        mean = jnp.mean(gated * gated, axis=1, keepdims=True)
        out = gated * lax.rsqrt(mean + EPSILON) * fix_ref[6:7]
        out = jnp.concatenate([out, jnp.zeros((6, 128), F32)], axis=0)
        out = pltpu.roll(out, m_ref[2], 1)
        for s in range(2):
            for h in range(2):
                read_out[s, h : h + 1, :] = out[s : s + 1, 64 * h : 64 * h + 2].astype(BF)

    return pl.pallas_call(
        body,
        out_shape=[jax.ShapeDtypeStruct((2, 2, 2, 128), BF), jax.ShapeDtypeStruct((2, 2, 2), BF)],
        in_specs=[SMEM, VMEM, VMEM],
        out_specs=[VMEM] * 2,
        compiler_params=GRANT,
        name="finished",
    )(meta, got, fixed)


def per_device(
    hidden_in, w_value, w_key, w_step, conv_value, conv_key, step_bias, decay_rate, decay_jump,
    new_value, new_key, new_query, new_gate, new_step, read_gain,
):
    sp_count, y_count, c_count = (lax.axis_size(a) for a in ("sp", "y", "c"))
    sp, y, c = (lax.axis_index(a) for a in ("sp", "y", "c"))
    tp_count = y_count * c_count
    count = sp_count * tp_count
    rows, width = hidden_in.shape[1:]
    heads = step_bias.shape[0]
    share = HEAD_DIM // sp_count
    half, reach = y_count // 2, y_count // 4

    def swap(v):
        return lax.ppermute(v, "c", [(0, 1), (1, 0)])

    def onward(v):
        pairs = []
        for i in range(y_count):
            pairs.append((2 * i, 2 * ((i + 1) % y_count)))
            pairs.append((2 * i + 1, 2 * ((i - 1) % y_count) + 1))
        return lax.ppermute(v, ("y", "c"), pairs)

    def across(v):
        return lax.ppermute(v, "y", [(i, (i + half) % y_count) for i in range(y_count)])

    meta = jnp.stack([y, c, (128 - sp * share) % 128, sp]).astype(jnp.int32)

    w_own, w_part = joined(meta, w_value, w_key, sp_count)
    w_part = jnp.broadcast_to(across(w_part)[None], (sp_count, *w_part.shape))
    w_far = lax.all_to_all(w_part, "sp", 0, 0, tiled=True).reshape(w_own.shape)
    w_near = w_own, swap(w_own)
    w_far = w_far, swap(w_far)

    ends = hidden_in[:, rows - 4 :, :].reshape(8, width)
    ends = lax.ppermute(ends, ("sp", "y", "c"), [(i, i + 1) for i in range(count - 1)])
    a = [jnp.concatenate([hidden_in.reshape(2 * rows, width), ends], axis=0)]
    a.append(onward(a[0]))
    b = [swap(a[0])]
    b.append(onward(b[0]))

    def ordered(v):
        return jnp.where(c == 0, v, jnp.roll(v, heads, axis=0))

    steps = w_step.T
    pairs = (lax.dynamic_slice_in_dim(steps, v * 2 * heads, 2 * heads, 0) for v in (y, (y + half) % y_count))
    w_steps = jnp.concatenate([ordered(v) for v in pairs], axis=0)
    rates = jnp.broadcast_to(jnp.stack([step_bias, decay_rate])[:, :, None], (2, heads, 128))
    taps = jnp.concatenate([conv_value, conv_key], axis=1).astype(F32).reshape(2, heads, 256)
    asked = new_query.astype(F32).reshape(2, heads, HEAD_DIM)
    small = jnp.concatenate([decay_jump.transpose(0, 2, 1), rates, taps, asked], axis=2)
    small = jnp.concatenate([small, swap(small)], axis=1)
    small = jnp.concatenate([small, across(small)], axis=1)
    length = tp_count * rows
    rates, taps = small[:, :, length : length + 128], small[:, :, length + 128 : length + 384]
    asked = small[:, 4 : 4 + heads, length + 384 :].reshape(2, heads * HEAD_DIM)
    taps = taps.reshape(2, 4, 2, 256).transpose(0, 2, 1, 3).reshape(4, 1024)
    jump = small[:, :, :length].reshape(2, 8, tp_count, rows).transpose(2, 1, 0, 3)
    jump = jump.reshape(tp_count, 8, 2 * rows)

    for k in range(1, reach):
        if k + 1 < reach:
            b.append(onward(b[k]))
        a.append(onward(a[k]))

    def add(runs, k, w, base):
        ends = k == 0 or k == reach
        xs = [a[k]] if ends else [a[k], b[k]]
        part = taps[:, 128 * base : 128 * base + 512]
        return piece_states(meta, xs, k, k == reach, w_steps, w, part, jump, rates, runs, base, rows, y_count)

    near = None
    for k in range(reach + 1):
        near = add(near, k, w_near, 0)
    decays = near[0][:, :, 128:, :]
    decays = [decays, swap(decays)]
    apart = across(jnp.concatenate(decays, axis=0))
    decays += [apart[:3], apart[3:]]

    fixed, query = terms(step_bias, decay_rate, new_step, new_value, new_key, new_query, new_gate, read_gain)
    near, decays, fixed, query, asked = lax.optimization_barrier((near, decays, fixed, query, asked))
    away = None
    for k in range(reach + 1):
        away = add(away, k, w_far, 4)
    keep, send, total = merged(meta, [*near, *away], decays, y_count)
    own, apart = summed(keep, swap(send), asked)
    sent = packed(own, across(apart), query, total, sp_count)
    got = lax.all_to_all(sent, "sp", 0, 0, tiled=True)
    return tuple(finished(meta, got, fixed))


def solution(mesh):
    tp = ("y", "c")
    chips = Mesh(mesh.devices.reshape(mesh.shape["sp"], mesh.shape["tp"] // 2, 2), ("sp", *tp))

    return jax.shard_map(
        per_device,
        mesh=chips,
        in_specs=(
            P(None, ("sp", *tp), None), P(None, tp), P(None, tp), P(), P(None, tp), P(None, tp), P(tp), P(tp),
            P(None, "sp", tp), P(None, tp), P(None, tp), P(None, tp), P(None, tp), P(None, tp), P(tp),
        ),
        out_specs=(P(None, tp, "sp", None), P(None, tp, "sp")),
        check_vma=False,
    )
```

```python
import jax
import jax.numpy as jnp
from jax import lax
from jax.experimental import pallas as pl
from jax.experimental.pallas import tpu as pltpu
from jax.sharding import Mesh
from jax.sharding import PartitionSpec as P

HEAD_DIM = 64
EPSILON = 1e-05
BF = jnp.bfloat16
F32 = jnp.float32
GRANT = pltpu.CompilerParams(vmem_limit_bytes=16 * 1024 * 1024)
VMEM = pl.BlockSpec(memory_space=pltpu.VMEM)
SMEM = pl.BlockSpec(memory_space=pltpu.SMEM)


def mm(a, b, dims, precision=None):
    return lax.dot_general(a, b, (dims, ((), ())), preferred_element_type=F32, precision=precision)


def halves(v):
    high = v.astype(BF)
    return high, (v - high.astype(F32)).astype(BF)


def product(a, b):
    (ah, al), (bh, bl) = halves(a), halves(b)
    dims = ((0,), (0,))
    return mm(ah, bh, dims) + (mm(al, bh, dims) + mm(ah, bl, dims))


def softplus(v):
    return jnp.maximum(v, 0.0) + jnp.log1p(jnp.exp(-jnp.abs(v)))


def piece_states(meta, xs, far, end, w_step, w, jump, rates, runs, rows, chips):
    depth = w[0].shape[0] - 4
    many, both = len(xs), 2 * rows
    given = [] if runs is None else list(runs)

    def body(m_ref, *refs):
        x_refs = refs[:many]
        s_ref, wa_ref, wb_ref, j_ref, r_ref = refs[many : many + 5]
        ins = refs[many + 5 : many + 5 + len(given)]
        own_out, other_out, ext = refs[many + 5 + len(given) :]
        outs = (own_out, other_out)
        y, c = m_ref[0], m_ref[1]
        low = c == 0
        away = jnp.where(low, y - far, y + far)
        wrapped = jnp.logical_or(away < 0, away >= chips)
        chip = jnp.where(away < 0, away + chips, jnp.where(away >= chips, away - chips, away))
        run = 2 if end else jnp.where(wrapped, 1, 0)
        place = (2 * chip + c, 2 * chip + 1 - c)
        for g in range(2):
            if given:
                outs[g][...] = ins[g][...]
            else:
                outs[g][...] = jnp.zeros(outs[g].shape, F32)

        lane = lax.broadcasted_iota(jnp.int32, (8, both), 1)
        i = lax.broadcasted_iota(jnp.int32, (both, both), 0)
        j = lax.broadcasted_iota(jnp.int32, (both, both), 1)
        below = jnp.where(jnp.logical_and(i > j, (i >= rows) == (j >= rows)), 1.0, 0.0)
        sizes, afters, sums = [], [], []
        for n in range(many):
            step = mm(s_ref[...], x_refs[n][...], ((1,), (1,))).astype(BF).astype(F32)[:, :both]
            size = softplus(step + r_ref[0][:, 0:1])
            decay = j_ref[place[n]] - r_ref[1][:, 0:1] * size
            sizes.append(size)
            afters.append(mm(decay, below, ((1,), (0,)), lax.Precision.HIGHEST))
            sums.append([
                jnp.sum(jnp.where(lane < rows, decay, 0.0), axis=1, keepdims=True),
                jnp.sum(jnp.where(lane < rows, 0.0, decay), axis=1, keepdims=True),
            ])
        total = [sum(v[s] for v in sums) for s in range(2)]
        before = [own_out[run, s, 128:136, :] for s in range(2)]
        lead = [jnp.where(low, v[:, 0:1], 0.0) for v in before]
        lifts = []
        for n in range(many):
            more = list(lead)
            if many == 2:
                first = low if n == 0 else jnp.logical_not(low)
                more = [more[s] + jnp.where(first, sums[1 - n][s], 0.0) for s in range(2)]
            weight = sizes[n] * jnp.exp(afters[n] + jnp.where(lane < rows, more[0], more[1]))
            weight = jnp.concatenate([weight, jnp.zeros((8, 256 - both), F32)], axis=1)
            lifts.append(jnp.transpose(weight))

        taps = jnp.concatenate([r[depth : depth + 4, :] for r in (wa_ref, wb_ref)], axis=1).astype(F32)
        for n in range(many):
            x = x_refs[n][...]
            for g, r in enumerate((wa_ref, wb_ref)):
                p = mm(x, r[:depth, :], ((1,), (0,))).astype(BF).astype(F32)
                for s in range(2):
                    ext[2 * n + s, 4:8, 256 * g : 256 * g + 256] = p[both + 4 * s : both + 4 * s + 4, :]
                    ext[2 * n + s, 8 : 8 + rows, 256 * g : 256 * g + 256] = p[s * rows : (s + 1) * rows, :]
        for s in range(2):
            states = [jnp.zeros((128, 128), F32)] * 2
            for n in range(many):
                mixed = ext[2 * n + s, 5 : 5 + rows, :] * taps[0:1, :]
                for k in range(1, 4):
                    mixed = mixed + ext[2 * n + s, 5 + k : 5 + k + rows, :] * taps[k : k + 1, :]
                mixed = mixed / (1.0 + jnp.exp(-mixed))
                lift = lifts[n][s * rows : (s + 1) * rows, :]
                for g in range(2):
                    parts = [
                        mixed[:, 256 * g + 64 * e : 256 * g + 64 * e + 64] * lift[:, 2 * g + e : 2 * g + e + 1]
                        for e in range(2)
                    ]
                    values = jnp.concatenate(parts, axis=1)
                    keys = mixed[:, 256 * g + 128 : 256 * g + 256]
                    states[g] = states[g] + product(values, keys)
            fade = jnp.where(low, 1.0, jnp.exp(total[s]))
            for g in range(2):
                for e in range(2):
                    part = slice(64 * e, 64 * e + 64)
                    old = outs[g][run, s, part, :]
                    outs[g][run, s, part, :] = old * fade[2 * g + e : 2 * g + e + 1, :] + states[g][part, :]
                outs[g][run, s, 128:136, :] = before[s] + total[s]

    shape = (3, 2, 136, 128)
    return pl.pallas_call(
        body,
        out_shape=[jax.ShapeDtypeStruct(shape, F32)] * 2,
        in_specs=[SMEM] + [VMEM] * (many + 5 + len(given)),
        out_specs=[VMEM] * 2,
        scratch_shapes=[pltpu.VMEM((2 * many, rows + 8, 512), F32)],
        cost_estimate=pl.CostEstimate(
            flops=32 * sum(x.shape[0] for x in xs) * w[0].size,
            transcendentals=0,
            bytes_accessed=4 * w[0].size,
        ),
        compiler_params=GRANT,
        name="piece_states",
    )(meta, *xs, w_step, *w, jump, rates, *given)


def joined(w_value, w_key, conv_value, conv_key):
    depth = w_value.shape[0]

    def body(v_ref, k_ref, cv_ref, ck_ref, out_ref):
        out_ref[:depth, :128] = v_ref[...]
        out_ref[:depth, 128:] = k_ref[...]
        out_ref[depth:, :128] = cv_ref[...]
        out_ref[depth:, 128:] = ck_ref[...]

    return pl.pallas_call(
        body,
        out_shape=jax.ShapeDtypeStruct((depth + conv_value.shape[0], 256), BF),
        in_specs=[VMEM] * 4,
        out_specs=VMEM,
        compiler_params=GRANT,
        name="joined",
    )(w_value, w_key, conv_value, conv_key)


def terms(step_bias, decay_rate, new_step, new_value, new_key, new_query, new_gate, read_gain):
    def body(b_ref, r_ref, n_ref, v_ref, k_ref, q_ref, g_ref, gain_ref, out_ref, query_ref):
        lane = lax.broadcasted_iota(jnp.int32, (1, 128), 1)

        def spread(a, b):
            return jnp.where(lane < HEAD_DIM, a, b)

        query = q_ref[...].astype(F32)
        query_ref[...] = query
        value, key, gate = (r[...].astype(F32) for r in (v_ref, k_ref, g_ref))
        match = jnp.sum(key * query, axis=1, keepdims=True)
        gates = gate / (1.0 + jnp.exp(-gate))
        rate = spread(r_ref[0], r_ref[1])
        for s in range(2):
            size = softplus(spread(n_ref[s, 0] + b_ref[0], n_ref[s, 1] + b_ref[1]))
            out_ref[s : s + 1, :] = jnp.exp(-rate * size)
            out_ref[2 + s : 3 + s, :] = size * match[s : s + 1, :] * value[s : s + 1, :]
        out_ref[4:6, :] = gates
        out_ref[6:7, :] = gain_ref[...].astype(F32)
        out_ref[7:8, :] = jnp.zeros((1, 128), F32)

    return pl.pallas_call(
        body,
        out_shape=[jax.ShapeDtypeStruct((8, 128), F32), jax.ShapeDtypeStruct((2, 128), F32)],
        in_specs=[SMEM] * 3 + [VMEM] * 5,
        out_specs=[VMEM] * 2,
        compiler_params=GRANT,
        name="terms",
    )(step_bias, decay_rate, new_step, new_value, new_key, new_query, new_gate, read_gain.reshape(1, 128))


def packed(meta, own, got, query, sp_count, chips):
    share = HEAD_DIM // sp_count

    def body(m_ref, a_ref, b_ref, q_ref, out_ref):
        def put(row, value):
            out_ref[:, row : row + 1, :] = jnp.broadcast_to(value[None], (sp_count, 1, 128))

        low = m_ref[1] == 0
        late = m_ref[0] < chips // 2
        lane = lax.broadcasted_iota(jnp.int32, (1, 128), 1)
        left = jnp.zeros((1, 128), F32)
        for s in range(2):
            mine = [a_ref[r, s, 128:130, :] for r in range(3)]
            theirs = [b_ref[r, s, 130:132, :] for r in range(3)]
            d1, d2, d3 = (jnp.where(low, m, t) for m, t in zip(mine, theirs))
            u1, u2, u3 = (jnp.where(low, t, m) for m, t in zip(mine, theirs))
            last = d3 + u3
            after_u1 = d2 + jnp.where(late, last, 0.0)
            after_d1 = after_u1 + u1
            after_u3 = jnp.where(late, d2, after_d1 + d1)
            after_d3 = after_u3 + u3
            after_u2 = after_d1 + d1 + jnp.where(late, 0.0, last)
            total = after_u2 + u2
            for e in range(2):
                left = jnp.where(lane == 2 * s + e, total[e : e + 1, :], left)
            down = [jnp.exp(v) for v in (after_d1, jnp.zeros_like(d2), after_d3)]
            up = [jnp.exp(v) for v in (after_u1, after_u2, after_u3)]
            reads = []
            for e in range(2):
                state = jnp.zeros((64, 128), F32)
                for r in range(3):
                    part = slice(64 * e, 64 * e + 64)
                    scale_a = jnp.where(low, down[r], up[r])[e : e + 1, :]
                    scale_b = jnp.where(low, up[r], down[r])[e : e + 1, :]
                    state = state + a_ref[r, s, part, :] * scale_a + b_ref[r, s, part, :] * scale_b
                reads.append(jnp.sum(state * q_ref[s : s + 1, :], axis=1).reshape(1, 64))
                cut = state.astype(BF).reshape(sp_count, share, 128)
                out_ref[:, 4 * s + 2 * e : 4 * s + 2 * e + share, :] = cut
            read = jnp.concatenate(reads, axis=1)
            high, low_part = halves(read)
            put(8 + s, high)
            put(10 + s, low_part)
        for k in range(3):
            part = left.astype(BF)
            left = left - part.astype(F32)
            put(12 + k, part)
        put(15, jnp.zeros((1, 128), BF))

    return pl.pallas_call(
        body,
        out_shape=jax.ShapeDtypeStruct((sp_count, 16, 128), BF),
        in_specs=[SMEM] + [VMEM] * 3,
        out_specs=VMEM,
        compiler_params=GRANT,
        name="packed",
    )(meta, own, got, query)


def finished(meta, got, fixed):
    sp_count = got.shape[0]

    def body(m_ref, got_ref, fix_ref, state_out, read_out):
        blocks = [got_ref[j].astype(F32) for j in range(sp_count)]
        decay = jnp.concatenate([g[12:13] + g[13:14] + g[14:15] for g in blocks], axis=0)
        i = lax.broadcasted_iota(jnp.int32, (sp_count, sp_count), 0)
        j = lax.broadcasted_iota(jnp.int32, (sp_count, sp_count), 1)
        after = jnp.where(j > i, 1.0, 0.0)
        fade = jnp.exp(mm(after, decay, ((1,), (0,)), lax.Precision.HIGHEST))
        one = [jnp.broadcast_to(fade[:, i : i + 1], (sp_count, 128)) for i in range(4)]
        lane = lax.broadcasted_iota(jnp.int32, (sp_count, 128), 1)
        both = [jnp.where(lane < HEAD_DIM, one[2 * s], one[2 * s + 1]) for s in range(2)]
        row = lax.broadcasted_iota(jnp.int32, (8, 128), 0)
        total = [jnp.zeros((8, 128), F32)] * 2
        for j, g in enumerate(blocks):
            a, b, c, d = (v[j : j + 1] for v in one)
            scale = jnp.where(row < 4, jnp.where(row < 2, a, b), jnp.where(row < 6, c, d))
            total[0] = total[0] + g[:8] * scale
            total[1] = total[1] + g[8:] * jnp.where(row % 2 == 0, both[0][j : j + 1], both[1][j : j + 1])
        total = jnp.concatenate(total, axis=0)
        for s in range(2):
            for h in range(2):
                state_out[s, h] = total[4 * s + 2 * h : 4 * s + 2 * h + 2].astype(BF)
        read = total[8:10] + total[10:12]
        gated = (fix_ref[0:2] * read + fix_ref[2:4]) * fix_ref[4:6]
        mean = jnp.mean(gated * gated, axis=1, keepdims=True)
        out = gated * lax.rsqrt(mean + EPSILON) * fix_ref[6:7]
        out = jnp.concatenate([out, jnp.zeros((6, 128), F32)], axis=0)
        out = pltpu.roll(out, m_ref[2], 1)
        for s in range(2):
            for h in range(2):
                read_out[s, h : h + 1, :] = out[s : s + 1, 64 * h : 64 * h + 2].astype(BF)

    return pl.pallas_call(
        body,
        out_shape=[jax.ShapeDtypeStruct((2, 2, 2, 128), BF), jax.ShapeDtypeStruct((2, 2, 2), BF)],
        in_specs=[SMEM, VMEM, VMEM],
        out_specs=[VMEM] * 2,
        compiler_params=GRANT,
        name="finished",
    )(meta, got, fixed)


def per_device(
    hidden_in, w_value, w_key, w_step, conv_value, conv_key, step_bias, decay_rate, decay_jump,
    new_value, new_key, new_query, new_gate, new_step, read_gain,
):
    sp_count, y_count, c_count = (lax.axis_size(a) for a in ("sp", "y", "c"))
    sp, y, c = (lax.axis_index(a) for a in ("sp", "y", "c"))
    tp_count = y_count * c_count
    count = sp_count * tp_count
    rows, width = hidden_in.shape[1:]
    heads = step_bias.shape[0]
    share = HEAD_DIM // sp_count
    half = y_count // 2

    def swap(v):
        return lax.ppermute(v, "c", [(0, 1), (1, 0)])

    def onward(v):
        pairs = []
        for i in range(y_count):
            pairs.append((2 * i, 2 * ((i + 1) % y_count)))
            pairs.append((2 * i + 1, 2 * ((i - 1) % y_count) + 1))
        return lax.ppermute(v, ("y", "c"), pairs)

    meta = jnp.stack([y, c, (128 - sp * share) % 128]).astype(jnp.int32)

    x = hidden_in.reshape(2 * rows, width)
    bare = onward(x)
    ends = hidden_in[:, rows - 4 :, :].reshape(8, width)
    ends = lax.ppermute(ends, ("sp", "y", "c"), [(i, i + 1) for i in range(count - 1)])
    a = [jnp.concatenate([x, ends], axis=0)]
    b = [swap(a[0])]
    b.append(onward(b[0]))
    pairs = []
    for i in range(y_count):
        pairs.append((2 * i + 1, 2 * ((i + 1) % y_count)))
        pairs.append((2 * i, 2 * ((i - 1) % y_count) + 1))
    near = lax.ppermute(b[0][2 * rows :], ("y", "c"), pairs)
    a.append(jnp.concatenate([bare, near], axis=0))

    w_own = joined(w_value, w_key, conv_value, conv_key)
    w_both = w_own, swap(w_own)
    pair = lax.dynamic_slice_in_dim(w_step.T, y * 2 * heads, 2 * heads, 0)
    pair = jnp.where(c == 0, pair, jnp.roll(pair, heads, axis=0))
    w_steps = jnp.pad(pair, ((0, 8 - 2 * heads), (0, 0)))
    rates = jnp.broadcast_to(jnp.stack([step_bias, decay_rate])[:, :, None], (2, heads, 128))
    jump = jnp.concatenate([decay_jump.transpose(0, 2, 1), rates], axis=2)
    jump = jnp.concatenate([jump, swap(jump)], axis=1)
    jump = jnp.pad(jump, ((0, 0), (0, 8 - 2 * heads), (0, 0)))
    rates = jump[:, :, tp_count * rows :]
    jump = jump[:, :, : tp_count * rows].reshape(2, 8, tp_count, rows).transpose(2, 1, 0, 3)
    jump = jump.reshape(tp_count, 8, 2 * rows)

    def add(runs, xs, far, end):
        return piece_states(meta, xs, far, end, w_steps, w_both, jump, rates, runs, rows, y_count)

    runs = add(None, [a[0]], 0, False)
    for s in range(1, half):
        a.append(onward(a[s]))
        if s + 1 < half:
            b.append(onward(b[s]))
        runs = add(runs, [a[s], b[s]], s, False)

    fixed, query = terms(step_bias, decay_rate, new_step, new_value, new_key, new_query, new_gate, read_gain)
    runs, fixed, query = lax.optimization_barrier((runs, fixed, query))
    own, other = add(runs, [a[half]], half, True)
    sent = packed(meta, own, swap(other), query, sp_count, y_count)
    got = lax.all_to_all(sent, "sp", 0, 0, tiled=True)
    return tuple(finished(meta, got, fixed))


def solution(mesh):
    tp = ("y", "c")
    chips = Mesh(mesh.devices.reshape(mesh.shape["sp"], mesh.shape["tp"] // 2, 2), ("sp", *tp))

    return jax.shard_map(
        per_device,
        mesh=chips,
        in_specs=(
            P(None, ("sp", *tp), None), P(None, tp), P(None, tp), P(), P(None, tp), P(None, tp), P(tp), P(tp),
            P(None, "sp", tp), P(None, tp), P(None, tp), P(None, tp), P(None, tp), P(None, tp), P(tp),
        ),
        out_specs=(P(None, tp, "sp", None), P(None, tp, "sp")),
        check_vma=False,
    )
```

```python
import jax
import jax.numpy as jnp
from jax import lax
from jax.experimental import pallas as pl
from jax.experimental.pallas import tpu as pltpu
from jax.sharding import Mesh
from jax.sharding import PartitionSpec as P

HEAD_DIM = 64
EPSILON = 1e-05
BF = jnp.bfloat16
F32 = jnp.float32
GRANT = pltpu.CompilerParams(vmem_limit_bytes=16 * 1024 * 1024)
VMEM = pl.BlockSpec(memory_space=pltpu.VMEM)
SMEM = pl.BlockSpec(memory_space=pltpu.SMEM)


def mm(a, b, dims, precision=None):
    return lax.dot_general(a, b, (dims, ((), ())), preferred_element_type=F32, precision=precision)


def halves(v):
    high = v.astype(BF)
    return high, (v - high.astype(F32)).astype(BF)


def product(a, b):
    (ah, al), (bh, bl) = halves(a), halves(b)
    dims = ((0,), (0,))
    return mm(ah, bh, dims) + (mm(al, bh, dims) + mm(ah, bl, dims))


def softplus(v):
    return jnp.maximum(v, 0.0) + jnp.log1p(jnp.exp(-jnp.abs(v)))


def piece_states(meta, xs, halo, far, end, w_step, w, jump, rates, runs, rows, chips):
    depth = w[0].shape[0] - 4
    many, both = len(xs), 2 * rows
    given = [] if runs is None else list(runs)

    def body(m_ref, *refs):
        x_refs = refs[:many]
        h_ref, s_ref, wa_ref, wb_ref, j_ref, r_ref = refs[many : many + 6]
        ins = refs[many + 6 : many + 6 + len(given)]
        own_out, other_out, ext, full = refs[many + 6 + len(given) :]
        outs = (own_out, other_out)
        y, c = m_ref[0], m_ref[1]
        low = c == 0
        away = jnp.where(low, y - far, y + far)
        wrapped = jnp.logical_or(away < 0, away >= chips)
        chip = jnp.where(away < 0, away + chips, jnp.where(away >= chips, away - chips, away))
        run = 2 if end else jnp.where(wrapped, 1, 0)
        place = (2 * chip + c, 2 * chip + 1 - c)
        for g in range(2):
            if given:
                outs[g][...] = ins[g][...]
            else:
                outs[g][...] = jnp.zeros(outs[g].shape, F32)

        lane = lax.broadcasted_iota(jnp.int32, (8, both), 1)
        i = lax.broadcasted_iota(jnp.int32, (both, both), 0)
        j = lax.broadcasted_iota(jnp.int32, (both, both), 1)
        below = jnp.where(jnp.logical_and(i > j, (i >= rows) == (j >= rows)), 1.0, 0.0)
        sizes, afters, sums = [], [], []
        for n in range(many):
            step = mm(s_ref[...], x_refs[n][...], ((1,), (1,))).astype(BF).astype(F32)
            size = softplus(step + r_ref[0][:, 0:1])
            decay = j_ref[place[n]] - r_ref[1][:, 0:1] * size
            sizes.append(size)
            afters.append(mm(decay, below, ((1,), (0,)), lax.Precision.HIGHEST))
            sums.append([
                jnp.sum(jnp.where(lane < rows, decay, 0.0), axis=1, keepdims=True),
                jnp.sum(jnp.where(lane < rows, 0.0, decay), axis=1, keepdims=True),
            ])
        total = [sum(v[s] for v in sums) for s in range(2)]
        before = [own_out[run, s, 128:136, :] for s in range(2)]
        lead = [jnp.where(low, v[:, 0:1], 0.0) for v in before]
        lifts = []
        for n in range(many):
            more = list(lead)
            if many == 2:
                first = low if n == 0 else jnp.logical_not(low)
                more = [more[s] + jnp.where(first, sums[1 - n][s], 0.0) for s in range(2)]
            weight = sizes[n] * jnp.exp(afters[n] + jnp.where(lane < rows, more[0], more[1]))
            weight = jnp.concatenate([weight, jnp.zeros((8, 256 - both), F32)], axis=1)
            lifts.append(jnp.transpose(weight))

        taps = jnp.concatenate([r[depth : depth + 4, :] for r in (wa_ref, wb_ref)], axis=1).astype(F32)
        full[:both, :] = x_refs[0][...]
        full[both:, :] = h_ref[...]
        for g, r in enumerate((wa_ref, wb_ref)):
            cols = slice(256 * g, 256 * g + 256)
            p = [
                mm((full if n == 0 else x_refs[n])[...], r[:depth, :], ((1,), (0,))).astype(BF).astype(F32)
                for n in range(many)
            ]
            for s in range(2):
                before_row = [p[0][both + 4 * s : both + 4 * s + 4, :]]
                if many == 2:
                    last = [v[(s + 1) * rows - 4 : (s + 1) * rows, :] for v in p]
                    outer = before_row[0]
                    before_row = [jnp.where(low, outer, last[1]), jnp.where(low, last[0], outer)]
                for n in range(many):
                    ext[2 * n + s, 4:8, cols] = before_row[n]
                    ext[2 * n + s, 8 : 8 + rows, cols] = p[n][s * rows : (s + 1) * rows, :]
        for s in range(2):
            states = [jnp.zeros((128, 128), F32)] * 2
            for n in range(many):
                mixed = ext[2 * n + s, 5 : 5 + rows, :] * taps[0:1, :]
                for k in range(1, 4):
                    mixed = mixed + ext[2 * n + s, 5 + k : 5 + k + rows, :] * taps[k : k + 1, :]
                mixed = mixed / (1.0 + jnp.exp(-mixed))
                lift = lifts[n][s * rows : (s + 1) * rows, :]
                for g in range(2):
                    parts = [
                        mixed[:, 256 * g + 64 * e : 256 * g + 64 * e + 64] * lift[:, 2 * g + e : 2 * g + e + 1]
                        for e in range(2)
                    ]
                    values = jnp.concatenate(parts, axis=1)
                    keys = mixed[:, 256 * g + 128 : 256 * g + 256]
                    states[g] = states[g] + product(values, keys)
            fade = jnp.where(low, 1.0, jnp.exp(total[s]))
            for g in range(2):
                for e in range(2):
                    part = slice(64 * e, 64 * e + 64)
                    old = outs[g][run, s, part, :]
                    outs[g][run, s, part, :] = old * fade[2 * g + e : 2 * g + e + 1, :] + states[g][part, :]
                outs[g][run, s, 128:136, :] = before[s] + total[s]

    shape = (3, 2, 136, 128)
    return pl.pallas_call(
        body,
        out_shape=[jax.ShapeDtypeStruct(shape, F32)] * 2,
        in_specs=[SMEM] + [VMEM] * (many + 6 + len(given)),
        out_specs=[VMEM] * 2,
        scratch_shapes=[pltpu.VMEM((2 * many, rows + 8, 512), F32), pltpu.VMEM((both + 8, depth), BF)],
        cost_estimate=pl.CostEstimate(
            flops=32 * sum(x.shape[0] for x in xs) * w[0].size,
            transcendentals=0,
            bytes_accessed=4 * w[0].size,
        ),
        compiler_params=GRANT,
        name="piece_states",
    )(meta, *xs, halo, w_step, *w, jump, rates, *given)


def joined(w_value, w_key, conv_value, conv_key):
    depth = w_value.shape[0]

    def body(v_ref, k_ref, cv_ref, ck_ref, out_ref):
        out_ref[:depth, :128] = v_ref[...]
        out_ref[:depth, 128:] = k_ref[...]
        out_ref[depth:, :128] = cv_ref[...]
        out_ref[depth:, 128:] = ck_ref[...]

    return pl.pallas_call(
        body,
        out_shape=jax.ShapeDtypeStruct((depth + conv_value.shape[0], 256), BF),
        in_specs=[VMEM] * 4,
        out_specs=VMEM,
        compiler_params=GRANT,
        name="joined",
    )(w_value, w_key, conv_value, conv_key)


def terms(step_bias, decay_rate, new_step, new_value, new_key, new_query, new_gate, read_gain):
    def body(b_ref, r_ref, n_ref, v_ref, k_ref, q_ref, g_ref, gain_ref, out_ref, query_ref):
        lane = lax.broadcasted_iota(jnp.int32, (1, 128), 1)

        def spread(a, b):
            return jnp.where(lane < HEAD_DIM, a, b)

        query = q_ref[...].astype(F32)
        query_ref[...] = query
        value, key, gate = (r[...].astype(F32) for r in (v_ref, k_ref, g_ref))
        match = jnp.sum(key * query, axis=1, keepdims=True)
        gates = gate / (1.0 + jnp.exp(-gate))
        rate = spread(r_ref[0], r_ref[1])
        for s in range(2):
            size = softplus(spread(n_ref[s, 0] + b_ref[0], n_ref[s, 1] + b_ref[1]))
            out_ref[s : s + 1, :] = jnp.exp(-rate * size)
            out_ref[2 + s : 3 + s, :] = size * match[s : s + 1, :] * value[s : s + 1, :]
        out_ref[4:6, :] = gates
        out_ref[6:7, :] = gain_ref[...].astype(F32)
        out_ref[7:8, :] = jnp.zeros((1, 128), F32)

    return pl.pallas_call(
        body,
        out_shape=[jax.ShapeDtypeStruct((8, 128), F32), jax.ShapeDtypeStruct((2, 128), F32)],
        in_specs=[SMEM] * 3 + [VMEM] * 5,
        out_specs=[VMEM] * 2,
        compiler_params=GRANT,
        name="terms",
    )(step_bias, decay_rate, new_step, new_value, new_key, new_query, new_gate, read_gain.reshape(1, 128))


def packed(meta, own, got, query, sp_count, chips):
    share = HEAD_DIM // sp_count

    def body(m_ref, a_ref, b_ref, q_ref, out_ref):
        def put(row, value):
            out_ref[:, row : row + 1, :] = jnp.broadcast_to(value[None], (sp_count, 1, 128))

        low = m_ref[1] == 0
        late = m_ref[0] < chips // 2
        lane = lax.broadcasted_iota(jnp.int32, (1, 128), 1)
        left = jnp.zeros((1, 128), F32)
        for s in range(2):
            mine = [a_ref[r, s, 128:130, :] for r in range(3)]
            theirs = [b_ref[r, s, 130:132, :] for r in range(3)]
            d1, d2, d3 = (jnp.where(low, m, t) for m, t in zip(mine, theirs))
            u1, u2, u3 = (jnp.where(low, t, m) for m, t in zip(mine, theirs))
            last = d3 + u3
            after_u1 = d2 + jnp.where(late, last, 0.0)
            after_d1 = after_u1 + u1
            after_u3 = jnp.where(late, d2, after_d1 + d1)
            after_d3 = after_u3 + u3
            after_u2 = after_d1 + d1 + jnp.where(late, 0.0, last)
            total = after_u2 + u2
            for e in range(2):
                left = jnp.where(lane == 2 * s + e, total[e : e + 1, :], left)
            down = [jnp.exp(v) for v in (after_d1, jnp.zeros_like(d2), after_d3)]
            up = [jnp.exp(v) for v in (after_u1, after_u2, after_u3)]
            reads = []
            for e in range(2):
                state = jnp.zeros((64, 128), F32)
                for r in range(3):
                    part = slice(64 * e, 64 * e + 64)
                    scale_a = jnp.where(low, down[r], up[r])[e : e + 1, :]
                    scale_b = jnp.where(low, up[r], down[r])[e : e + 1, :]
                    state = state + a_ref[r, s, part, :] * scale_a + b_ref[r, s, part, :] * scale_b
                reads.append(jnp.sum(state * q_ref[s : s + 1, :], axis=1).reshape(1, 64))
                cut = state.astype(BF).reshape(sp_count, share, 128)
                out_ref[:, 4 * s + 2 * e : 4 * s + 2 * e + share, :] = cut
            read = jnp.concatenate(reads, axis=1)
            high, low_part = halves(read)
            put(8 + s, high)
            put(10 + s, low_part)
        for k in range(3):
            part = left.astype(BF)
            left = left - part.astype(F32)
            put(12 + k, part)
        put(15, jnp.zeros((1, 128), BF))

    return pl.pallas_call(
        body,
        out_shape=jax.ShapeDtypeStruct((sp_count, 16, 128), BF),
        in_specs=[SMEM] + [VMEM] * 3,
        out_specs=VMEM,
        compiler_params=GRANT,
        name="packed",
    )(meta, own, got, query)


def finished(meta, got, fixed):
    sp_count = got.shape[0]

    def body(m_ref, got_ref, fix_ref, state_out, read_out):
        blocks = [got_ref[j].astype(F32) for j in range(sp_count)]
        decay = jnp.concatenate([g[12:13] + g[13:14] + g[14:15] for g in blocks], axis=0)
        i = lax.broadcasted_iota(jnp.int32, (sp_count, sp_count), 0)
        j = lax.broadcasted_iota(jnp.int32, (sp_count, sp_count), 1)
        after = jnp.where(j > i, 1.0, 0.0)
        fade = jnp.exp(mm(after, decay, ((1,), (0,)), lax.Precision.HIGHEST))
        one = [jnp.broadcast_to(fade[:, i : i + 1], (sp_count, 128)) for i in range(4)]
        lane = lax.broadcasted_iota(jnp.int32, (sp_count, 128), 1)
        both = [jnp.where(lane < HEAD_DIM, one[2 * s], one[2 * s + 1]) for s in range(2)]
        row = lax.broadcasted_iota(jnp.int32, (8, 128), 0)
        total = [jnp.zeros((8, 128), F32)] * 2
        for j, g in enumerate(blocks):
            a, b, c, d = (v[j : j + 1] for v in one)
            scale = jnp.where(row < 4, jnp.where(row < 2, a, b), jnp.where(row < 6, c, d))
            total[0] = total[0] + g[:8] * scale
            total[1] = total[1] + g[8:] * jnp.where(row % 2 == 0, both[0][j : j + 1], both[1][j : j + 1])
        total = jnp.concatenate(total, axis=0)
        for s in range(2):
            for h in range(2):
                state_out[s, h] = total[4 * s + 2 * h : 4 * s + 2 * h + 2].astype(BF)
        read = total[8:10] + total[10:12]
        gated = (fix_ref[0:2] * read + fix_ref[2:4]) * fix_ref[4:6]
        mean = jnp.mean(gated * gated, axis=1, keepdims=True)
        out = gated * lax.rsqrt(mean + EPSILON) * fix_ref[6:7]
        out = jnp.concatenate([out, jnp.zeros((6, 128), F32)], axis=0)
        out = pltpu.roll(out, m_ref[2], 1)
        for s in range(2):
            for h in range(2):
                read_out[s, h : h + 1, :] = out[s : s + 1, 64 * h : 64 * h + 2].astype(BF)

    return pl.pallas_call(
        body,
        out_shape=[jax.ShapeDtypeStruct((2, 2, 2, 128), BF), jax.ShapeDtypeStruct((2, 2, 2), BF)],
        in_specs=[SMEM, VMEM, VMEM],
        out_specs=[VMEM] * 2,
        compiler_params=GRANT,
        name="finished",
    )(meta, got, fixed)


def per_device(
    hidden_in, w_value, w_key, w_step, conv_value, conv_key, step_bias, decay_rate, decay_jump,
    new_value, new_key, new_query, new_gate, new_step, read_gain,
):
    sp_count, y_count, c_count = (lax.axis_size(a) for a in ("sp", "y", "c"))
    sp, y, c = (lax.axis_index(a) for a in ("sp", "y", "c"))
    tp_count = y_count * c_count
    count = sp_count * tp_count
    rows, width = hidden_in.shape[1:]
    heads = step_bias.shape[0]
    share = HEAD_DIM // sp_count
    half = y_count // 2

    def swap(v):
        return lax.ppermute(v, "c", [(0, 1), (1, 0)])

    def onward(v):
        pairs = []
        for i in range(y_count):
            pairs.append((2 * i, 2 * ((i + 1) % y_count)))
            pairs.append((2 * i + 1, 2 * ((i - 1) % y_count) + 1))
        return lax.ppermute(v, ("y", "c"), pairs)

    meta = jnp.stack([y, c, (128 - sp * share) % 128]).astype(jnp.int32)

    def last(v):
        return v.reshape(2, rows, width)[:, rows - 4 :, :].reshape(8, width)

    a = [hidden_in.reshape(2 * rows, width)]
    a.append(onward(a[0]))
    b = [swap(a[0])]
    b.append(onward(b[0]))
    ends = last(a[0]), last(b[0])
    before = jnp.where(c == 1, *ends)
    before = lax.ppermute(before, ("sp", "y", "c"), [(i, i + 2) for i in range(count - 2)])

    def straight(v, far):
        pairs = []
        for i in range(y_count):
            pairs.append((2 * i + 1, 2 * ((i + far) % y_count)))
            pairs.append((2 * i, 2 * ((i - far) % y_count) + 1))
        return lax.ppermute(v, ("y", "c"), pairs)

    w_own = joined(w_value, w_key, conv_value, conv_key)
    w_both = w_own, swap(w_own)
    pair = lax.dynamic_slice_in_dim(w_step.T, y * 2 * heads, 2 * heads, 0)
    pair = jnp.where(c == 0, pair, jnp.roll(pair, heads, axis=0))
    w_steps = jnp.pad(pair, ((0, 8 - 2 * heads), (0, 0)))
    rates = jnp.broadcast_to(jnp.stack([step_bias, decay_rate])[:, :, None], (2, heads, 128))
    jump = jnp.concatenate([decay_jump.transpose(0, 2, 1), rates], axis=2)
    jump = jnp.concatenate([jump, swap(jump)], axis=1)
    jump = jnp.pad(jump, ((0, 0), (0, 8 - 2 * heads), (0, 0)))
    rates = jump[:, :, tp_count * rows :]
    jump = jump[:, :, : tp_count * rows].reshape(2, 8, tp_count, rows).transpose(2, 1, 0, 3)
    jump = jump.reshape(tp_count, 8, 2 * rows)

    def add(runs, xs, halo, far, end):
        return piece_states(meta, xs, halo, far, end, w_steps, w_both, jump, rates, runs, rows, y_count)

    runs = add(None, [a[0]], jnp.where(c == 0, before, ends[1]), 0, False)
    for s in range(1, half):
        a.append(onward(a[s]))
        if s + 1 < half:
            b.append(onward(b[s]))
        runs = add(runs, [a[s], b[s]], straight(before, s), s, False)

    fixed, query = terms(step_bias, decay_rate, new_step, new_value, new_key, new_query, new_gate, read_gain)
    end = straight(jnp.where(c == 1, before, ends[0]), half)
    runs, fixed, query, end = lax.optimization_barrier((runs, fixed, query, end))
    own, other = add(runs, [a[half]], end, half, True)
    sent = packed(meta, own, swap(other), query, sp_count, y_count)
    got = lax.all_to_all(sent, "sp", 0, 0, tiled=True)
    return tuple(finished(meta, got, fixed))


def solution(mesh):
    tp = ("y", "c")
    chips = Mesh(mesh.devices.reshape(mesh.shape["sp"], mesh.shape["tp"] // 2, 2), ("sp", *tp))

    return jax.shard_map(
        per_device,
        mesh=chips,
        in_specs=(
            P(None, ("sp", *tp), None), P(None, tp), P(None, tp), P(), P(None, tp), P(None, tp), P(tp), P(tp),
            P(None, "sp", tp), P(None, tp), P(None, tp), P(None, tp), P(None, tp), P(None, tp), P(tp),
        ),
        out_specs=(P(None, tp, "sp", None), P(None, tp, "sp")),
        check_vma=False,
    )
```

```python
import jax
import jax.numpy as jnp
from jax import lax
from jax.experimental import pallas as pl
from jax.experimental.pallas import tpu as pltpu
from jax.sharding import Mesh
from jax.sharding import PartitionSpec as P

HEAD_DIM = 64
EPSILON = 1e-05
BF = jnp.bfloat16
F32 = jnp.float32
GRANT = pltpu.CompilerParams(vmem_limit_bytes=16 * 1024 * 1024)
VMEM = pl.BlockSpec(memory_space=pltpu.VMEM)
SMEM = pl.BlockSpec(memory_space=pltpu.SMEM)


def mm(a, b, dims, precision=None):
    return lax.dot_general(a, b, (dims, ((), ())), preferred_element_type=F32, precision=precision)


def halves(v):
    high = v.astype(BF)
    return high, (v - high.astype(F32)).astype(BF)


def product(a, b):
    (ah, al), (bh, bl) = halves(a), halves(b)
    dims = ((0,), (0,))
    return mm(ah, bh, dims) + (mm(al, bh, dims) + mm(ah, bl, dims))


def softplus(v):
    return jnp.maximum(v, 0.0) + jnp.log1p(jnp.exp(-jnp.abs(v)))


def piece_states(meta, xs, halo, far, end, w_step, w, jump, rates, runs, rows, chips):
    depth = w[0].shape[0] - 4
    many, both = len(xs), 2 * rows
    given = [] if runs is None else list(runs)
    xs = xs if halo is None else [*xs, halo]
    held = len(xs)

    def body(m_ref, *refs):
        x_refs = refs[:held]
        s_ref, wa_ref, wb_ref, j_ref, r_ref = refs[held : held + 5]
        ins = refs[held + 5 : held + 5 + len(given)]
        own_out, other_out, ext, full = refs[held + 5 + len(given) :]
        outs = (own_out, other_out)
        y, c = m_ref[0], m_ref[1]
        low = c == 0
        away = jnp.where(low, y - far, y + far)
        wrapped = jnp.logical_or(away < 0, away >= chips)
        chip = jnp.where(away < 0, away + chips, jnp.where(away >= chips, away - chips, away))
        run = 2 if end else jnp.where(wrapped, 1, 0)
        place = (2 * chip + c, 2 * chip + 1 - c)
        for g in range(2):
            if given:
                outs[g][...] = ins[g][...]
            else:
                outs[g][...] = jnp.zeros(outs[g].shape, F32)

        lane = lax.broadcasted_iota(jnp.int32, (8, both), 1)
        i = lax.broadcasted_iota(jnp.int32, (both, both), 0)
        j = lax.broadcasted_iota(jnp.int32, (both, both), 1)
        below = jnp.where(jnp.logical_and(i > j, (i >= rows) == (j >= rows)), 1.0, 0.0)
        sizes, afters, sums = [], [], []
        for n in range(many):
            step = mm(s_ref[...], x_refs[n][...], ((1,), (1,))).astype(BF).astype(F32)[:, :both]
            size = softplus(step + r_ref[0][:, 0:1])
            decay = j_ref[place[n]] - r_ref[1][:, 0:1] * size
            sizes.append(size)
            afters.append(mm(decay, below, ((1,), (0,)), lax.Precision.HIGHEST))
            sums.append([
                jnp.sum(jnp.where(lane < rows, decay, 0.0), axis=1, keepdims=True),
                jnp.sum(jnp.where(lane < rows, 0.0, decay), axis=1, keepdims=True),
            ])
        total = [sum(v[s] for v in sums) for s in range(2)]
        before = [own_out[run, s, 128:136, :] for s in range(2)]
        lead = [jnp.where(low, v[:, 0:1], 0.0) for v in before]
        lifts = []
        for n in range(many):
            more = list(lead)
            if many == 2:
                first = low if n == 0 else jnp.logical_not(low)
                more = [more[s] + jnp.where(first, sums[1 - n][s], 0.0) for s in range(2)]
            weight = sizes[n] * jnp.exp(afters[n] + jnp.where(lane < rows, more[0], more[1]))
            weight = jnp.concatenate([weight, jnp.zeros((8, 256 - both), F32)], axis=1)
            lifts.append(jnp.transpose(weight))

        taps = jnp.concatenate([r[depth : depth + 4, :] for r in (wa_ref, wb_ref)], axis=1).astype(F32)
        if many == 1:
            full[:both, :] = x_refs[0][...]
            full[both:, :] = x_refs[1][...]
        inputs = [full] if many == 1 else x_refs
        for g, r in enumerate((wa_ref, wb_ref)):
            cols = slice(256 * g, 256 * g + 256)
            p = [
                mm(v[...], r[:depth, :], ((1,), (0,))).astype(BF).astype(F32)
                for v in inputs
            ]
            for s in range(2):
                before_row = [p[many - 1][both + 4 * s : both + 4 * s + 4, :]]
                if many == 2:
                    last = [v[(s + 1) * rows - 4 : (s + 1) * rows, :] for v in p]
                    outer = before_row[0]
                    before_row = [jnp.where(low, outer, last[1]), jnp.where(low, last[0], outer)]
                for n in range(many):
                    ext[2 * n + s, 4:8, cols] = before_row[n]
                    ext[2 * n + s, 8 : 8 + rows, cols] = p[n][s * rows : (s + 1) * rows, :]
        for s in range(2):
            states = [jnp.zeros((128, 128), F32)] * 2
            for n in range(many):
                mixed = ext[2 * n + s, 5 : 5 + rows, :] * taps[0:1, :]
                for k in range(1, 4):
                    mixed = mixed + ext[2 * n + s, 5 + k : 5 + k + rows, :] * taps[k : k + 1, :]
                mixed = mixed / (1.0 + jnp.exp(-mixed))
                lift = lifts[n][s * rows : (s + 1) * rows, :]
                for g in range(2):
                    parts = [
                        mixed[:, 256 * g + 64 * e : 256 * g + 64 * e + 64] * lift[:, 2 * g + e : 2 * g + e + 1]
                        for e in range(2)
                    ]
                    values = jnp.concatenate(parts, axis=1)
                    keys = mixed[:, 256 * g + 128 : 256 * g + 256]
                    states[g] = states[g] + product(values, keys)
            fade = jnp.where(low, 1.0, jnp.exp(total[s]))
            for g in range(2):
                for e in range(2):
                    part = slice(64 * e, 64 * e + 64)
                    old = outs[g][run, s, part, :]
                    outs[g][run, s, part, :] = old * fade[2 * g + e : 2 * g + e + 1, :] + states[g][part, :]
                outs[g][run, s, 128:136, :] = before[s] + total[s]

    shape = (3, 2, 136, 128)
    return pl.pallas_call(
        body,
        out_shape=[jax.ShapeDtypeStruct(shape, F32)] * 2,
        in_specs=[SMEM] + [VMEM] * (held + 5 + len(given)),
        out_specs=[VMEM] * 2,
        scratch_shapes=[pltpu.VMEM((2 * many, rows + 8, 512), F32), pltpu.VMEM((both + 8, depth), BF)],
        cost_estimate=pl.CostEstimate(
            flops=32 * sum(x.shape[0] for x in xs) * w[0].size,
            transcendentals=0,
            bytes_accessed=4 * w[0].size,
        ),
        compiler_params=GRANT,
        name="piece_states",
    )(meta, *xs, w_step, *w, jump, rates, *given)


def joined(w_value, w_key, conv_value, conv_key):
    depth = w_value.shape[0]

    def body(v_ref, k_ref, cv_ref, ck_ref, out_ref):
        out_ref[:depth, :128] = v_ref[...]
        out_ref[:depth, 128:] = k_ref[...]
        out_ref[depth:, :128] = cv_ref[...]
        out_ref[depth:, 128:] = ck_ref[...]

    return pl.pallas_call(
        body,
        out_shape=jax.ShapeDtypeStruct((depth + conv_value.shape[0], 256), BF),
        in_specs=[VMEM] * 4,
        out_specs=VMEM,
        compiler_params=GRANT,
        name="joined",
    )(w_value, w_key, conv_value, conv_key)


def terms(step_bias, decay_rate, new_step, new_value, new_key, new_query, new_gate, read_gain):
    def body(b_ref, r_ref, n_ref, v_ref, k_ref, q_ref, g_ref, gain_ref, out_ref, query_ref):
        lane = lax.broadcasted_iota(jnp.int32, (1, 128), 1)

        def spread(a, b):
            return jnp.where(lane < HEAD_DIM, a, b)

        query = q_ref[...].astype(F32)
        query_ref[...] = query
        value, key, gate = (r[...].astype(F32) for r in (v_ref, k_ref, g_ref))
        match = jnp.sum(key * query, axis=1, keepdims=True)
        gates = gate / (1.0 + jnp.exp(-gate))
        rate = spread(r_ref[0], r_ref[1])
        for s in range(2):
            size = softplus(spread(n_ref[s, 0] + b_ref[0], n_ref[s, 1] + b_ref[1]))
            out_ref[s : s + 1, :] = jnp.exp(-rate * size)
            out_ref[2 + s : 3 + s, :] = size * match[s : s + 1, :] * value[s : s + 1, :]
        out_ref[4:6, :] = gates
        out_ref[6:7, :] = gain_ref[...].astype(F32)
        out_ref[7:8, :] = jnp.zeros((1, 128), F32)

    return pl.pallas_call(
        body,
        out_shape=[jax.ShapeDtypeStruct((8, 128), F32), jax.ShapeDtypeStruct((2, 128), F32)],
        in_specs=[SMEM] * 3 + [VMEM] * 5,
        out_specs=[VMEM] * 2,
        compiler_params=GRANT,
        name="terms",
    )(step_bias, decay_rate, new_step, new_value, new_key, new_query, new_gate, read_gain.reshape(1, 128))


def packed(meta, own, got, query, sp_count, chips):
    share = HEAD_DIM // sp_count

    def body(m_ref, a_ref, b_ref, q_ref, out_ref):
        def put(row, value):
            out_ref[:, row : row + 1, :] = jnp.broadcast_to(value[None], (sp_count, 1, 128))

        low = m_ref[1] == 0
        late = m_ref[0] < chips // 2
        lane = lax.broadcasted_iota(jnp.int32, (1, 128), 1)
        left = jnp.zeros((1, 128), F32)
        for s in range(2):
            mine = [a_ref[r, s, 128:130, :] for r in range(3)]
            theirs = [b_ref[r, s, 130:132, :] for r in range(3)]
            d1, d2, d3 = (jnp.where(low, m, t) for m, t in zip(mine, theirs))
            u1, u2, u3 = (jnp.where(low, t, m) for m, t in zip(mine, theirs))
            last = d3 + u3
            after_u1 = d2 + jnp.where(late, last, 0.0)
            after_d1 = after_u1 + u1
            after_u3 = jnp.where(late, d2, after_d1 + d1)
            after_d3 = after_u3 + u3
            after_u2 = after_d1 + d1 + jnp.where(late, 0.0, last)
            total = after_u2 + u2
            for e in range(2):
                left = jnp.where(lane == 2 * s + e, total[e : e + 1, :], left)
            down = [jnp.exp(v) for v in (after_d1, jnp.zeros_like(d2), after_d3)]
            up = [jnp.exp(v) for v in (after_u1, after_u2, after_u3)]
            reads = []
            for e in range(2):
                state = jnp.zeros((64, 128), F32)
                for r in range(3):
                    part = slice(64 * e, 64 * e + 64)
                    scale_a = jnp.where(low, down[r], up[r])[e : e + 1, :]
                    scale_b = jnp.where(low, up[r], down[r])[e : e + 1, :]
                    state = state + a_ref[r, s, part, :] * scale_a + b_ref[r, s, part, :] * scale_b
                reads.append(jnp.sum(state * q_ref[s : s + 1, :], axis=1).reshape(1, 64))
                cut = state.astype(BF).reshape(sp_count, share, 128)
                out_ref[:, 4 * s + 2 * e : 4 * s + 2 * e + share, :] = cut
            read = jnp.concatenate(reads, axis=1)
            high, low_part = halves(read)
            put(8 + s, high)
            put(10 + s, low_part)
        for k in range(3):
            part = left.astype(BF)
            left = left - part.astype(F32)
            put(12 + k, part)
        put(15, jnp.zeros((1, 128), BF))

    return pl.pallas_call(
        body,
        out_shape=jax.ShapeDtypeStruct((sp_count, 16, 128), BF),
        in_specs=[SMEM] + [VMEM] * 3,
        out_specs=VMEM,
        compiler_params=GRANT,
        name="packed",
    )(meta, own, got, query)


def finished(meta, got, fixed):
    sp_count = got.shape[0]

    def body(m_ref, got_ref, fix_ref, state_out, read_out):
        blocks = [got_ref[j].astype(F32) for j in range(sp_count)]
        decay = jnp.concatenate([g[12:13] + g[13:14] + g[14:15] for g in blocks], axis=0)
        i = lax.broadcasted_iota(jnp.int32, (sp_count, sp_count), 0)
        j = lax.broadcasted_iota(jnp.int32, (sp_count, sp_count), 1)
        after = jnp.where(j > i, 1.0, 0.0)
        fade = jnp.exp(mm(after, decay, ((1,), (0,)), lax.Precision.HIGHEST))
        one = [jnp.broadcast_to(fade[:, i : i + 1], (sp_count, 128)) for i in range(4)]
        lane = lax.broadcasted_iota(jnp.int32, (sp_count, 128), 1)
        both = [jnp.where(lane < HEAD_DIM, one[2 * s], one[2 * s + 1]) for s in range(2)]
        row = lax.broadcasted_iota(jnp.int32, (8, 128), 0)
        total = [jnp.zeros((8, 128), F32)] * 2
        for j, g in enumerate(blocks):
            a, b, c, d = (v[j : j + 1] for v in one)
            scale = jnp.where(row < 4, jnp.where(row < 2, a, b), jnp.where(row < 6, c, d))
            total[0] = total[0] + g[:8] * scale
            total[1] = total[1] + g[8:] * jnp.where(row % 2 == 0, both[0][j : j + 1], both[1][j : j + 1])
        total = jnp.concatenate(total, axis=0)
        for s in range(2):
            for h in range(2):
                state_out[s, h] = total[4 * s + 2 * h : 4 * s + 2 * h + 2].astype(BF)
        read = total[8:10] + total[10:12]
        gated = (fix_ref[0:2] * read + fix_ref[2:4]) * fix_ref[4:6]
        mean = jnp.mean(gated * gated, axis=1, keepdims=True)
        out = gated * lax.rsqrt(mean + EPSILON) * fix_ref[6:7]
        out = jnp.concatenate([out, jnp.zeros((6, 128), F32)], axis=0)
        out = pltpu.roll(out, m_ref[2], 1)
        for s in range(2):
            for h in range(2):
                read_out[s, h : h + 1, :] = out[s : s + 1, 64 * h : 64 * h + 2].astype(BF)

    return pl.pallas_call(
        body,
        out_shape=[jax.ShapeDtypeStruct((2, 2, 2, 128), BF), jax.ShapeDtypeStruct((2, 2, 2), BF)],
        in_specs=[SMEM, VMEM, VMEM],
        out_specs=[VMEM] * 2,
        compiler_params=GRANT,
        name="finished",
    )(meta, got, fixed)


def per_device(
    hidden_in, w_value, w_key, w_step, conv_value, conv_key, step_bias, decay_rate, decay_jump,
    new_value, new_key, new_query, new_gate, new_step, read_gain,
):
    sp_count, y_count, c_count = (lax.axis_size(a) for a in ("sp", "y", "c"))
    sp, y, c = (lax.axis_index(a) for a in ("sp", "y", "c"))
    tp_count = y_count * c_count
    count = sp_count * tp_count
    rows, width = hidden_in.shape[1:]
    heads = step_bias.shape[0]
    share = HEAD_DIM // sp_count
    half = y_count // 2

    def swap(v):
        return lax.ppermute(v, "c", [(0, 1), (1, 0)])

    def onward(v):
        pairs = []
        for i in range(y_count):
            pairs.append((2 * i, 2 * ((i + 1) % y_count)))
            pairs.append((2 * i + 1, 2 * ((i - 1) % y_count) + 1))
        return lax.ppermute(v, ("y", "c"), pairs)

    meta = jnp.stack([y, c, (128 - sp * share) % 128]).astype(jnp.int32)

    def last(v):
        return v.reshape(2, rows, width)[:, rows - 4 :, :].reshape(8, width)

    a = [hidden_in.reshape(2 * rows, width)]
    a.append(onward(a[0]))
    b = [swap(a[0])]
    b.append(onward(b[0]))
    ends = last(a[0]), last(b[0])
    before = jnp.where(c == 1, *ends)
    before = lax.ppermute(before, ("sp", "y", "c"), [(i, i + 2) for i in range(count - 2)])

    near = onward(before)
    b[1] = jnp.concatenate([b[1], near], axis=0)

    later = (w_value, w_key, conv_value, conv_key, w_step, decay_jump, step_bias, decay_rate)
    a[1], *later = lax.optimization_barrier((a[1], *later))
    w_value, w_key, conv_value, conv_key, w_step, decay_jump, step_bias, decay_rate = later

    w_own = joined(w_value, w_key, conv_value, conv_key)
    w_both = w_own, swap(w_own)
    pair = lax.dynamic_slice_in_dim(w_step.T, y * 2 * heads, 2 * heads, 0)
    pair = jnp.where(c == 0, pair, jnp.roll(pair, heads, axis=0))
    w_steps = jnp.pad(pair, ((0, 8 - 2 * heads), (0, 0)))
    rates = jnp.broadcast_to(jnp.stack([step_bias, decay_rate])[:, :, None], (2, heads, 128))
    jump = jnp.concatenate([decay_jump.transpose(0, 2, 1), rates], axis=2)
    jump = jnp.concatenate([jump, swap(jump)], axis=1)
    jump = jnp.pad(jump, ((0, 0), (0, 8 - 2 * heads), (0, 0)))
    rates = jump[:, :, tp_count * rows :]
    jump = jump[:, :, : tp_count * rows].reshape(2, 8, tp_count, rows).transpose(2, 1, 0, 3)
    jump = jump.reshape(tp_count, 8, 2 * rows)

    def add(runs, xs, halo, far, end):
        return piece_states(meta, xs, halo, far, end, w_steps, w_both, jump, rates, runs, rows, y_count)

    runs = add(None, [a[0]], jnp.where(c == 0, before, ends[1]), 0, False)
    for s in range(1, half):
        a.append(onward(a[s]))
        if s + 1 < half:
            b.append(onward(b[s]))
        if s == half - 2:
            a[s + 1], runs = lax.optimization_barrier((a[s + 1], runs))
        runs = add(runs, [a[s], b[s]], None, s, False)

    fixed, query = terms(step_bias, decay_rate, new_step, new_value, new_key, new_query, new_gate, read_gain)
    end = b[half - 1]
    end = onward(jnp.where(c == 0, end[2 * rows :], last(end[: 2 * rows])))
    runs, fixed, query, end = lax.optimization_barrier((runs, fixed, query, end))
    own, other = add(runs, [a[half]], end, half, True)
    sent = packed(meta, own, swap(other), query, sp_count, y_count)
    got = lax.all_to_all(sent, "sp", 0, 0, tiled=True)
    return tuple(finished(meta, got, fixed))


def solution(mesh):
    tp = ("y", "c")
    chips = Mesh(mesh.devices.reshape(mesh.shape["sp"], mesh.shape["tp"] // 2, 2), ("sp", *tp))

    return jax.shard_map(
        per_device,
        mesh=chips,
        in_specs=(
            P(None, ("sp", *tp), None), P(None, tp), P(None, tp), P(), P(None, tp), P(None, tp), P(tp), P(tp),
            P(None, "sp", tp), P(None, tp), P(None, tp), P(None, tp), P(None, tp), P(None, tp), P(tp),
        ),
        out_specs=(P(None, tp, "sp", None), P(None, tp, "sp")),
        check_vma=False,
    )
```

```python
import jax
import jax.numpy as jnp
from jax import lax
from jax.experimental import pallas as pl
from jax.experimental.pallas import tpu as pltpu
from jax.sharding import Mesh
from jax.sharding import PartitionSpec as P

HEAD_DIM = 64
EPSILON = 1e-05
BF = jnp.bfloat16
F32 = jnp.float32
GRANT = pltpu.CompilerParams(vmem_limit_bytes=16 * 1024 * 1024)
VMEM = pl.BlockSpec(memory_space=pltpu.VMEM)
SMEM = pl.BlockSpec(memory_space=pltpu.SMEM)


def mm(a, b, dims, precision=None):
    return lax.dot_general(a, b, (dims, ((), ())), preferred_element_type=F32, precision=precision)


def halves(v):
    high = v.astype(BF)
    return high, (v - high.astype(F32)).astype(BF)


def product(a, b):
    (ah, al), (bh, bl) = halves(a), halves(b)
    dims = ((0,), (0,))
    return mm(ah, bh, dims) + (mm(al, bh, dims) + mm(ah, bl, dims))


def softplus(v):
    return jnp.maximum(v, 0.0) + jnp.log1p(jnp.exp(-jnp.abs(v)))


def piece_states(meta, xs, halo, far, end, w_step, w, jump, rates, runs, rows, chips):
    depth = w[0].shape[0] - 4
    many, both = len(xs), 2 * rows
    given = [] if runs is None else list(runs)
    xs = xs if halo is None else [*xs, halo]
    held = len(xs)

    def body(m_ref, *refs):
        x_refs = refs[:held]
        s_ref, wa_ref, wb_ref, j_ref, r_ref = refs[held : held + 5]
        ins = refs[held + 5 : held + 5 + len(given)]
        own_out, other_out, ext, full = refs[held + 5 + len(given) :]
        outs = (own_out, other_out)
        y, c = m_ref[0], m_ref[1]
        low = c == 0
        away = jnp.where(low, y - far, y + far)
        wrapped = jnp.logical_or(away < 0, away >= chips)
        chip = jnp.where(away < 0, away + chips, jnp.where(away >= chips, away - chips, away))
        run = 2 if end else jnp.where(wrapped, 1, 0)
        place = (2 * chip + c, 2 * chip + 1 - c)
        for g in range(2):
            if given:
                outs[g][...] = ins[g][...]
            else:
                outs[g][...] = jnp.zeros(outs[g].shape, F32)

        lane = lax.broadcasted_iota(jnp.int32, (8, both), 1)
        i = lax.broadcasted_iota(jnp.int32, (both, both), 0)
        j = lax.broadcasted_iota(jnp.int32, (both, both), 1)
        below = jnp.where(jnp.logical_and(i > j, (i >= rows) == (j >= rows)), 1.0, 0.0)
        sizes, afters, sums = [], [], []
        for n in range(many):
            step = mm(s_ref[...], x_refs[n][...], ((1,), (1,))).astype(BF).astype(F32)[:, :both]
            size = softplus(step + r_ref[0][:, 0:1])
            decay = j_ref[place[n]] - r_ref[1][:, 0:1] * size
            sizes.append(size)
            afters.append(mm(decay, below, ((1,), (0,)), lax.Precision.HIGHEST))
            sums.append([
                jnp.sum(jnp.where(lane < rows, decay, 0.0), axis=1, keepdims=True),
                jnp.sum(jnp.where(lane < rows, 0.0, decay), axis=1, keepdims=True),
            ])
        total = [sum(v[s] for v in sums) for s in range(2)]
        before = [own_out[run, s, 128:136, :] for s in range(2)]
        lead = [jnp.where(low, v[:, 0:1], 0.0) for v in before]
        lifts = []
        for n in range(many):
            more = list(lead)
            if many == 2:
                first = low if n == 0 else jnp.logical_not(low)
                more = [more[s] + jnp.where(first, sums[1 - n][s], 0.0) for s in range(2)]
            weight = sizes[n] * jnp.exp(afters[n] + jnp.where(lane < rows, more[0], more[1]))
            weight = jnp.concatenate([weight, jnp.zeros((8, 256 - both), F32)], axis=1)
            lifts.append(jnp.transpose(weight))

        taps = jnp.concatenate([r[depth : depth + 4, :] for r in (wa_ref, wb_ref)], axis=1).astype(F32)
        if many == 1:
            full[:both, :] = x_refs[0][...]
            full[both:, :] = x_refs[1][...]
        inputs = [full] if many == 1 else x_refs
        for g, r in enumerate((wa_ref, wb_ref)):
            cols = slice(256 * g, 256 * g + 256)
            p = [
                mm(v[...], r[:depth, :], ((1,), (0,))).astype(BF).astype(F32)
                for v in inputs
            ]
            for s in range(2):
                before_row = [p[many - 1][both + 4 * s : both + 4 * s + 4, :]]
                if many == 2:
                    last = [v[(s + 1) * rows - 4 : (s + 1) * rows, :] for v in p]
                    outer = before_row[0]
                    before_row = [jnp.where(low, outer, last[1]), jnp.where(low, last[0], outer)]
                for n in range(many):
                    ext[2 * n + s, 4:8, cols] = before_row[n]
                    ext[2 * n + s, 8 : 8 + rows, cols] = p[n][s * rows : (s + 1) * rows, :]
        for s in range(2):
            states = [jnp.zeros((128, 128), F32)] * 2
            for n in range(many):
                mixed = ext[2 * n + s, 5 : 5 + rows, :] * taps[0:1, :]
                for k in range(1, 4):
                    mixed = mixed + ext[2 * n + s, 5 + k : 5 + k + rows, :] * taps[k : k + 1, :]
                mixed = mixed / (1.0 + jnp.exp(-mixed))
                lift = lifts[n][s * rows : (s + 1) * rows, :]
                for g in range(2):
                    parts = [
                        mixed[:, 256 * g + 64 * e : 256 * g + 64 * e + 64] * lift[:, 2 * g + e : 2 * g + e + 1]
                        for e in range(2)
                    ]
                    values = jnp.concatenate(parts, axis=1)
                    keys = mixed[:, 256 * g + 128 : 256 * g + 256]
                    states[g] = states[g] + product(values, keys)
            fade = jnp.where(low, 1.0, jnp.exp(total[s]))
            for g in range(2):
                for e in range(2):
                    part = slice(64 * e, 64 * e + 64)
                    old = outs[g][run, s, part, :]
                    outs[g][run, s, part, :] = old * fade[2 * g + e : 2 * g + e + 1, :] + states[g][part, :]
                outs[g][run, s, 128:136, :] = before[s] + total[s]

    shape = (3, 2, 136, 128)
    return pl.pallas_call(
        body,
        out_shape=[jax.ShapeDtypeStruct(shape, F32)] * 2,
        in_specs=[SMEM] + [VMEM] * (held + 5 + len(given)),
        out_specs=[VMEM] * 2,
        scratch_shapes=[pltpu.VMEM((2 * many, rows + 8, 512), F32), pltpu.VMEM((both + 8, depth), BF)],
        cost_estimate=pl.CostEstimate(
            flops=32 * sum(x.shape[0] for x in xs) * w[0].size,
            transcendentals=0,
            bytes_accessed=4 * w[0].size,
        ),
        compiler_params=GRANT,
        name="piece_states",
    )(meta, *xs, w_step, *w, jump, rates, *given)


def joined(w_value, w_key, conv_value, conv_key):
    depth = w_value.shape[0]

    def body(v_ref, k_ref, cv_ref, ck_ref, out_ref):
        out_ref[:depth, :128] = v_ref[...]
        out_ref[:depth, 128:] = k_ref[...]
        out_ref[depth:, :128] = cv_ref[...]
        out_ref[depth:, 128:] = ck_ref[...]

    return pl.pallas_call(
        body,
        out_shape=jax.ShapeDtypeStruct((depth + conv_value.shape[0], 256), BF),
        in_specs=[VMEM] * 4,
        out_specs=VMEM,
        compiler_params=GRANT,
        name="joined",
    )(w_value, w_key, conv_value, conv_key)


def terms(step_bias, decay_rate, new_step, new_value, new_key, new_query, new_gate, read_gain):
    def body(b_ref, r_ref, n_ref, v_ref, k_ref, q_ref, g_ref, gain_ref, out_ref, query_ref):
        lane = lax.broadcasted_iota(jnp.int32, (1, 128), 1)

        def spread(a, b):
            return jnp.where(lane < HEAD_DIM, a, b)

        query = q_ref[...].astype(F32)
        query_ref[...] = query
        value, key, gate = (r[...].astype(F32) for r in (v_ref, k_ref, g_ref))
        match = jnp.sum(key * query, axis=1, keepdims=True)
        gates = gate / (1.0 + jnp.exp(-gate))
        rate = spread(r_ref[0], r_ref[1])
        for s in range(2):
            size = softplus(spread(n_ref[s, 0] + b_ref[0], n_ref[s, 1] + b_ref[1]))
            out_ref[s : s + 1, :] = jnp.exp(-rate * size)
            out_ref[2 + s : 3 + s, :] = size * match[s : s + 1, :] * value[s : s + 1, :]
        out_ref[4:6, :] = gates
        out_ref[6:7, :] = gain_ref[...].astype(F32)
        out_ref[7:8, :] = jnp.zeros((1, 128), F32)

    return pl.pallas_call(
        body,
        out_shape=[jax.ShapeDtypeStruct((8, 128), F32), jax.ShapeDtypeStruct((2, 128), F32)],
        in_specs=[SMEM] * 3 + [VMEM] * 5,
        out_specs=[VMEM] * 2,
        compiler_params=GRANT,
        name="terms",
    )(step_bias, decay_rate, new_step, new_value, new_key, new_query, new_gate, read_gain.reshape(1, 128))


def packed(meta, own, got, query, sp_count, chips):
    share = HEAD_DIM // sp_count

    def body(m_ref, a_ref, b_ref, q_ref, out_ref):
        def put(row, value):
            out_ref[:, row : row + 1, :] = jnp.broadcast_to(value[None], (sp_count, 1, 128))

        low = m_ref[1] == 0
        late = m_ref[0] < chips // 2
        lane = lax.broadcasted_iota(jnp.int32, (1, 128), 1)
        left = jnp.zeros((1, 128), F32)
        for s in range(2):
            mine = [a_ref[r, s, 128:130, :] for r in range(3)]
            theirs = [b_ref[r, s, 130:132, :] for r in range(3)]
            d1, d2, d3 = (jnp.where(low, m, t) for m, t in zip(mine, theirs))
            u1, u2, u3 = (jnp.where(low, t, m) for m, t in zip(mine, theirs))
            last = d3 + u3
            after_u1 = d2 + jnp.where(late, last, 0.0)
            after_d1 = after_u1 + u1
            after_u3 = jnp.where(late, d2, after_d1 + d1)
            after_d3 = after_u3 + u3
            after_u2 = after_d1 + d1 + jnp.where(late, 0.0, last)
            total = after_u2 + u2
            for e in range(2):
                left = jnp.where(lane == 2 * s + e, total[e : e + 1, :], left)
            down = [jnp.exp(v) for v in (after_d1, jnp.zeros_like(d2), after_d3)]
            up = [jnp.exp(v) for v in (after_u1, after_u2, after_u3)]
            reads = []
            for e in range(2):
                state = jnp.zeros((64, 128), F32)
                for r in range(3):
                    part = slice(64 * e, 64 * e + 64)
                    scale_a = jnp.where(low, down[r], up[r])[e : e + 1, :]
                    scale_b = jnp.where(low, up[r], down[r])[e : e + 1, :]
                    state = state + a_ref[r, s, part, :] * scale_a + b_ref[r, s, part, :] * scale_b
                reads.append(jnp.sum(state * q_ref[s : s + 1, :], axis=1).reshape(1, 64))
                cut = state.astype(BF).reshape(sp_count, share, 128)
                out_ref[:, 4 * s + 2 * e : 4 * s + 2 * e + share, :] = cut
            read = jnp.concatenate(reads, axis=1)
            high, low_part = halves(read)
            put(8 + s, high)
            put(10 + s, low_part)
        for k in range(3):
            part = left.astype(BF)
            left = left - part.astype(F32)
            put(12 + k, part)
        put(15, jnp.zeros((1, 128), BF))

    return pl.pallas_call(
        body,
        out_shape=jax.ShapeDtypeStruct((sp_count, 16, 128), BF),
        in_specs=[SMEM] + [VMEM] * 3,
        out_specs=VMEM,
        compiler_params=GRANT,
        name="packed",
    )(meta, own, got, query)


def finished(meta, got, fixed):
    sp_count = got.shape[0]

    def body(m_ref, got_ref, fix_ref, state_out, read_out):
        blocks = [got_ref[j].astype(F32) for j in range(sp_count)]
        decay = jnp.concatenate([g[12:13] + g[13:14] + g[14:15] for g in blocks], axis=0)
        i = lax.broadcasted_iota(jnp.int32, (sp_count, sp_count), 0)
        j = lax.broadcasted_iota(jnp.int32, (sp_count, sp_count), 1)
        after = jnp.where(j > i, 1.0, 0.0)
        fade = jnp.exp(mm(after, decay, ((1,), (0,)), lax.Precision.HIGHEST))
        one = [jnp.broadcast_to(fade[:, i : i + 1], (sp_count, 128)) for i in range(4)]
        lane = lax.broadcasted_iota(jnp.int32, (sp_count, 128), 1)
        both = [jnp.where(lane < HEAD_DIM, one[2 * s], one[2 * s + 1]) for s in range(2)]
        row = lax.broadcasted_iota(jnp.int32, (8, 128), 0)
        total = [jnp.zeros((8, 128), F32)] * 2
        for j, g in enumerate(blocks):
            a, b, c, d = (v[j : j + 1] for v in one)
            scale = jnp.where(row < 4, jnp.where(row < 2, a, b), jnp.where(row < 6, c, d))
            total[0] = total[0] + g[:8] * scale
            total[1] = total[1] + g[8:] * jnp.where(row % 2 == 0, both[0][j : j + 1], both[1][j : j + 1])
        total = jnp.concatenate(total, axis=0)
        for s in range(2):
            for h in range(2):
                state_out[s, h] = total[4 * s + 2 * h : 4 * s + 2 * h + 2].astype(BF)
        read = total[8:10] + total[10:12]
        gated = (fix_ref[0:2] * read + fix_ref[2:4]) * fix_ref[4:6]
        mean = jnp.mean(gated * gated, axis=1, keepdims=True)
        out = gated * lax.rsqrt(mean + EPSILON) * fix_ref[6:7]
        out = jnp.concatenate([out, jnp.zeros((6, 128), F32)], axis=0)
        out = pltpu.roll(out, m_ref[2], 1)
        for s in range(2):
            for h in range(2):
                read_out[s, h : h + 1, :] = out[s : s + 1, 64 * h : 64 * h + 2].astype(BF)

    return pl.pallas_call(
        body,
        out_shape=[jax.ShapeDtypeStruct((2, 2, 2, 128), BF), jax.ShapeDtypeStruct((2, 2, 2), BF)],
        in_specs=[SMEM, VMEM, VMEM],
        out_specs=[VMEM] * 2,
        compiler_params=GRANT,
        name="finished",
    )(meta, got, fixed)


def per_device(
    hidden_in, w_value, w_key, w_step, conv_value, conv_key, step_bias, decay_rate, decay_jump,
    new_value, new_key, new_query, new_gate, new_step, read_gain,
):
    sp_count, y_count, c_count = (lax.axis_size(a) for a in ("sp", "y", "c"))
    sp, y, c = (lax.axis_index(a) for a in ("sp", "y", "c"))
    tp_count = y_count * c_count
    count = sp_count * tp_count
    rows, width = hidden_in.shape[1:]
    heads = step_bias.shape[0]
    share = HEAD_DIM // sp_count
    half = y_count // 2

    def swap(v):
        return lax.ppermute(v, "c", [(0, 1), (1, 0)])

    def onward(v):
        pairs = []
        for i in range(y_count):
            pairs.append((2 * i, 2 * ((i + 1) % y_count)))
            pairs.append((2 * i + 1, 2 * ((i - 1) % y_count) + 1))
        return lax.ppermute(v, ("y", "c"), pairs)

    meta = jnp.stack([y, c, (128 - sp * share) % 128]).astype(jnp.int32)

    def last(v):
        return v.reshape(2, rows, width)[:, rows - 4 :, :].reshape(8, width)

    a = [hidden_in.reshape(2 * rows, width)]
    a.append(onward(a[0]))
    b = [swap(a[0])]
    b.append(onward(b[0]))
    ends = last(a[0]), last(b[0])
    before = jnp.where(c == 1, *ends)
    before = lax.ppermute(before, ("sp", "y", "c"), [(i, i + 2) for i in range(count - 2)])

    near = onward(before)
    edge = jnp.where(c == 0, before, ends[1])

    later = (w_value, w_key, conv_value, conv_key, w_step, decay_jump, step_bias, decay_rate)
    b[1], *later = lax.optimization_barrier((b[1], *later))
    w_value, w_key, conv_value, conv_key, w_step, decay_jump, step_bias, decay_rate = later
    b[1] = jnp.concatenate([b[1], near], axis=0)

    w_own = joined(w_value, w_key, conv_value, conv_key)
    w_both = w_own, swap(w_own)
    pair = lax.dynamic_slice_in_dim(w_step.T, y * 2 * heads, 2 * heads, 0)
    pair = jnp.where(c == 0, pair, jnp.roll(pair, heads, axis=0))
    w_steps = jnp.pad(pair, ((0, 8 - 2 * heads), (0, 0)))
    rates = jnp.broadcast_to(jnp.stack([step_bias, decay_rate])[:, :, None], (2, heads, 128))
    jump = jnp.concatenate([decay_jump.transpose(0, 2, 1), rates], axis=2)
    jump = jnp.concatenate([jump, swap(jump)], axis=1)
    jump = jnp.pad(jump, ((0, 0), (0, 8 - 2 * heads), (0, 0)))
    rates = jump[:, :, tp_count * rows :]
    jump = jump[:, :, : tp_count * rows].reshape(2, 8, tp_count, rows).transpose(2, 1, 0, 3)
    jump = jump.reshape(tp_count, 8, 2 * rows)

    def add(runs, xs, halo, far, end):
        return piece_states(meta, xs, halo, far, end, w_steps, w_both, jump, rates, runs, rows, y_count)

    runs = add(None, [a[0]], edge, 0, False)
    for s in range(1, half):
        a.append(onward(a[s]))
        if s + 1 < half:
            b.append(onward(b[s]))
        if s == half - 2:
            a[s + 1], runs = lax.optimization_barrier((a[s + 1], runs))
        runs = add(runs, [a[s], b[s]], None, s, False)

    fixed, query = terms(step_bias, decay_rate, new_step, new_value, new_key, new_query, new_gate, read_gain)
    end = b[half - 1]
    end = onward(jnp.where(c == 0, end[2 * rows :], last(end[: 2 * rows])))
    runs, fixed, query, end = lax.optimization_barrier((runs, fixed, query, end))
    own, other = add(runs, [a[half]], end, half, True)
    sent = packed(meta, own, swap(other), query, sp_count, y_count)
    got = lax.all_to_all(sent, "sp", 0, 0, tiled=True)
    return tuple(finished(meta, got, fixed))


def solution(mesh):
    tp = ("y", "c")
    chips = Mesh(mesh.devices.reshape(mesh.shape["sp"], mesh.shape["tp"] // 2, 2), ("sp", *tp))

    return jax.shard_map(
        per_device,
        mesh=chips,
        in_specs=(
            P(None, ("sp", *tp), None), P(None, tp), P(None, tp), P(), P(None, tp), P(None, tp), P(tp), P(tp),
            P(None, "sp", tp), P(None, tp), P(None, tp), P(None, tp), P(None, tp), P(None, tp), P(tp),
        ),
        out_specs=(P(None, tp, "sp", None), P(None, tp, "sp")),
        check_vma=False,
    )
```

```python
import jax
import jax.numpy as jnp
from jax import lax
from jax.experimental import pallas as pl
from jax.experimental.pallas import tpu as pltpu
from jax.sharding import Mesh
from jax.sharding import PartitionSpec as P

HEAD_DIM = 64
EPSILON = 1e-05
BF = jnp.bfloat16
F32 = jnp.float32
GRANT = pltpu.CompilerParams(vmem_limit_bytes=16 * 1024 * 1024)
VMEM = pl.BlockSpec(memory_space=pltpu.VMEM)
SMEM = pl.BlockSpec(memory_space=pltpu.SMEM)


def mm(a, b, dims, precision=None):
    return lax.dot_general(a, b, (dims, ((), ())), preferred_element_type=F32, precision=precision)


def halves(v):
    high = v.astype(BF)
    return high, (v - high.astype(F32)).astype(BF)


def product(a, b):
    (ah, al), (bh, bl) = halves(a), halves(b)
    dims = ((0,), (0,))
    return mm(ah, bh, dims) + (mm(al, bh, dims) + mm(ah, bl, dims))


def softplus(v):
    return jnp.maximum(v, 0.0) + jnp.log1p(jnp.exp(-jnp.abs(v)))


def piece_states(meta, xs, halo, far, end, w_step, w, jump, rates, runs, rows, chips):
    many, both = len(xs), 2 * rows
    depth = w[0].shape[0] - 4
    given = [] if runs is None else list(runs)
    xs = xs if halo is None else [*xs, halo]
    held = len(xs)

    def body(m_ref, *refs):
        x_refs = list(refs[:held])
        s_ref, wa_ref, wb_ref, j_ref, r_ref = refs[held : held + 5]
        ins = refs[held + 5 : held + 5 + len(given)]
        own_out, other_out, ext, full = refs[held + 5 + len(given) :]
        if held > many:
            full[:both, :] = x_refs[0][...]
            full[both:, :] = x_refs[1][...]
            x_refs = [full]
        outs = (own_out, other_out)
        y, c = m_ref[0], m_ref[1]
        low = c == 0
        away = jnp.where(low, y - far, y + far)
        wrapped = jnp.logical_or(away < 0, away >= chips)
        chip = jnp.where(away < 0, away + chips, jnp.where(away >= chips, away - chips, away))
        run = 2 if end else jnp.where(wrapped, 1, 0)
        place = (2 * chip + c, 2 * chip + 1 - c)
        for g in range(2):
            if given:
                outs[g][...] = ins[g][...]
            else:
                outs[g][...] = jnp.zeros(outs[g].shape, F32)

        lane = lax.broadcasted_iota(jnp.int32, (8, both), 1)
        i = lax.broadcasted_iota(jnp.int32, (both, both), 0)
        j = lax.broadcasted_iota(jnp.int32, (both, both), 1)
        below = jnp.where(jnp.logical_and(i > j, (i >= rows) == (j >= rows)), 1.0, 0.0)
        sizes, afters, sums = [], [], []
        for n in range(many):
            step = mm(s_ref[...], x_refs[n][...], ((1,), (1,))).astype(BF).astype(F32)[:, :both]
            size = softplus(step + r_ref[0][:, 0:1])
            decay = j_ref[place[n]] - r_ref[1][:, 0:1] * size
            sizes.append(size)
            afters.append(mm(decay, below, ((1,), (0,)), lax.Precision.HIGHEST))
            sums.append([
                jnp.sum(jnp.where(lane < rows, decay, 0.0), axis=1, keepdims=True),
                jnp.sum(jnp.where(lane < rows, 0.0, decay), axis=1, keepdims=True),
            ])
        total = [sum(v[s] for v in sums) for s in range(2)]
        before = [own_out[run, s, 128:136, :] for s in range(2)]
        lead = [jnp.where(low, v[:, 0:1], 0.0) for v in before]
        lifts = []
        for n in range(many):
            more = list(lead)
            if many == 2:
                first = low if n == 0 else jnp.logical_not(low)
                more = [more[s] + jnp.where(first, sums[1 - n][s], 0.0) for s in range(2)]
            weight = sizes[n] * jnp.exp(afters[n] + jnp.where(lane < rows, more[0], more[1]))
            weight = jnp.concatenate([weight, jnp.zeros((8, 256 - both), F32)], axis=1)
            lifts.append(jnp.transpose(weight))

        taps = jnp.concatenate([r[depth : depth + 4, :] for r in (wa_ref, wb_ref)], axis=1).astype(F32)
        for g, r in enumerate((wa_ref, wb_ref)):
            cols = slice(256 * g, 256 * g + 256)
            p = [mm(v[...], r[:depth, :], ((1,), (0,))).astype(BF).astype(F32) for v in x_refs]
            for n in range(many):
                base = both + 8 * (many - 1 - n)
                for s in range(2):
                    ext[2 * n + s, 4:8, cols] = p[-1][base + 4 * s : base + 4 * s + 4, :]
                    ext[2 * n + s, 8 : 8 + rows, cols] = p[n][s * rows : (s + 1) * rows, :]
        for s in range(2):
            states = [jnp.zeros((128, 128), F32)] * 2
            for n in range(many):
                mixed = ext[2 * n + s, 5 : 5 + rows, :] * taps[0:1, :]
                for k in range(1, 4):
                    mixed = mixed + ext[2 * n + s, 5 + k : 5 + k + rows, :] * taps[k : k + 1, :]
                mixed = mixed / (1.0 + jnp.exp(-mixed))
                lift = lifts[n][s * rows : (s + 1) * rows, :]
                for g in range(2):
                    parts = [
                        mixed[:, 256 * g + 64 * e : 256 * g + 64 * e + 64] * lift[:, 2 * g + e : 2 * g + e + 1]
                        for e in range(2)
                    ]
                    values = jnp.concatenate(parts, axis=1)
                    keys = mixed[:, 256 * g + 128 : 256 * g + 256]
                    states[g] = states[g] + product(values, keys)
            fade = jnp.where(low, 1.0, jnp.exp(total[s]))
            for g in range(2):
                for e in range(2):
                    part = slice(64 * e, 64 * e + 64)
                    old = outs[g][run, s, part, :]
                    outs[g][run, s, part, :] = old * fade[2 * g + e : 2 * g + e + 1, :] + states[g][part, :]
                outs[g][run, s, 128:136, :] = before[s] + total[s]

    shape = (3, 2, 136, 128)
    return pl.pallas_call(
        body,
        out_shape=[jax.ShapeDtypeStruct(shape, F32)] * 2,
        in_specs=[SMEM] + [VMEM] * (held + 5 + len(given)),
        out_specs=[VMEM] * 2,
        scratch_shapes=[pltpu.VMEM((2 * many, rows + 8, 512), F32), pltpu.VMEM((both + 8, depth), BF)],
        cost_estimate=pl.CostEstimate(
            flops=32 * sum(x.shape[0] for x in xs) * w[0].size,
            transcendentals=0,
            bytes_accessed=4 * w[0].size,
        ),
        compiler_params=GRANT,
        name="piece_states",
    )(meta, *xs, w_step, *w, jump, rates, *given)


def joined(w_value, w_key, conv_value, conv_key):
    depth = w_value.shape[0]

    def body(v_ref, k_ref, cv_ref, ck_ref, out_ref):
        out_ref[:depth, :128] = v_ref[...]
        out_ref[:depth, 128:] = k_ref[...]
        out_ref[depth:, :128] = cv_ref[...]
        out_ref[depth:, 128:] = ck_ref[...]

    return pl.pallas_call(
        body,
        out_shape=jax.ShapeDtypeStruct((depth + conv_value.shape[0], 256), BF),
        in_specs=[VMEM] * 4,
        out_specs=VMEM,
        compiler_params=GRANT,
        name="joined",
    )(w_value, w_key, conv_value, conv_key)


def terms(step_bias, decay_rate, new_step, new_value, new_key, new_query, new_gate, read_gain):
    def body(b_ref, r_ref, n_ref, v_ref, k_ref, q_ref, g_ref, gain_ref, out_ref, query_ref):
        lane = lax.broadcasted_iota(jnp.int32, (1, 128), 1)

        def spread(a, b):
            return jnp.where(lane < HEAD_DIM, a, b)

        query = q_ref[...].astype(F32)
        query_ref[...] = query
        value, key, gate = (r[...].astype(F32) for r in (v_ref, k_ref, g_ref))
        match = jnp.sum(key * query, axis=1, keepdims=True)
        gates = gate / (1.0 + jnp.exp(-gate))
        rate = spread(r_ref[0], r_ref[1])
        for s in range(2):
            size = softplus(spread(n_ref[s, 0] + b_ref[0], n_ref[s, 1] + b_ref[1]))
            out_ref[s : s + 1, :] = jnp.exp(-rate * size)
            out_ref[2 + s : 3 + s, :] = size * match[s : s + 1, :] * value[s : s + 1, :]
        out_ref[4:6, :] = gates
        out_ref[6:7, :] = gain_ref[...].astype(F32)
        out_ref[7:8, :] = jnp.zeros((1, 128), F32)

    return pl.pallas_call(
        body,
        out_shape=[jax.ShapeDtypeStruct((8, 128), F32), jax.ShapeDtypeStruct((2, 128), F32)],
        in_specs=[SMEM] * 3 + [VMEM] * 5,
        out_specs=[VMEM] * 2,
        compiler_params=GRANT,
        name="terms",
    )(step_bias, decay_rate, new_step, new_value, new_key, new_query, new_gate, read_gain.reshape(1, 128))


def packed(meta, own, got, query, sp_count, chips):
    share = HEAD_DIM // sp_count

    def body(m_ref, a_ref, b_ref, q_ref, out_ref):
        def put(row, value):
            out_ref[:, row : row + 1, :] = jnp.broadcast_to(value[None], (sp_count, 1, 128))

        low = m_ref[1] == 0
        late = m_ref[0] < chips // 2
        lane = lax.broadcasted_iota(jnp.int32, (1, 128), 1)
        left = jnp.zeros((1, 128), F32)
        for s in range(2):
            mine = [a_ref[r, s, 128:130, :] for r in range(3)]
            theirs = [b_ref[r, s, 130:132, :] for r in range(3)]
            d1, d2, d3 = (jnp.where(low, m, t) for m, t in zip(mine, theirs))
            u1, u2, u3 = (jnp.where(low, t, m) for m, t in zip(mine, theirs))
            last = d3 + u3
            after_u1 = d2 + jnp.where(late, last, 0.0)
            after_d1 = after_u1 + u1
            after_u3 = jnp.where(late, d2, after_d1 + d1)
            after_d3 = after_u3 + u3
            after_u2 = after_d1 + d1 + jnp.where(late, 0.0, last)
            total = after_u2 + u2
            for e in range(2):
                left = jnp.where(lane == 2 * s + e, total[e : e + 1, :], left)
            down = [jnp.exp(v) for v in (after_d1, jnp.zeros_like(d2), after_d3)]
            up = [jnp.exp(v) for v in (after_u1, after_u2, after_u3)]
            reads = []
            for e in range(2):
                state = jnp.zeros((64, 128), F32)
                for r in range(3):
                    part = slice(64 * e, 64 * e + 64)
                    scale_a = jnp.where(low, down[r], up[r])[e : e + 1, :]
                    scale_b = jnp.where(low, up[r], down[r])[e : e + 1, :]
                    state = state + a_ref[r, s, part, :] * scale_a + b_ref[r, s, part, :] * scale_b
                reads.append(jnp.sum(state * q_ref[s : s + 1, :], axis=1).reshape(1, 64))
                cut = state.astype(BF).reshape(sp_count, share, 128)
                out_ref[:, 4 * s + 2 * e : 4 * s + 2 * e + share, :] = cut
            read = jnp.concatenate(reads, axis=1)
            high, low_part = halves(read)
            put(8 + s, high)
            put(10 + s, low_part)
        for k in range(3):
            part = left.astype(BF)
            left = left - part.astype(F32)
            put(12 + k, part)
        put(15, jnp.zeros((1, 128), BF))

    return pl.pallas_call(
        body,
        out_shape=jax.ShapeDtypeStruct((sp_count, 16, 128), BF),
        in_specs=[SMEM] + [VMEM] * 3,
        out_specs=VMEM,
        compiler_params=GRANT,
        name="packed",
    )(meta, own, got, query)


def finished(meta, got, fixed):
    sp_count = got.shape[0]

    def body(m_ref, got_ref, fix_ref, state_out, read_out):
        blocks = [got_ref[j].astype(F32) for j in range(sp_count)]
        decay = jnp.concatenate([g[12:13] + g[13:14] + g[14:15] for g in blocks], axis=0)
        i = lax.broadcasted_iota(jnp.int32, (sp_count, sp_count), 0)
        j = lax.broadcasted_iota(jnp.int32, (sp_count, sp_count), 1)
        after = jnp.where(j > i, 1.0, 0.0)
        fade = jnp.exp(mm(after, decay, ((1,), (0,)), lax.Precision.HIGHEST))
        one = [jnp.broadcast_to(fade[:, i : i + 1], (sp_count, 128)) for i in range(4)]
        lane = lax.broadcasted_iota(jnp.int32, (sp_count, 128), 1)
        both = [jnp.where(lane < HEAD_DIM, one[2 * s], one[2 * s + 1]) for s in range(2)]
        row = lax.broadcasted_iota(jnp.int32, (8, 128), 0)
        total = [jnp.zeros((8, 128), F32)] * 2
        for j, g in enumerate(blocks):
            a, b, c, d = (v[j : j + 1] for v in one)
            scale = jnp.where(row < 4, jnp.where(row < 2, a, b), jnp.where(row < 6, c, d))
            total[0] = total[0] + g[:8] * scale
            total[1] = total[1] + g[8:] * jnp.where(row % 2 == 0, both[0][j : j + 1], both[1][j : j + 1])
        total = jnp.concatenate(total, axis=0)
        for s in range(2):
            for h in range(2):
                state_out[s, h] = total[4 * s + 2 * h : 4 * s + 2 * h + 2].astype(BF)
        read = total[8:10] + total[10:12]
        gated = (fix_ref[0:2] * read + fix_ref[2:4]) * fix_ref[4:6]
        mean = jnp.mean(gated * gated, axis=1, keepdims=True)
        out = gated * lax.rsqrt(mean + EPSILON) * fix_ref[6:7]
        out = jnp.concatenate([out, jnp.zeros((6, 128), F32)], axis=0)
        out = pltpu.roll(out, m_ref[2], 1)
        for s in range(2):
            for h in range(2):
                read_out[s, h : h + 1, :] = out[s : s + 1, 64 * h : 64 * h + 2].astype(BF)

    return pl.pallas_call(
        body,
        out_shape=[jax.ShapeDtypeStruct((2, 2, 2, 128), BF), jax.ShapeDtypeStruct((2, 2, 2), BF)],
        in_specs=[SMEM, VMEM, VMEM],
        out_specs=[VMEM] * 2,
        compiler_params=GRANT,
        name="finished",
    )(meta, got, fixed)


def per_device(
    hidden_in, w_value, w_key, w_step, conv_value, conv_key, step_bias, decay_rate, decay_jump,
    new_value, new_key, new_query, new_gate, new_step, read_gain,
):
    sp_count, y_count, c_count = (lax.axis_size(a) for a in ("sp", "y", "c"))
    sp, y, c = (lax.axis_index(a) for a in ("sp", "y", "c"))
    tp_count = y_count * c_count
    count = sp_count * tp_count
    rows, width = hidden_in.shape[1:]
    heads = step_bias.shape[0]
    share = HEAD_DIM // sp_count
    half = y_count // 2

    def swap(v):
        return lax.ppermute(v, "c", [(0, 1), (1, 0)])

    def onward(v):
        pairs = []
        for i in range(y_count):
            pairs.append((2 * i, 2 * ((i + 1) % y_count)))
            pairs.append((2 * i + 1, 2 * ((i - 1) % y_count) + 1))
        return lax.ppermute(v, ("y", "c"), pairs)

    meta = jnp.stack([y, c, (128 - sp * share) % 128]).astype(jnp.int32)

    x = hidden_in.reshape(2 * rows, width)
    ends = hidden_in[:, rows - 4 :, :].reshape(8, width)
    ends = lax.ppermute(ends, ("sp", "y", "c"), [(i, i + 1) for i in range(count - 1)])
    a = [x, onward(x)]
    first = jnp.concatenate([x, ends], axis=0)
    b = [jnp.concatenate([swap(first), ends], axis=0)]
    b.append(onward(b[0]))

    w_own = joined(w_value, w_key, conv_value, conv_key)
    w_both = w_own, swap(w_own)
    pair = lax.dynamic_slice_in_dim(w_step.T, y * 2 * heads, 2 * heads, 0)
    pair = jnp.where(c == 0, pair, jnp.roll(pair, heads, axis=0))
    w_steps = jnp.pad(pair, ((0, 8 - 2 * heads), (0, 0)))
    rates = jnp.broadcast_to(jnp.stack([step_bias, decay_rate])[:, :, None], (2, heads, 128))
    jump = jnp.concatenate([decay_jump.transpose(0, 2, 1), rates], axis=2)
    jump = jnp.concatenate([jump, swap(jump)], axis=1)
    jump = jnp.pad(jump, ((0, 0), (0, 8 - 2 * heads), (0, 0)))
    rates = jump[:, :, tp_count * rows :]
    jump = jump[:, :, : tp_count * rows].reshape(2, 8, tp_count, rows).transpose(2, 1, 0, 3)
    jump = jump.reshape(tp_count, 8, 2 * rows)

    def add(runs, xs, halo, far, end):
        return piece_states(meta, xs, halo, far, end, w_steps, w_both, jump, rates, runs, rows, y_count)

    runs = add(None, [first], None, 0, False)
    for s in range(1, half):
        a.append(onward(a[s]))
        if s + 1 < half:
            b.append(onward(b[s]))
        runs = add(runs, [a[s], b[s]], None, s, False)

    fixed, query = terms(step_bias, decay_rate, new_step, new_value, new_key, new_query, new_gate, read_gain)
    runs, fixed, query = lax.optimization_barrier((runs, fixed, query))
    last = onward(b[half - 1][2 * rows + 8 :])
    own, other = add(runs, [a[half]], last, half, True)
    sent = packed(meta, own, swap(other), query, sp_count, y_count)
    got = lax.all_to_all(sent, "sp", 0, 0, tiled=True)
    return tuple(finished(meta, got, fixed))


def solution(mesh):
    tp = ("y", "c")
    chips = Mesh(mesh.devices.reshape(mesh.shape["sp"], mesh.shape["tp"] // 2, 2), ("sp", *tp))

    return jax.shard_map(
        per_device,
        mesh=chips,
        in_specs=(
            P(None, ("sp", *tp), None), P(None, tp), P(None, tp), P(), P(None, tp), P(None, tp), P(tp), P(tp),
            P(None, "sp", tp), P(None, tp), P(None, tp), P(None, tp), P(None, tp), P(None, tp), P(tp),
        ),
        out_specs=(P(None, tp, "sp", None), P(None, tp, "sp")),
        check_vma=False,
    )
```

```python
import jax
import jax.numpy as jnp
from jax import lax
from jax.experimental import pallas as pl
from jax.experimental.pallas import tpu as pltpu
from jax.sharding import Mesh
from jax.sharding import PartitionSpec as P

HEAD_DIM = 64
EPSILON = 1e-05
BF = jnp.bfloat16
F32 = jnp.float32
GRANT = pltpu.CompilerParams(vmem_limit_bytes=16 * 1024 * 1024)
VMEM = pl.BlockSpec(memory_space=pltpu.VMEM)
SMEM = pl.BlockSpec(memory_space=pltpu.SMEM)


def mm(a, b, dims, precision=None):
    return lax.dot_general(a, b, (dims, ((), ())), preferred_element_type=F32, precision=precision)


def halves(v):
    high = v.astype(BF)
    return high, (v - high.astype(F32)).astype(BF)


def product(a, b):
    (ah, al), (bh, bl) = halves(a), halves(b)
    dims = ((0,), (0,))
    return mm(ah, bh, dims) + (mm(al, bh, dims) + mm(ah, bl, dims))


def softplus(v):
    return jnp.maximum(v, 0.0) + jnp.log1p(jnp.exp(-jnp.abs(v)))


def piece_states(meta, xs, halo, far, end, w_step, w, jump, rates, runs, groups, rows, chips):
    many, both = len(xs), 2 * rows
    depth = w[0].shape[0] - 4
    given = [] if runs is None else list(runs)
    xs = xs if halo is None else [*xs, halo]
    held, wide = len(xs), len(groups)

    def body(m_ref, *refs):
        x_refs = list(refs[:held])
        s_ref, j_ref, r_ref, *w_refs = refs[held : held + 3 + wide]
        ins = refs[held + 3 + wide : held + 3 + wide + len(given)]
        *outs, ext, full = refs[held + 3 + wide + len(given) :]
        if held > many:
            full[:both, :] = x_refs[0][...]
            full[both:, :] = x_refs[1][...]
            x_refs = [full]
        y, c = m_ref[0], m_ref[1]
        low = c == 0
        away = jnp.where(low, y - far, y + far)
        wrapped = jnp.logical_or(away < 0, away >= chips)
        chip = jnp.where(away < 0, away + chips, jnp.where(away >= chips, away - chips, away))
        run = 2 if end else jnp.where(wrapped, 1, 0)
        place = (2 * chip + c, 2 * chip + 1 - c)
        for g in range(wide):
            if given:
                outs[g][...] = ins[g][...]
            else:
                outs[g][...] = jnp.zeros(outs[g].shape, F32)

        lane = lax.broadcasted_iota(jnp.int32, (8, both), 1)
        i = lax.broadcasted_iota(jnp.int32, (both, both), 0)
        j = lax.broadcasted_iota(jnp.int32, (both, both), 1)
        below = jnp.where(jnp.logical_and(i > j, (i >= rows) == (j >= rows)), 1.0, 0.0)
        sizes, afters, sums = [], [], []
        for n in range(many):
            step = mm(s_ref[...], x_refs[n][...], ((1,), (1,))).astype(BF).astype(F32)[:, :both]
            size = softplus(step + r_ref[0][:, 0:1])
            decay = j_ref[place[n]] - r_ref[1][:, 0:1] * size
            sizes.append(size)
            afters.append(mm(decay, below, ((1,), (0,)), lax.Precision.HIGHEST))
            sums.append([
                jnp.sum(jnp.where(lane < rows, decay, 0.0), axis=1, keepdims=True),
                jnp.sum(jnp.where(lane < rows, 0.0, decay), axis=1, keepdims=True),
            ])
        total = [sum(v[s] for v in sums) for s in range(2)]
        before = [outs[0][run, s, 128:136, :] for s in range(2)]
        lead = [jnp.where(low, v[:, 0:1], 0.0) for v in before]
        lifts = []
        for n in range(many):
            more = list(lead)
            if many == 2:
                first = low if n == 0 else jnp.logical_not(low)
                more = [more[s] + jnp.where(first, sums[1 - n][s], 0.0) for s in range(2)]
            weight = sizes[n] * jnp.exp(afters[n] + jnp.where(lane < rows, more[0], more[1]))
            weight = jnp.concatenate([weight, jnp.zeros((8, 256 - both), F32)], axis=1)
            lifts.append(jnp.transpose(weight))

        taps = jnp.concatenate([r[depth : depth + 4, :] for r in w_refs], axis=1).astype(F32)
        for g, r in enumerate(w_refs):
            cols = slice(256 * g, 256 * g + 256)
            p = [mm(v[...], r[:depth, :], ((1,), (0,))).astype(BF).astype(F32) for v in x_refs]
            for n in range(many):
                base = both + 8 * (many - 1 - n)
                for s in range(2):
                    ext[2 * n + s, 4:8, cols] = p[-1][base + 4 * s : base + 4 * s + 4, :]
                    ext[2 * n + s, 8 : 8 + rows, cols] = p[n][s * rows : (s + 1) * rows, :]
        for s in range(2):
            states = [jnp.zeros((128, 128), F32)] * wide
            for n in range(many):
                mixed = ext[2 * n + s, 5 : 5 + rows, :] * taps[0:1, :]
                for k in range(1, 4):
                    mixed = mixed + ext[2 * n + s, 5 + k : 5 + k + rows, :] * taps[k : k + 1, :]
                mixed = mixed / (1.0 + jnp.exp(-mixed))
                lift = lifts[n][s * rows : (s + 1) * rows, :]
                for g in range(wide):
                    head = 2 * groups[g]
                    parts = [
                        mixed[:, 256 * g + 64 * e : 256 * g + 64 * e + 64] * lift[:, head + e : head + e + 1]
                        for e in range(2)
                    ]
                    values = jnp.concatenate(parts, axis=1)
                    keys = mixed[:, 256 * g + 128 : 256 * g + 256]
                    states[g] = states[g] + product(values, keys)
            fade = jnp.where(low, 1.0, jnp.exp(total[s]))
            for g in range(wide):
                for e in range(2):
                    head = 2 * groups[g] + e
                    part = slice(64 * e, 64 * e + 64)
                    old = outs[g][run, s, part, :]
                    outs[g][run, s, part, :] = old * fade[head : head + 1, :] + states[g][part, :]
                outs[g][run, s, 128:136, :] = before[s] + total[s]

    shape = (3, 2, 136, 128)
    return pl.pallas_call(
        body,
        out_shape=[jax.ShapeDtypeStruct(shape, F32)] * wide,
        in_specs=[SMEM] + [VMEM] * (held + 3 + wide + len(given)),
        out_specs=[VMEM] * wide,
        scratch_shapes=[pltpu.VMEM((2 * many, rows + 8, 256 * wide), F32), pltpu.VMEM((both + 8, depth), BF)],
        cost_estimate=pl.CostEstimate(
            flops=32 * sum(x.shape[0] for x in xs) * w[0].size,
            transcendentals=0,
            bytes_accessed=4 * w[0].size,
        ),
        compiler_params=GRANT,
        name="piece_states",
    )(meta, *xs, w_step, jump, rates, *w, *given)


def joined(w_value, w_key, conv_value, conv_key):
    depth = w_value.shape[0]

    def body(v_ref, k_ref, cv_ref, ck_ref, out_ref):
        out_ref[:depth, :128] = v_ref[...]
        out_ref[:depth, 128:] = k_ref[...]
        out_ref[depth:, :128] = cv_ref[...]
        out_ref[depth:, 128:] = ck_ref[...]

    return pl.pallas_call(
        body,
        out_shape=jax.ShapeDtypeStruct((depth + conv_value.shape[0], 256), BF),
        in_specs=[VMEM] * 4,
        out_specs=VMEM,
        compiler_params=GRANT,
        name="joined",
    )(w_value, w_key, conv_value, conv_key)


def terms(step_bias, decay_rate, new_step, new_value, new_key, new_query, new_gate, read_gain):
    def body(b_ref, r_ref, n_ref, v_ref, k_ref, q_ref, g_ref, gain_ref, out_ref, query_ref):
        lane = lax.broadcasted_iota(jnp.int32, (1, 128), 1)

        def spread(a, b):
            return jnp.where(lane < HEAD_DIM, a, b)

        query = q_ref[...].astype(F32)
        query_ref[...] = query
        value, key, gate = (r[...].astype(F32) for r in (v_ref, k_ref, g_ref))
        match = jnp.sum(key * query, axis=1, keepdims=True)
        gates = gate / (1.0 + jnp.exp(-gate))
        rate = spread(r_ref[0], r_ref[1])
        for s in range(2):
            size = softplus(spread(n_ref[s, 0] + b_ref[0], n_ref[s, 1] + b_ref[1]))
            out_ref[s : s + 1, :] = jnp.exp(-rate * size)
            out_ref[2 + s : 3 + s, :] = size * match[s : s + 1, :] * value[s : s + 1, :]
        out_ref[4:6, :] = gates
        out_ref[6:7, :] = gain_ref[...].astype(F32)
        out_ref[7:8, :] = jnp.zeros((1, 128), F32)

    return pl.pallas_call(
        body,
        out_shape=[jax.ShapeDtypeStruct((8, 128), F32), jax.ShapeDtypeStruct((2, 128), F32)],
        in_specs=[SMEM] * 3 + [VMEM] * 5,
        out_specs=[VMEM] * 2,
        compiler_params=GRANT,
        name="terms",
    )(step_bias, decay_rate, new_step, new_value, new_key, new_query, new_gate, read_gain.reshape(1, 128))


def packed(meta, own, got, query, sp_count, chips):
    share = HEAD_DIM // sp_count

    def body(m_ref, a_ref, b_ref, q_ref, out_ref):
        def put(row, value):
            out_ref[:, row : row + 1, :] = jnp.broadcast_to(value[None], (sp_count, 1, 128))

        low = m_ref[1] == 0
        late = m_ref[0] < chips // 2
        lane = lax.broadcasted_iota(jnp.int32, (1, 128), 1)
        left = jnp.zeros((1, 128), F32)
        for s in range(2):
            mine = [a_ref[r, s, 128:130, :] for r in range(3)]
            theirs = [b_ref[r, s, 130:132, :] for r in range(3)]
            d1, d2, d3 = (jnp.where(low, m, t) for m, t in zip(mine, theirs))
            u1, u2, u3 = (jnp.where(low, t, m) for m, t in zip(mine, theirs))
            last = d3 + u3
            after_u1 = d2 + jnp.where(late, last, 0.0)
            after_d1 = after_u1 + u1
            after_u3 = jnp.where(late, d2, after_d1 + d1)
            after_d3 = after_u3 + u3
            after_u2 = after_d1 + d1 + jnp.where(late, 0.0, last)
            total = after_u2 + u2
            for e in range(2):
                left = jnp.where(lane == 2 * s + e, total[e : e + 1, :], left)
            down = [jnp.exp(v) for v in (after_d1, jnp.zeros_like(d2), after_d3)]
            up = [jnp.exp(v) for v in (after_u1, after_u2, after_u3)]
            reads = []
            for e in range(2):
                state = jnp.zeros((64, 128), F32)
                for r in range(3):
                    part = slice(64 * e, 64 * e + 64)
                    scale_a = jnp.where(low, down[r], up[r])[e : e + 1, :]
                    scale_b = jnp.where(low, up[r], down[r])[e : e + 1, :]
                    state = state + a_ref[r, s, part, :] * scale_a + b_ref[r, s, part, :] * scale_b
                reads.append(jnp.sum(state * q_ref[s : s + 1, :], axis=1).reshape(1, 64))
                cut = state.astype(BF).reshape(sp_count, share, 128)
                out_ref[:, 4 * s + 2 * e : 4 * s + 2 * e + share, :] = cut
            read = jnp.concatenate(reads, axis=1)
            high, low_part = halves(read)
            put(8 + s, high)
            put(10 + s, low_part)
        for k in range(3):
            part = left.astype(BF)
            left = left - part.astype(F32)
            put(12 + k, part)
        put(15, jnp.zeros((1, 128), BF))

    return pl.pallas_call(
        body,
        out_shape=jax.ShapeDtypeStruct((sp_count, 16, 128), BF),
        in_specs=[SMEM] + [VMEM] * 3,
        out_specs=VMEM,
        compiler_params=GRANT,
        name="packed",
    )(meta, own, got, query)


def finished(meta, got, fixed):
    sp_count = got.shape[0]

    def body(m_ref, got_ref, fix_ref, state_out, read_out):
        blocks = [got_ref[j].astype(F32) for j in range(sp_count)]
        decay = jnp.concatenate([g[12:13] + g[13:14] + g[14:15] for g in blocks], axis=0)
        i = lax.broadcasted_iota(jnp.int32, (sp_count, sp_count), 0)
        j = lax.broadcasted_iota(jnp.int32, (sp_count, sp_count), 1)
        after = jnp.where(j > i, 1.0, 0.0)
        fade = jnp.exp(mm(after, decay, ((1,), (0,)), lax.Precision.HIGHEST))
        one = [jnp.broadcast_to(fade[:, i : i + 1], (sp_count, 128)) for i in range(4)]
        lane = lax.broadcasted_iota(jnp.int32, (sp_count, 128), 1)
        both = [jnp.where(lane < HEAD_DIM, one[2 * s], one[2 * s + 1]) for s in range(2)]
        row = lax.broadcasted_iota(jnp.int32, (8, 128), 0)
        total = [jnp.zeros((8, 128), F32)] * 2
        for j, g in enumerate(blocks):
            a, b, c, d = (v[j : j + 1] for v in one)
            scale = jnp.where(row < 4, jnp.where(row < 2, a, b), jnp.where(row < 6, c, d))
            total[0] = total[0] + g[:8] * scale
            total[1] = total[1] + g[8:] * jnp.where(row % 2 == 0, both[0][j : j + 1], both[1][j : j + 1])
        total = jnp.concatenate(total, axis=0)
        for s in range(2):
            for h in range(2):
                state_out[s, h] = total[4 * s + 2 * h : 4 * s + 2 * h + 2].astype(BF)
        read = total[8:10] + total[10:12]
        gated = (fix_ref[0:2] * read + fix_ref[2:4]) * fix_ref[4:6]
        mean = jnp.mean(gated * gated, axis=1, keepdims=True)
        out = gated * lax.rsqrt(mean + EPSILON) * fix_ref[6:7]
        out = jnp.concatenate([out, jnp.zeros((6, 128), F32)], axis=0)
        out = pltpu.roll(out, m_ref[2], 1)
        for s in range(2):
            for h in range(2):
                read_out[s, h : h + 1, :] = out[s : s + 1, 64 * h : 64 * h + 2].astype(BF)

    return pl.pallas_call(
        body,
        out_shape=[jax.ShapeDtypeStruct((2, 2, 2, 128), BF), jax.ShapeDtypeStruct((2, 2, 2), BF)],
        in_specs=[SMEM, VMEM, VMEM],
        out_specs=[VMEM] * 2,
        compiler_params=GRANT,
        name="finished",
    )(meta, got, fixed)


def per_device(
    hidden_in, w_value, w_key, w_step, conv_value, conv_key, step_bias, decay_rate, decay_jump,
    new_value, new_key, new_query, new_gate, new_step, read_gain,
):
    sp_count, y_count, c_count = (lax.axis_size(a) for a in ("sp", "y", "c"))
    sp, y, c = (lax.axis_index(a) for a in ("sp", "y", "c"))
    tp_count = y_count * c_count
    count = sp_count * tp_count
    rows, width = hidden_in.shape[1:]
    heads = step_bias.shape[0]
    share = HEAD_DIM // sp_count
    half = y_count // 2

    def swap(v):
        return lax.ppermute(v, "c", [(0, 1), (1, 0)])

    def onward(v):
        pairs = []
        for i in range(y_count):
            pairs.append((2 * i, 2 * ((i + 1) % y_count)))
            pairs.append((2 * i + 1, 2 * ((i - 1) % y_count) + 1))
        return lax.ppermute(v, ("y", "c"), pairs)

    meta = jnp.stack([y, c, (128 - sp * share) % 128]).astype(jnp.int32)

    x = hidden_in.reshape(2 * rows, width)
    ends = hidden_in[:, rows - 4 :, :].reshape(8, width)
    ends = lax.ppermute(ends, ("sp", "y", "c"), [(i, i + 1) for i in range(count - 1)])
    a = [x, onward(x)]
    first = jnp.concatenate([x, ends], axis=0)
    b = [swap(first)]
    b.append(jnp.concatenate([onward(b[0]), onward(ends)], axis=0))

    w_own = joined(w_value, w_key, conv_value, conv_key)
    w_both = w_own, swap(w_own)
    pair = lax.dynamic_slice_in_dim(w_step.T, y * 2 * heads, 2 * heads, 0)
    pair = jnp.where(c == 0, pair, jnp.roll(pair, heads, axis=0))
    w_steps = jnp.pad(pair, ((0, 8 - 2 * heads), (0, 0)))
    rates = jnp.broadcast_to(jnp.stack([step_bias, decay_rate])[:, :, None], (2, heads, 128))
    jump = jnp.concatenate([decay_jump.transpose(0, 2, 1), rates], axis=2)
    jump = jnp.concatenate([jump, swap(jump)], axis=1)
    jump = jnp.pad(jump, ((0, 0), (0, 8 - 2 * heads), (0, 0)))
    rates = jump[:, :, tp_count * rows :]
    jump = jump[:, :, : tp_count * rows].reshape(2, 8, tp_count, rows).transpose(2, 1, 0, 3)
    jump = jump.reshape(tp_count, 8, 2 * rows)

    def add(runs, xs, halo, far, end, groups=(0, 1)):
        w = [w_both[g] for g in groups]
        runs = runs and [runs[g] for g in groups]
        return piece_states(meta, xs, halo, far, end, w_steps, w, jump, rates, runs, groups, rows, y_count)

    runs = add(None, [first], None, 0, False)
    for s in range(1, half):
        a.append(onward(a[s]))
        if s + 1 < half:
            b.append(onward(b[s]))
        runs = add(runs, [a[s], b[s]], None, s, False)

    fixed, query = terms(step_bias, decay_rate, new_step, new_value, new_key, new_query, new_gate, read_gain)
    runs, fixed, query = lax.optimization_barrier((runs, fixed, query))
    last = onward(b[half - 1][2 * rows + 8 :])
    (other,) = add(runs, [a[half]], last, half, True, (1,))
    other = swap(other)
    (own,) = add(runs, [a[half]], last, half, True, (0,))
    sent = packed(meta, own, other, query, sp_count, y_count)
    got = lax.all_to_all(sent, "sp", 0, 0, tiled=True)
    return tuple(finished(meta, got, fixed))


def solution(mesh):
    tp = ("y", "c")
    chips = Mesh(mesh.devices.reshape(mesh.shape["sp"], mesh.shape["tp"] // 2, 2), ("sp", *tp))

    return jax.shard_map(
        per_device,
        mesh=chips,
        in_specs=(
            P(None, ("sp", *tp), None), P(None, tp), P(None, tp), P(), P(None, tp), P(None, tp), P(tp), P(tp),
            P(None, "sp", tp), P(None, tp), P(None, tp), P(None, tp), P(None, tp), P(None, tp), P(tp),
        ),
        out_specs=(P(None, tp, "sp", None), P(None, tp, "sp")),
        check_vma=False,
    )
```

```python
import jax
import jax.numpy as jnp
from jax import lax
from jax.experimental import pallas as pl
from jax.experimental.pallas import tpu as pltpu
from jax.sharding import Mesh
from jax.sharding import PartitionSpec as P

HEAD_DIM = 64
EPSILON = 1e-05
BF = jnp.bfloat16
F32 = jnp.float32
GRANT = pltpu.CompilerParams(vmem_limit_bytes=16 * 1024 * 1024)
VMEM = pl.BlockSpec(memory_space=pltpu.VMEM)
SMEM = pl.BlockSpec(memory_space=pltpu.SMEM)


def mm(a, b, dims, precision=None):
    return lax.dot_general(a, b, (dims, ((), ())), preferred_element_type=F32, precision=precision)


def halves(v):
    high = v.astype(BF)
    return high, (v - high.astype(F32)).astype(BF)


def product(a, b):
    (ah, al), (bh, bl) = halves(a), halves(b)
    dims = ((0,), (0,))
    return mm(ah, bh, dims) + (mm(al, bh, dims) + mm(ah, bl, dims))


def softplus(v):
    return jnp.maximum(v, 0.0) + jnp.log1p(jnp.exp(-jnp.abs(v)))


def piece_states(meta, xs, halo, far, end, w_step, w, jump, rates, runs, rows, chips):
    many, both = len(xs), 2 * rows
    depth = w[0].shape[0] - 4
    given = [] if runs is None else list(runs)
    xs = xs if halo is None else [*xs, halo]
    held = len(xs)

    def body(m_ref, *refs):
        x_refs = list(refs[:held])
        s_ref, wa_ref, wb_ref, j_ref, r_ref = refs[held : held + 5]
        ins = refs[held + 5 : held + 5 + len(given)]
        own_out, other_out, ext, full = refs[held + 5 + len(given) :]
        if held > many:
            full[:both, :] = x_refs[0][...]
            full[both:, :] = x_refs[1][...]
            x_refs = [full]
        outs = (own_out, other_out)
        y, c = m_ref[0], m_ref[1]
        low = c == 0
        away = jnp.where(low, y - far, y + far)
        wrapped = jnp.logical_or(away < 0, away >= chips)
        chip = jnp.where(away < 0, away + chips, jnp.where(away >= chips, away - chips, away))
        run = 2 if end else jnp.where(wrapped, 1, 0)
        place = (2 * chip + c, 2 * chip + 1 - c)
        for g in range(2):
            if given:
                outs[g][...] = ins[g][...]
            else:
                outs[g][...] = jnp.zeros(outs[g].shape, F32)

        lane = lax.broadcasted_iota(jnp.int32, (8, both), 1)
        i = lax.broadcasted_iota(jnp.int32, (both, both), 0)
        j = lax.broadcasted_iota(jnp.int32, (both, both), 1)
        below = jnp.where(jnp.logical_and(i > j, (i >= rows) == (j >= rows)), 1.0, 0.0)
        sizes, afters, sums = [], [], []
        for n in range(many):
            step = mm(s_ref[...], x_refs[n][...], ((1,), (1,))).astype(BF).astype(F32)[:, :both]
            size = softplus(step + r_ref[0][:, 0:1])
            decay = j_ref[place[n]] - r_ref[1][:, 0:1] * size
            sizes.append(size)
            afters.append(mm(decay, below, ((1,), (0,)), lax.Precision.HIGHEST))
            sums.append([
                jnp.sum(jnp.where(lane < rows, decay, 0.0), axis=1, keepdims=True),
                jnp.sum(jnp.where(lane < rows, 0.0, decay), axis=1, keepdims=True),
            ])
        total = [sum(v[s] for v in sums) for s in range(2)]
        before = [own_out[run, s, 128:136, :] for s in range(2)]
        lead = [jnp.where(low, v[:, 0:1], 0.0) for v in before]
        lifts = []
        for n in range(many):
            more = list(lead)
            if many == 2:
                first = low if n == 0 else jnp.logical_not(low)
                more = [more[s] + jnp.where(first, sums[1 - n][s], 0.0) for s in range(2)]
            weight = sizes[n] * jnp.exp(afters[n] + jnp.where(lane < rows, more[0], more[1]))
            weight = jnp.concatenate([weight, jnp.zeros((8, 256 - both), F32)], axis=1)
            lifts.append(jnp.transpose(weight))

        taps = jnp.concatenate([r[depth : depth + 4, :] for r in (wa_ref, wb_ref)], axis=1).astype(F32)
        for g, r in enumerate((wa_ref, wb_ref)):
            cols = slice(256 * g, 256 * g + 256)
            p = [mm(v[...], r[:depth, :], ((1,), (0,))).astype(BF).astype(F32) for v in x_refs]
            for n in range(many):
                base = both + 8 * (many - 1 - n)
                for s in range(2):
                    ext[2 * n + s, 4:8, cols] = p[-1][base + 4 * s : base + 4 * s + 4, :]
                    ext[2 * n + s, 8 : 8 + rows, cols] = p[n][s * rows : (s + 1) * rows, :]
        for s in range(2):
            states = [jnp.zeros((128, 128), F32)] * 2
            for n in range(many):
                mixed = ext[2 * n + s, 5 : 5 + rows, :] * taps[0:1, :]
                for k in range(1, 4):
                    mixed = mixed + ext[2 * n + s, 5 + k : 5 + k + rows, :] * taps[k : k + 1, :]
                mixed = mixed / (1.0 + jnp.exp(-mixed))
                lift = lifts[n][s * rows : (s + 1) * rows, :]
                for g in range(2):
                    parts = [
                        mixed[:, 256 * g + 64 * e : 256 * g + 64 * e + 64] * lift[:, 2 * g + e : 2 * g + e + 1]
                        for e in range(2)
                    ]
                    values = jnp.concatenate(parts, axis=1)
                    keys = mixed[:, 256 * g + 128 : 256 * g + 256]
                    states[g] = states[g] + product(values, keys)
            fade = jnp.where(low, 1.0, jnp.exp(total[s]))
            for g in range(2):
                for e in range(2):
                    part = slice(64 * e, 64 * e + 64)
                    old = outs[g][run, s, part, :]
                    outs[g][run, s, part, :] = old * fade[2 * g + e : 2 * g + e + 1, :] + states[g][part, :]
                outs[g][run, s, 128:136, :] = before[s] + total[s]

    shape = (3, 2, 136, 128)
    return pl.pallas_call(
        body,
        out_shape=[jax.ShapeDtypeStruct(shape, F32)] * 2,
        in_specs=[SMEM] + [VMEM] * (held + 5 + len(given)),
        out_specs=[VMEM] * 2,
        scratch_shapes=[pltpu.VMEM((2 * many, rows + 8, 512), F32), pltpu.VMEM((both + 8, depth), BF)],
        cost_estimate=pl.CostEstimate(
            flops=32 * sum(x.shape[0] for x in xs) * w[0].size,
            transcendentals=0,
            bytes_accessed=4 * w[0].size,
        ),
        compiler_params=GRANT,
        name="piece_states",
    )(meta, *xs, w_step, *w, jump, rates, *given)


def joined(w_value, w_key, conv_value, conv_key):
    depth = w_value.shape[0]

    def body(v_ref, k_ref, cv_ref, ck_ref, out_ref):
        out_ref[:depth, :128] = v_ref[...]
        out_ref[:depth, 128:] = k_ref[...]
        out_ref[depth:, :128] = cv_ref[...]
        out_ref[depth:, 128:] = ck_ref[...]

    return pl.pallas_call(
        body,
        out_shape=jax.ShapeDtypeStruct((depth + conv_value.shape[0], 256), BF),
        in_specs=[VMEM] * 4,
        out_specs=VMEM,
        compiler_params=GRANT,
        name="joined",
    )(w_value, w_key, conv_value, conv_key)


def stacked(*parts):
    counts = [v.shape[0] for v in parts]

    def body(*refs):
        start = 0
        for ref, count in zip(refs[:-1], counts):
            refs[-1][start : start + count, :] = ref[...]
            start += count

    return pl.pallas_call(
        body,
        out_shape=jax.ShapeDtypeStruct((sum(counts), parts[0].shape[1]), parts[0].dtype),
        in_specs=[VMEM] * len(parts),
        out_specs=VMEM,
        compiler_params=GRANT,
        name="stacked",
    )(*parts)


def terms(step_bias, decay_rate, new_step, new_value, new_key, new_query, new_gate, read_gain):
    def body(b_ref, r_ref, n_ref, v_ref, k_ref, q_ref, g_ref, gain_ref, out_ref, query_ref):
        lane = lax.broadcasted_iota(jnp.int32, (1, 128), 1)

        def spread(a, b):
            return jnp.where(lane < HEAD_DIM, a, b)

        query = q_ref[...].astype(F32)
        query_ref[...] = query
        value, key, gate = (r[...].astype(F32) for r in (v_ref, k_ref, g_ref))
        match = jnp.sum(key * query, axis=1, keepdims=True)
        gates = gate / (1.0 + jnp.exp(-gate))
        rate = spread(r_ref[0], r_ref[1])
        for s in range(2):
            size = softplus(spread(n_ref[s, 0] + b_ref[0], n_ref[s, 1] + b_ref[1]))
            out_ref[s : s + 1, :] = jnp.exp(-rate * size)
            out_ref[2 + s : 3 + s, :] = size * match[s : s + 1, :] * value[s : s + 1, :]
        out_ref[4:6, :] = gates
        out_ref[6:7, :] = gain_ref[...].astype(F32)
        out_ref[7:8, :] = jnp.zeros((1, 128), F32)

    return pl.pallas_call(
        body,
        out_shape=[jax.ShapeDtypeStruct((8, 128), F32), jax.ShapeDtypeStruct((2, 128), F32)],
        in_specs=[SMEM] * 3 + [VMEM] * 5,
        out_specs=[VMEM] * 2,
        compiler_params=GRANT,
        name="terms",
    )(step_bias, decay_rate, new_step, new_value, new_key, new_query, new_gate, read_gain.reshape(1, 128))


def packed(meta, own, got, query, sp_count, chips):
    share = HEAD_DIM // sp_count

    def body(m_ref, a_ref, b_ref, q_ref, out_ref):
        def put(row, value):
            out_ref[:, row : row + 1, :] = jnp.broadcast_to(value[None], (sp_count, 1, 128))

        low = m_ref[1] == 0
        late = m_ref[0] < chips // 2
        lane = lax.broadcasted_iota(jnp.int32, (1, 128), 1)
        left = jnp.zeros((1, 128), F32)
        for s in range(2):
            mine = [a_ref[r, s, 128:130, :] for r in range(3)]
            theirs = [b_ref[r, s, 130:132, :] for r in range(3)]
            d1, d2, d3 = (jnp.where(low, m, t) for m, t in zip(mine, theirs))
            u1, u2, u3 = (jnp.where(low, t, m) for m, t in zip(mine, theirs))
            last = d3 + u3
            after_u1 = d2 + jnp.where(late, last, 0.0)
            after_d1 = after_u1 + u1
            after_u3 = jnp.where(late, d2, after_d1 + d1)
            after_d3 = after_u3 + u3
            after_u2 = after_d1 + d1 + jnp.where(late, 0.0, last)
            total = after_u2 + u2
            for e in range(2):
                left = jnp.where(lane == 2 * s + e, total[e : e + 1, :], left)
            down = [jnp.exp(v) for v in (after_d1, jnp.zeros_like(d2), after_d3)]
            up = [jnp.exp(v) for v in (after_u1, after_u2, after_u3)]
            reads = []
            for e in range(2):
                state = jnp.zeros((64, 128), F32)
                for r in range(3):
                    part = slice(64 * e, 64 * e + 64)
                    scale_a = jnp.where(low, down[r], up[r])[e : e + 1, :]
                    scale_b = jnp.where(low, up[r], down[r])[e : e + 1, :]
                    state = state + a_ref[r, s, part, :] * scale_a + b_ref[r, s, part, :] * scale_b
                reads.append(jnp.sum(state * q_ref[s : s + 1, :], axis=1).reshape(1, 64))
                cut = state.astype(BF).reshape(sp_count, share, 128)
                out_ref[:, 4 * s + 2 * e : 4 * s + 2 * e + share, :] = cut
            read = jnp.concatenate(reads, axis=1)
            high, low_part = halves(read)
            put(8 + s, high)
            put(10 + s, low_part)
        for k in range(3):
            part = left.astype(BF)
            left = left - part.astype(F32)
            put(12 + k, part)
        put(15, jnp.zeros((1, 128), BF))

    return pl.pallas_call(
        body,
        out_shape=jax.ShapeDtypeStruct((sp_count, 16, 128), BF),
        in_specs=[SMEM] + [VMEM] * 3,
        out_specs=VMEM,
        compiler_params=GRANT,
        name="packed",
    )(meta, own, got, query)


def finished(meta, got, fixed):
    sp_count = got.shape[0]

    def body(m_ref, got_ref, fix_ref, state_out, read_out):
        blocks = [got_ref[j].astype(F32) for j in range(sp_count)]
        decay = jnp.concatenate([g[12:13] + g[13:14] + g[14:15] for g in blocks], axis=0)
        i = lax.broadcasted_iota(jnp.int32, (sp_count, sp_count), 0)
        j = lax.broadcasted_iota(jnp.int32, (sp_count, sp_count), 1)
        after = jnp.where(j > i, 1.0, 0.0)
        fade = jnp.exp(mm(after, decay, ((1,), (0,)), lax.Precision.HIGHEST))
        one = [jnp.broadcast_to(fade[:, i : i + 1], (sp_count, 128)) for i in range(4)]
        lane = lax.broadcasted_iota(jnp.int32, (sp_count, 128), 1)
        both = [jnp.where(lane < HEAD_DIM, one[2 * s], one[2 * s + 1]) for s in range(2)]
        row = lax.broadcasted_iota(jnp.int32, (8, 128), 0)
        total = [jnp.zeros((8, 128), F32)] * 2
        for j, g in enumerate(blocks):
            a, b, c, d = (v[j : j + 1] for v in one)
            scale = jnp.where(row < 4, jnp.where(row < 2, a, b), jnp.where(row < 6, c, d))
            total[0] = total[0] + g[:8] * scale
            total[1] = total[1] + g[8:] * jnp.where(row % 2 == 0, both[0][j : j + 1], both[1][j : j + 1])
        total = jnp.concatenate(total, axis=0)
        for s in range(2):
            for h in range(2):
                state_out[s, h] = total[4 * s + 2 * h : 4 * s + 2 * h + 2].astype(BF)
        read = total[8:10] + total[10:12]
        gated = (fix_ref[0:2] * read + fix_ref[2:4]) * fix_ref[4:6]
        mean = jnp.mean(gated * gated, axis=1, keepdims=True)
        out = gated * lax.rsqrt(mean + EPSILON) * fix_ref[6:7]
        out = jnp.concatenate([out, jnp.zeros((6, 128), F32)], axis=0)
        out = pltpu.roll(out, m_ref[2], 1)
        for s in range(2):
            for h in range(2):
                read_out[s, h : h + 1, :] = out[s : s + 1, 64 * h : 64 * h + 2].astype(BF)

    return pl.pallas_call(
        body,
        out_shape=[jax.ShapeDtypeStruct((2, 2, 2, 128), BF), jax.ShapeDtypeStruct((2, 2, 2), BF)],
        in_specs=[SMEM, VMEM, VMEM],
        out_specs=[VMEM] * 2,
        compiler_params=GRANT,
        name="finished",
    )(meta, got, fixed)


def per_device(
    hidden_in, w_value, w_key, w_step, conv_value, conv_key, step_bias, decay_rate, decay_jump,
    new_value, new_key, new_query, new_gate, new_step, read_gain,
):
    sp_count, y_count, c_count = (lax.axis_size(a) for a in ("sp", "y", "c"))
    sp, y, c = (lax.axis_index(a) for a in ("sp", "y", "c"))
    tp_count = y_count * c_count
    count = sp_count * tp_count
    rows, width = hidden_in.shape[1:]
    heads = step_bias.shape[0]
    share = HEAD_DIM // sp_count
    half = y_count // 2

    def swap(v):
        return lax.ppermute(v, "c", [(0, 1), (1, 0)])

    def onward(v):
        pairs = []
        for i in range(y_count):
            pairs.append((2 * i, 2 * ((i + 1) % y_count)))
            pairs.append((2 * i + 1, 2 * ((i - 1) % y_count) + 1))
        return lax.ppermute(v, ("y", "c"), pairs)

    meta = jnp.stack([y, c, (128 - sp * share) % 128]).astype(jnp.int32)

    x = hidden_in.reshape(2 * rows, width)
    ends = hidden_in[:, rows - 4 :, :].reshape(8, width)
    ends = lax.ppermute(ends, ("sp", "y", "c"), [(i, i + 1) for i in range(count - 1)])
    a = [x, onward(x)]
    first = jnp.concatenate([x, ends], axis=0)
    b = [stacked(swap(first), ends)]
    b.append(onward(b[0]))

    w_own = joined(w_value, w_key, conv_value, conv_key)
    w_both = w_own, stacked(swap(w_own))
    pair = lax.dynamic_slice_in_dim(w_step.T, y * 2 * heads, 2 * heads, 0)
    pair = jnp.where(c == 0, pair, jnp.roll(pair, heads, axis=0))
    w_steps = jnp.pad(pair, ((0, 8 - 2 * heads), (0, 0)))
    rates = jnp.broadcast_to(jnp.stack([step_bias, decay_rate])[:, :, None], (2, heads, 128))
    jump = jnp.concatenate([decay_jump.transpose(0, 2, 1), rates], axis=2)
    jump = jnp.concatenate([jump, swap(jump)], axis=1)
    jump = jnp.pad(jump, ((0, 0), (0, 8 - 2 * heads), (0, 0)))
    rates = jump[:, :, tp_count * rows :]
    jump = jump[:, :, : tp_count * rows].reshape(2, 8, tp_count, rows).transpose(2, 1, 0, 3)
    jump = jump.reshape(tp_count, 8, 2 * rows)

    def add(runs, xs, halo, far, end):
        return piece_states(meta, xs, halo, far, end, w_steps, w_both, jump, rates, runs, rows, y_count)

    runs = add(None, [first], None, 0, False)
    for s in range(1, half):
        a.append(onward(a[s]))
        if s + 1 < half:
            b.append(onward(b[s]))
        runs = add(runs, [a[s], b[s]], None, s, False)

    fixed, query = terms(step_bias, decay_rate, new_step, new_value, new_key, new_query, new_gate, read_gain)
    runs, fixed, query = lax.optimization_barrier((runs, fixed, query))
    last = onward(b[half - 1][2 * rows + 8 :])
    own, other = add(runs, [a[half]], last, half, True)
    sent = packed(meta, own, swap(other), query, sp_count, y_count)
    got = lax.all_to_all(sent, "sp", 0, 0, tiled=True)
    return tuple(finished(meta, got, fixed))


def solution(mesh):
    tp = ("y", "c")
    chips = Mesh(mesh.devices.reshape(mesh.shape["sp"], mesh.shape["tp"] // 2, 2), ("sp", *tp))

    return jax.shard_map(
        per_device,
        mesh=chips,
        in_specs=(
            P(None, ("sp", *tp), None), P(None, tp), P(None, tp), P(), P(None, tp), P(None, tp), P(tp), P(tp),
            P(None, "sp", tp), P(None, tp), P(None, tp), P(None, tp), P(None, tp), P(None, tp), P(tp),
        ),
        out_specs=(P(None, tp, "sp", None), P(None, tp, "sp")),
        check_vma=False,
    )
```
